32 devices in a mesh: sp: 8 (over z, y), tp: 4 (over x, core).
Axes of the slice: x: 2, y: 2, z: 4, core: 2. Of those that a mesh axis runs over, the one named last changes fastest.
Arguments:
- resid: bfloat16 [4096, 2048], P('sp', 'tp'), may hold values from -41 to 41
- queries: bfloat16 [4096, 1024], P('sp', 'tp'), may hold values from -6 to 6
- keys: bfloat16 [4096, 1024], P('sp', 'tp'), may hold values from -6 to 6
- values: bfloat16 [4096, 1024], P('sp', 'tp'), may hold values from -6 to 6
- mix_lambda: float32 [8], P('tp'), may hold values from 0.3 to 0.8
- head_gain: float32 [128], replicated, may hold values from 0.1 to 1.9
- out_weight: bfloat16 [1024, 2048], P(None, 'tp'), may hold values from -0.1875 to 0.1875
- norm_gain: float32 [2048], P('tp'), may hold values from 0.1 to 1.9
- gate_weight: bfloat16 [2048, 5632], P('sp', 'tp'), may hold values from -0.125 to 0.125
- up_weight: bfloat16 [2048, 5632], P('sp', 'tp'), may hold values from -0.125 to 0.125
- conv_weight: float32 [3, 5632], P(None, 'tp'), may hold values from -3.5 to 3.5
- conv_bias: float32 [5632], P('tp'), may hold values from -3 to 3
- down_weight: bfloat16 [5632, 2048], P('tp', 'sp'), may hold values from -0.078125 to 0.078125
Outputs:
- layer_out: bfloat16 [4096, 2048], P('sp', 'tp')
The draws below stay inside these ranges and needn't reach their ends.
All inputs are finite; a program needn't handle non-finite values.
Results may differ from the reference program's by a relative error of at most 0.009.
Values may be sent and summed in bfloat16 or wider, within the bound.
A program may use at most 128 MiB of HBM per device.

```python
import math
import jax
import jax.numpy as jnp
from jax import lax

D = 2048
HEADS = 8
HD = 64
VD = 128
FF = 5632
TOKENS = 4096
N_TP = 4


def pair_draw(key):
    width = HEADS * 2 * HD
    query_part = 1.3 * jnp.clip(jax.random.normal(jax.random.fold_in(key, 11), (TOKENS, width), jnp.float32), -4.0, 4.0)
    key_part = 1.3 * jnp.clip(jax.random.normal(jax.random.fold_in(key, 12), (TOKENS, width), jnp.float32), -4.0, 4.0)
    return (query_part, key_part)


def draw_queries(key, part):
    return pair_draw(key)[0].astype(jnp.bfloat16)


def draw_keys(key, part):
    return pair_draw(key)[1].astype(jnp.bfloat16)


def draw_resid(key, part):
    base = jax.random.fold_in(key, 21)
    row_scale = 10.0 ** (jax.random.uniform(jax.random.fold_in(base, 1), (TOKENS, 1), jnp.float32) - 0.5)
    position = jnp.arange(D, dtype=jnp.float32)[None, :] / D
    column_scale = 10.0 ** (0.7 * position + 0.3 * jax.random.uniform(jax.random.fold_in(base, 2), (1, D), jnp.float32) - 0.5)
    noise = jnp.clip(jax.random.normal(jax.random.fold_in(base, 4), (TOKENS, D), jnp.float32), -4.0, 4.0)
    return (noise * row_scale * column_scale).astype(jnp.bfloat16)


def levels(own_key, extent, pieces, smallest, high):
    loudness = 1.0
    for dim, blocks in pieces:
        steps = jax.random.uniform(jax.random.fold_in(jax.random.fold_in(own_key, 6), dim), (blocks,), jnp.float32, smallest / len(pieces), high / len(pieces))
        loudness = loudness * jnp.repeat(jnp.exp(steps), extent[dim] // blocks).reshape((-1,) + (1,) * (len(extent) - 1 - dim))
    return loudness


def normal_values(own_key, extent, scale, most, cuts=(), kind=jnp.bfloat16):
    level = levels(own_key, extent, cuts, -0.22, 0.18) if cuts else 1.0
    result = jax.random.normal(own_key, extent, jnp.float32) * scale * level
    return jnp.minimum(jnp.maximum(result, -most), most).astype(kind)


def setup_inputs(seed: int = 0) -> dict:
    arg_keys = jax.random.split(jax.random.key(seed), 14)
    resid = draw_resid(jax.random.fold_in(arg_keys[13], 71), 0)
    queries = draw_queries(jax.random.fold_in(arg_keys[13], 71), 0)
    keys = draw_keys(jax.random.fold_in(arg_keys[13], 71), 0)
    values = normal_values(arg_keys[3], (TOKENS, HEADS * VD), 1.0, 6.0, ((0, 8), (1, 4)))
    mix_lambda = jnp.clip(0.3 + 0.5 * jax.random.uniform(arg_keys[4], (HEADS,), jnp.float32) ** levels(arg_keys[4], (HEADS,), ((0, 4),), -0.2, 0.2), 0.3, 0.8)
    head_gain = jnp.clip(1.0 + 0.18 * jax.random.normal(arg_keys[5], (VD,), jnp.float32), 0.1, 1.9)
    out_weight = normal_values(arg_keys[6], (HEADS * VD, D), (HEADS * VD) ** -0.5, 0.1875, ((1, 4),))
    norm_gain = jnp.clip(1.0 + 0.18 * jax.random.normal(arg_keys[7], (D,), jnp.float32), 0.1, 1.9)
    gate_weight = normal_values(arg_keys[8], (D, FF), D ** -0.5, 0.125, ((0, 8), (1, 4)))
    up_weight = normal_values(arg_keys[9], (D, FF), D ** -0.5, 0.125, ((0, 8), (1, 4)))
    conv_weight = normal_values(arg_keys[10], (3, FF), 3 ** -0.5, 3.5, ((1, 4),), jnp.float32)
    conv_bias = normal_values(arg_keys[11], (FF,), 0.5, 3.0, ((0, 4),), jnp.float32)
    down_weight = normal_values(arg_keys[12], (FF, D), FF ** -0.5, 0.078125, ((0, 4), (1, 8)))
    return {"resid": resid, "queries": queries, "keys": keys, "values": values, "mix_lambda": mix_lambda, "head_gain": head_gain, "out_weight": out_weight, "norm_gain": norm_gain, "gate_weight": gate_weight, "up_weight": up_weight, "conv_weight": conv_weight, "conv_bias": conv_bias, "down_weight": down_weight}


def head_attention(query_head, key_head, value_head, weight_two):
    length = query_head.shape[0]
    scale = HD ** (-0.5)
    block = math.gcd(length, 512)
    query_blocks = query_head.reshape(length // block, block, 2, HD)
    key_float = key_head.astype(jnp.float32)
    value_float = value_head.astype(jnp.float32)

    def one_block(query_block):
        scores = jnp.einsum('qmd,kmd->mqk', query_block.astype(jnp.float32), key_float) * scale
        highest = lax.optimization_barrier(jnp.max(scores, axis=-1, keepdims=True))
        shifted = jnp.exp(scores - highest)
        totals = lax.optimization_barrier(jnp.sum(shifted, axis=-1))
        unnormed = lax.optimization_barrier(shifted.astype(jnp.bfloat16)).astype(jnp.float32)
        mapped = jnp.einsum('mqk,ke->mqe', unnormed, value_float) / totals[..., None]
        return mapped[0] - weight_two * mapped[1]
    return lax.map(one_block, query_blocks).reshape(length, VD)

def reference(resid, queries, keys, values, mix_lambda, head_gain, out_weight, norm_gain, gate_weight, up_weight, conv_weight, conv_bias, down_weight):
    length = queries.shape[0]
    query_heads = jnp.transpose(queries.reshape(length, HEADS, 2, HD), (1, 0, 2, 3))
    key_heads = jnp.transpose(keys.reshape(length, HEADS, 2, HD), (1, 0, 2, 3))
    value_heads = jnp.transpose(values.reshape(length, HEADS, VD), (1, 0, 2))
    mixed = lax.map(lambda parts: head_attention(parts[0], parts[1], parts[2], parts[3]), (query_heads, key_heads, value_heads, mix_lambda))
    spread = lax.optimization_barrier(jnp.mean(mixed * mixed, axis=-1, keepdims=True))
    normed = mixed * lax.rsqrt(spread + 1e-06) * head_gain * 0.8
    heads_out = jnp.transpose(normed, (1, 0, 2)).reshape(length, HEADS * VD).astype(jnp.bfloat16)
    after_mixer = resid.astype(jnp.float32) + jnp.dot(heads_out, out_weight, preferred_element_type=jnp.float32)
    squares = lax.optimization_barrier(jnp.mean(after_mixer * after_mixer, axis=-1, keepdims=True))
    normed_rows = (after_mixer * lax.rsqrt(squares + 1e-06) * norm_gain).astype(jnp.bfloat16)
    gated = jnp.dot(normed_rows, gate_weight, preferred_element_type=jnp.float32).astype(jnp.bfloat16)
    upward = jnp.dot(normed_rows, up_weight, preferred_element_type=jnp.float32)
    padded = jnp.pad(gated.astype(jnp.float32), ((1, 1), (0, 0)))
    conv = padded[:-2] * conv_weight[0] + padded[1:-1] * conv_weight[1] + padded[2:] * conv_weight[2] + conv_bias
    hidden = (jax.nn.silu(conv) * upward).astype(jnp.bfloat16)
    span = FF // N_TP
    hidden_blocks = jnp.transpose(hidden.reshape(length, N_TP, span), (1, 0, 2))
    down_blocks = down_weight.reshape(N_TP, span, D)

    def block_sum(carry, pair):
        part = jnp.dot(pair[0], pair[1], preferred_element_type=jnp.float32).astype(jnp.bfloat16)
        return (carry + part.astype(jnp.float32), None)
    mixer_out, unused = lax.scan(block_sum, jnp.zeros((length, D), jnp.float32), (hidden_blocks, down_blocks))
    return (after_mixer + mixer_out).astype(jnp.bfloat16)
```

```python
import functools
import math

import jax
import jax.numpy as jnp
from jax import lax
from jax.experimental import pallas as pl
from jax.experimental.pallas import tpu as pltpu
from jax.sharding import PartitionSpec as P

D = 2048
HD = 64
VD = 128


def with_halo(cells, sides, width):
    for axis, dim in sides:
        count = lax.axis_size(axis)
        ends = count - 1
        head = lax.slice_in_dim(cells, 0, width, axis=dim)
        tail = lax.slice_in_dim(cells, cells.shape[dim] - width, cells.shape[dim], axis=dim)
        cells = jnp.concatenate(
            [
                lax.ppermute(tail, axis, [(i, (i + 1) % count) for i in range(ends)]),
                cells,
                lax.ppermute(head, axis, [((i + 1) % count, i) for i in range(ends)]),
            ],
            axis=dim,
        )
    return cells


def on_device(
    resid,
    queries,
    keys,
    values,
    mix_lambda,
    head_gain,
    out_weight,
    norm_gain,
    gate_weight,
    up_weight,
    conv_weight,
    conv_bias,
    down_weight,
):
    length = queries.shape[0]
    heads = mix_lambda.shape[0]
    scale = HD ** (-0.5)
    query_heads = queries.reshape(length, heads, 2, HD)
    initial = (
        jnp.full((heads, 2, length), -1e30, jnp.float32),
        jnp.zeros((heads, 2, length), jnp.float32),
        jnp.zeros((heads, 2, length, VD), jnp.float32),
    )
    key_rows = lax.all_gather(keys, "sp", axis=0, tiled=True)
    value_rows = lax.all_gather(values, "sp", axis=0, tiled=True)
    count = key_rows.shape[0]
    block = math.gcd(count, 2048)
    key_blocks = key_rows.reshape(count // block, block, heads, 2, HD)
    value_blocks = value_rows.reshape(count // block, block, heads, VD)

    def advance(state, blocks):
        running, totals, weighted = state
        key_block, value_block = blocks
        scores = (
            jnp.einsum(
                "qhmd,khmd->hmqk", query_heads, key_block, preferred_element_type=jnp.float32
            )
            * scale
        )
        highest = jnp.maximum(running, jnp.max(scores, axis=-1))
        factor = jnp.exp(running - highest)
        shifted = jnp.exp(scores - highest[..., None])
        totals = totals * factor + jnp.sum(shifted, axis=-1)
        weighted = weighted * factor[..., None] + jnp.einsum(
            "hmqk,khe->hmqe",
            shifted.astype(jnp.bfloat16),
            value_block,
            preferred_element_type=jnp.float32,
        )
        return ((highest, totals, weighted), None)

    result, unused = lax.scan(advance, initial, (key_blocks, value_blocks))
    running, totals, weighted = result
    mapped = weighted / totals[..., None]
    mixed = mapped[:, 0] - mix_lambda[:, None, None] * mapped[:, 1]
    spread = jnp.mean(mixed * mixed, axis=-1, keepdims=True)
    normed = mixed * lax.rsqrt(spread + 1e-06) * head_gain * 0.8
    heads_out = jnp.transpose(normed, (1, 0, 2)).reshape(length, heads * VD).astype(jnp.bfloat16)
    projected = jnp.dot(
        lax.all_gather(heads_out, "tp", axis=1, tiled=True),
        out_weight,
        preferred_element_type=jnp.float32,
    )
    after_mixer = resid.astype(jnp.float32) + projected
    squares = lax.psum(jnp.sum(after_mixer * after_mixer, axis=1), "tp")
    normed_rows = (after_mixer * lax.rsqrt(squares / D + 1e-06)[:, None] * norm_gain).astype(
        jnp.bfloat16
    )
    full_rows = lax.all_gather(normed_rows, "tp", axis=1, tiled=True)
    gate_sum = jnp.dot(
        full_rows,
        lax.all_gather(gate_weight, "sp", axis=0, tiled=True),
        preferred_element_type=jnp.float32,
    )
    upward = jnp.dot(
        full_rows,
        lax.all_gather(up_weight, "sp", axis=0, tiled=True),
        preferred_element_type=jnp.float32,
    )
    gated = gate_sum.astype(jnp.bfloat16)
    padded = with_halo(gated, (("sp", 0),), 1).astype(jnp.float32)
    conv = (
        padded[:-2] * conv_weight[0]
        + padded[1:-1] * conv_weight[1]
        + padded[2:] * conv_weight[2]
        + conv_bias
    )
    hidden = (jax.nn.silu(conv) * upward).astype(jnp.bfloat16)
    partial_terms = jnp.dot(
        hidden,
        lax.all_gather(down_weight, "sp", axis=1, tiled=True),
        preferred_element_type=jnp.float32,
    )
    mixer_out = lax.psum_scatter(
        partial_terms.astype(jnp.bfloat16), "tp", scatter_dimension=1, tiled=True
    ).astype(jnp.float32)
    return (after_mixer + mixer_out).astype(jnp.bfloat16)


EDGE = 16
LANES = 128


def layer_kernel(
    sp,
    tp,
    resid,
    queries,
    keys,
    values,
    mix_lambda,
    head_gain,
    out_weight,
    norm_gain,
    gate_weight,
    up_weight,
    conv_weight,
    conv_bias,
    down_weight,
    out,
    q_all,
    qs,
    kv,
    gates,
    ups,
    downs,
    peaks,
    totals,
    weighted,
    heads_own,
    heads_all,
    out_all,
    resid_all,
    gain_all,
    after,
    after_own,
    rows_all,
    gate_acc,
    up_acc,
    hidden,
    held,
    stage,
    from_core,
    from_x,
    from_z,
    local_sem,
    send_sem,
    recv_sem,
    q_sem,
    head_send,
    head_recv,
    out_send,
    out_recv,
    resid_send,
    resid_recv,
    gain_send,
    gain_recv,
    row_sem,
    after_sem,
    edge_send,
    edge_recv,
    part_send,
    core_recv,
    x_recv,
    z_recv,
):
    bf16, f32 = jnp.bfloat16, jnp.float32
    div, rem = lax.div, lax.rem
    me = lax.axis_index("sp")
    t = lax.axis_index("tp")
    z, y = div(me, 2), rem(me, 2)
    h, q = div(z, 2), rem(z, 2)
    x, c = div(t, 2), rem(t, 2)
    mate = me + 2 - 4 * q
    across = me + 1 - 2 * y
    far = me + 4 - 8 * h
    fmate = far + 2 - 4 * q
    adjacent = me + 2 - 4 * h
    amate = across + 2 - 4 * q
    afar = across + 4 - 8 * h
    afmate = afar + 2 - 4 * q
    inner = h != q
    sibling = t + 1 - 2 * c
    xdev = t + 2 - 4 * x
    xsib = sibling + 2 - 4 * x

    length = queries.shape[0]
    depth, ff = gate_weight.shape
    features = resid.shape[1]
    big = gates.shape[2]
    small = ff - big
    down_cols = down_weight.shape[1]
    half_sp = sp // 2
    K, V, GATE, UP, DOWN = range(5)
    ACROSS, FAR, MATE, ADJACENT = range(4)

    drains = []

    def both(a, b):
        return b if a is None else jnp.logical_and(a, b)

    def when(cond, body):
        if cond is None:
            body()
        else:
            pl.when(cond)(body)

    def remote(src, dst, send, recv, target):
        return pltpu.make_async_remote_copy(
            src_ref=src,
            dst_ref=dst,
            send_sem=send,
            recv_sem=recv,
            device_id=target,
            device_id_type=pl.DeviceIdType.MESH,
        )

    def ship(make, cond=None):
        when(cond, lambda: make().start())
        drains.append((cond, make))

    def variants(array, part):
        if array in (K, V):
            return ((None, 0),)
        return ((c == part, big), (c != part, small))

    def landing(array, src, size):
        if array in (K, V):
            return kv.at[src, array]
        if array == DOWN:
            return downs.at[src, pl.ds(0, size)]
        return (gates, ups)[array - GATE].at[src, :, pl.ds(0, size)]

    def origin(array, part, size):
        if array in (K, V):
            cols = pl.ds(pl.multiple_of(part * VD, VD), VD)
            return (keys, values)[array].at[:, cols]
        cut = pl.ds(pl.multiple_of(part * (ff - size), LANES), size)
        if array == DOWN:
            return down_weight.at[cut]
        return (gate_weight, up_weight)[array - GATE].at[:, cut]

    def send(array, src, way, target, part=None, cond=None):
        for which, size in variants(array, q if part is None else part):

            def make(size=size):
                here = landing(array, src, size)
                return remote(
                    here if part is None else origin(array, part, size),
                    here,
                    send_sem.at[array, way, src],
                    recv_sem.at[array, src],
                    {"sp": target},
                )

            ship(make, both(cond, which) if which is not None else cond)

    def feed(array, *ways):
        other = 1 - q
        for way in ways:
            if way == ACROSS:
                send(array, me, ACROSS, across, part=q)
            elif way == FAR:
                send(array, me, FAR, far, part=q)
            elif way == MATE:
                send(array, me, MATE, mate, part=other)
            else:
                send(array, me, ADJACENT, adjacent, part=other, cond=inner)

    def arrive(array, src):
        for which, size in variants(array, q):

            def wait(size=size):
                here = landing(array, src, size)
                remote(
                    here, here, send_sem.at[array, 0, src], recv_sem.at[array, src], {"sp": across}
                ).wait_recv()

            when(which, wait)

    def pass_on(array, src, *ways):
        arrive(array, src)
        for way in ways:
            if way == FAR:
                send(array, src, FAR, far, cond=inner)
            else:
                send(array, src, ACROSS, across)

    for way in (MATE, ADJACENT, FAR, ACROSS):
        for array in (K, V):
            feed(array, way)

    def q_copy():
        cols = pl.ds(pl.multiple_of((1 - q) * VD, VD), VD)
        return remote(queries.at[:, cols], q_all.at[q], q_sem.at[0], q_sem.at[1], {"sp": mate})

    ship(q_copy)

    local = []

    def fetch(src, dst, cond=None):
        sem = local_sem.at[len(local)]
        make = lambda: pltpu.make_async_copy(src, dst, sem)
        local.append((cond, make))
        when(cond, lambda: make().start())

    def fetched(first, last=None):
        for cond, make in local[first:last]:
            when(cond, lambda: make().wait())

    own_cols = pl.ds(pl.multiple_of(q * VD, VD), VD)
    fetch(queries.at[:, own_cols], q_all.at[q])
    for array in (K, V):
        fetch(origin(array, q, 0), landing(array, me, 0))
    early = len(local)
    for array in (GATE, UP, DOWN):
        for which, size in variants(array, q):
            fetch(origin(array, q, size), landing(array, me, size), which)
    fetch(out_weight, out_all.at[t])
    fetch(resid, resid_all.at[t], c == q)
    fetch(norm_gain, gain_all.at[t])

    def out_copy(src, slot, target, send):
        return lambda: remote(
            src, out_all.at[slot], out_send.at[send], out_recv.at[slot], {"tp": target}
        )

    def gain_copy(target, send):
        return lambda: remote(
            norm_gain, gain_all.at[t], gain_send.at[send], gain_recv.at[t], {"tp": target}
        )

    def resid_copy(src, slot, target, send):
        return lambda: remote(
            src, resid_all.at[slot], resid_send.at[send], resid_recv.at[slot], target
        )

    for i, target in enumerate((sibling, xdev, xsib)):
        ship(gain_copy(target, i))
    ship(out_copy(out_weight, t, xdev, 0))
    ship(resid_copy(resid, t, {"tp": 2 * (1 - x) + q}, 0))
    ship(out_copy(out_weight, t, sibling, 1))
    ship(resid_copy(resid, t, {"tp": sibling}, 1), c != q)

    peaks[...] = jnp.full(peaks.shape, -1e30, f32)
    totals[...] = jnp.zeros(totals.shape, f32)
    weighted[...] = jnp.zeros(weighted.shape, f32)

    @pl.when(c != q)
    def _():
        downs[:, small:, :] = jnp.zeros((sp, big - small, down_cols), bf16)

    fetched(0, early)
    lanes = lax.broadcasted_iota(jnp.int32, (1, VD), 1)

    def spread_queries(block):
        value = q_all[block].astype(f32) * HD**-0.5
        at = pl.ds(pl.multiple_of(block * length, length), length)
        for m in range(2):
            keep = lanes < HD if m == 0 else lanes >= HD
            qs[m, at, :] = jnp.where(keep, value, 0.0).astype(bf16)

    rows = math.gcd(length, 256)

    def attend(src, first=0, last=2 * length // rows):
        def row_block(r, carry):
            at = pl.ds(pl.multiple_of(r * rows, rows), rows)
            key_block = kv[src, K]
            value_block = kv[src, V]
            for m in range(2):
                s = lax.dot_general(
                    qs[m, at, :], key_block, (((1,), (1,)), ((), ())), preferred_element_type=f32
                )
                old = peaks[m, at, :]
                new = jnp.maximum(old, jnp.max(s, axis=1, keepdims=True))
                factor = jnp.exp(old - new)
                p = jnp.exp(s - jnp.concatenate([new] * (length // VD), axis=1))
                peaks[m, at, :] = new
                summed = totals[m, at, :] * factor
                for j in range(length // VD):
                    summed = summed + p[:, j * VD : (j + 1) * VD]
                totals[m, at, :] = summed
                weighted[m, at, :] = weighted[m, at, :] * factor + jnp.dot(
                    p.astype(bf16), value_block, preferred_element_type=f32
                )
            return carry

        lax.fori_loop(first, last, row_block, 0)

    def kv_pass(src, *ways):
        for array in (K, V):
            pass_on(array, src, *ways)

    per_block = length // rows
    spread_queries(q)
    attend(me, q * per_block, (q + 1) * per_block)
    kv_pass(mate, FAR, ACROSS)
    feed(GATE, ADJACENT, FAR, MATE, ACROSS)
    q_copy().wait_recv()
    spread_queries(1 - q)
    attend(me, (1 - q) * per_block, (2 - q) * per_block)
    attend(mate)
    kv_pass(across)
    attend(across)
    kv_pass(far, ACROSS)
    kv_pass(amate)
    attend(amate)
    kv_pass(fmate, ACROSS)
    pass_on(GATE, mate, FAR, ACROSS)
    feed(UP, ADJACENT, FAR, MATE, ACROSS)
    attend(far)
    ship(resid_copy(resid, t, {"sp": mate, "tp": 2 * x + q}, 2))
    attend(fmate)
    kv_pass(afar)
    attend(afar)
    feed(DOWN, ADJACENT, FAR, MATE)
    kv_pass(afmate)
    attend(afmate)

    head = 2 * t + q
    for b in range(2):
        at = slice(b * length, (b + 1) * length)
        first = weighted[0, at, :] / jnp.sum(totals[0, at, :], axis=1, keepdims=True)
        second = weighted[1, at, :] / jnp.sum(totals[1, at, :], axis=1, keepdims=True)
        mixed = first - mix_lambda[q] * second
        spread = jnp.mean(mixed * mixed, axis=1, keepdims=True)
        normed = mixed * lax.rsqrt(spread + 1e-06) * head_gain[...] * 0.8
        heads_own[b] = normed.astype(bf16)

        @pl.when(c == b)
        def _():
            heads_all[head] = heads_own[b]

    def head_copy(src, slot, target, send):
        return lambda: remote(
            src, heads_all.at[slot], head_send.at[send], head_recv.at[slot], target
        )

    for b in range(2):
        ship(head_copy(heads_own.at[b], head, {"sp": mate, "tp": 2 * x + b}, b))
    for b in range(2):
        ship(head_copy(heads_own.at[b], head, {"tp": 2 * (1 - x) + b}, 2 + b))
        ship(head_copy(heads_own.at[b], head, {"tp": sibling}, 4 + b), c != b)

    def head_wait(slot):
        head_copy(heads_all.at[slot], slot, {"tp": sibling}, 0)().wait_recv()

    out_copy(out_weight, xdev, sibling, 0)().wait_recv()
    ship(out_copy(out_all.at[xdev], xdev, sibling, 2))

    def resid_wait(slot):
        resid_copy(resid, slot, {"tp": sibling}, 0)().wait_recv()

    for k in range(2):
        slot = 2 * x + k
        when(c != q, lambda: resid_wait(slot))
        ship(resid_copy(resid_all.at[slot], slot, {"tp": xdev}, 3 + k), c != q)
    for k in range(2):
        slot = 2 * (2 * x + k) + 1 - q
        head_wait(slot)
        ship(head_copy(heads_all.at[slot], slot, {"tp": xdev}, 6 + k))

    pass_on(UP, mate, FAR, ACROSS)
    pass_on(GATE, far, ACROSS)
    fetched(early)

    out_copy(out_weight, sibling, sibling, 0)().wait_recv()
    out_copy(out_weight, xsib, sibling, 0)().wait_recv()
    for slot in (sibling, xdev, xsib):
        remote(
            norm_gain, gain_all.at[slot], gain_send.at[0], gain_recv.at[slot], {"tp": sibling}
        ).wait_recv()
    when(c == q, lambda: resid_wait(sibling))
    for k in range(2):
        resid_wait(2 * (1 - x) + k)
    head_wait(2 * sibling + q)
    for k in range(2):
        head_wait(2 * (2 * (1 - x) + k) + q)
    for k in range(2):
        head_wait(2 * (2 * (1 - x) + k) + 1 - q)

    row_sum = jnp.zeros((length, 1), f32)
    for j in range(tp):
        cols = slice(j * features, (j + 1) * features)
        total = resid_all[j].astype(f32) + jnp.dot(
            jnp.concatenate([heads_all[i] for i in range(heads_all.shape[0])], axis=1),
            out_all[j],
            preferred_element_type=f32,
        )
        after[:, cols] = total
        row_sum = row_sum + jnp.sum(total * total, axis=1, keepdims=True)
    inverse = lax.rsqrt(row_sum / D + 1e-06)
    for j in range(tp):
        cols = slice(j * features, (j + 1) * features)
        rows_all[c, EDGE : EDGE + length, cols] = (
            after[:, cols] * inverse * gain_all[j]
        ).astype(bf16)

    def row_copy(block):
        here = rows_all.at[block, pl.ds(EDGE, length)]
        return remote(here, here, row_sem.at[0], row_sem.at[1], {"tp": sibling})

    ship(lambda: row_copy(c))

    def own_features(device):
        return pl.ds(pl.multiple_of(device * features, features), features)

    def after_copy():
        return remote(
            after.at[:, own_features(sibling)],
            after_own,
            after_sem.at[0],
            after_sem.at[1],
            {"tp": sibling},
        )

    ship(after_copy, c == q)

    @pl.when(c == q)
    def _():
        after_own[...] = after[:, own_features(t)]

    pass_on(GATE, fmate, ACROSS)
    feed(DOWN, ACROSS)
    row_copy(1 - c).wait_recv()

    begin, end, top, bottom = EDGE, length, 0, EDGE + length

    def edge_copy(i, source_block, source, block, dest, target):
        def rows_at(start):
            return pl.ds(pl.multiple_of(start, EDGE), EDGE)

        return remote(
            rows_all.at[source_block, rows_at(source)],
            rows_all.at[block, rows_at(dest)],
            edge_send.at[i],
            edge_recv.at[i],
            {"sp": target},
        )

    def pick(first, second):
        return first + y * (second - first)

    def edge(i):
        return (
            lambda: edge_copy(0, 0, pick(end, begin), 0, pick(top, bottom), across),
            lambda: edge_copy(
                1, pick(1, 0), pick(begin, end), pick(0, 1), pick(bottom, top), across
            ),
            lambda: edge_copy(2, 1, pick(end, begin), 1, pick(top, bottom), across),
        )[i]

    for i in range(3):
        ship(edge(i))
    before = jnp.logical_and(y == 1, h == 0)
    behind = jnp.logical_and(y == 0, h == 1)
    onward = lambda: edge_copy(3, 1, end, 0, top, jnp.minimum(me + half_sp - 1, sp - 1))
    back = lambda: edge_copy(3, 0, begin, 1, bottom, jnp.maximum(me - half_sp + 1, 0))
    ship(onward, before)
    ship(back, behind)

    @pl.when(jnp.logical_and(y == 0, h == 0))
    def _():
        rows_all[0, 0:EDGE, :] = jnp.zeros((EDGE, rows_all.shape[2]), bf16)

    @pl.when(jnp.logical_and(y == 1, h == 1))
    def _():
        rows_all[1, EDGE + length :, :] = jnp.zeros((EDGE, rows_all.shape[2]), bf16)

    for array in (GATE, UP):
        arrive(array, across)
        arrive(array, amate)
    pass_on(DOWN, mate, FAR, ACROSS)

    for i in range(3):
        edge(i)().wait_recv()
    when(before, lambda: onward().wait_recv())
    when(behind, lambda: back().wait_recv())

    span = half_sp * depth
    wide = 2 * LANES

    def expand(acc, weight, half, start, count, fresh):
        deep = pl.ds(pl.multiple_of(half * span, span), span)
        blocks = pl.ds(half * half_sp, half_sp)

        def tile(i, carry):
            b, cols = rem(i, 2), pl.ds(pl.multiple_of(div(i, 2) * wide, wide), wide)
            part = jnp.dot(
                rows_all[b, start : start + count, deep],
                weight[blocks, :, cols].reshape(span, wide),
                preferred_element_type=f32,
            )
            if fresh:
                acc[b, :, cols] = part
            else:
                acc[b, :, cols] += part
            return carry

        lax.fori_loop(0, 2 * (big // wide), tile, 0)

    expand(gate_acc, gates, h, 0, length + 2 * EDGE, True)
    expand(up_acc, ups, h, EDGE, length, True)
    pass_on(UP, far, ACROSS)
    arrive(GATE, afar)
    arrive(GATE, afmate)
    expand(gate_acc, gates, 1 - h, 0, length + 2 * EDGE, False)
    pass_on(UP, fmate, ACROSS)
    arrive(UP, afar)
    arrive(UP, afmate)
    expand(up_acc, ups, 1 - h, EDGE, length, False)

    base = jnp.where(c == q, q * (ff - big), q * (ff - small))

    def activate(b, carry):
        for j in range(big // LANES):
            cols = slice(j * LANES, (j + 1) * LANES)
            spot = jnp.minimum(base + j * LANES, ff - LANES)
            taps = pl.ds(pl.multiple_of(spot, LANES), LANES)

            def fill():
                def tap(start):
                    return gate_acc[b, start : start + length, cols].astype(bf16).astype(f32)

                conv = (
                    tap(EDGE - 1) * conv_weight[0:1, taps]
                    + tap(EDGE) * conv_weight[1:2, taps]
                    + tap(EDGE + 1) * conv_weight[2:3, taps]
                    + conv_bias[:, taps]
                )
                hidden[b, :, cols] = (conv / (1.0 + jnp.exp(-conv)) * up_acc[b, :, cols]).astype(
                    bf16
                )

            if (j + 1) * LANES <= small:
                fill()
            else:
                pl.when(c == q)(fill)

                @pl.when(c != q)
                def _():
                    hidden[b, :, cols] = jnp.zeros((length, LANES), bf16)

        return carry

    lax.fori_loop(0, 2, activate, 0)

    per = sp // tp

    def owner(s):
        o = div(s, per)
        return div(o, 2), rem(o, 2)

    def core_slot(s):
        return div(s, half_sp) * per + rem(s, per)

    def core_copy(s):
        return remote(
            stage.at[s], from_core.at[core_slot(s)], part_send.at[s],
            core_recv.at[core_slot(s)], {"tp": sibling},
        )

    def x_copy(s):
        return remote(
            stage.at[s], from_x.at[rem(s, per)], part_send.at[s], x_recv.at[rem(s, per)],
            {"tp": xdev},
        )

    def z_copy(s):
        return remote(
            stage.at[s, 0], from_z.at[rem(s, per)], part_send.at[s], z_recv.at[rem(s, per)],
            {"sp": mate},
        )

    def multiply(s):
        ox, oc = owner(s)
        product = jnp.dot(
            hidden[...].reshape(2 * length, big), downs[s], preferred_element_type=f32
        ).reshape(2, length, down_cols)

        @pl.when(c != oc)
        def _():
            stage[s] = product.astype(bf16)

        @pl.when(c == oc)
        def _():
            held[core_slot(s)] = product

        ship(lambda: core_copy(s), c != oc)

    def add_core(s):
        ox, oc = owner(s)
        mine = c == oc
        slot = core_slot(s)
        when(mine, lambda: core_copy(s).wait_recv())

        @pl.when(jnp.logical_and(mine, x != ox))
        def _():
            stage[s] = (held[slot] + from_core[slot].astype(f32)).astype(bf16)

        ship(lambda: x_copy(s), jnp.logical_and(mine, x != ox))

    def out_cols(s):
        return pl.ds(pl.multiple_of(rem(s, per) * down_cols, down_cols), down_cols)

    def add_x(s):
        ox, oc = owner(s)
        mine = jnp.logical_and(c == oc, x == ox)
        slot = core_slot(s)

        def summed(b):
            return (
                held[slot, b]
                + from_core[slot, b].astype(f32)
                + from_x[rem(s, per), b].astype(f32)
            )

        @pl.when(mine)
        def _():
            x_copy(s).wait_recv()
            stage[s, 0] = summed(1 - q).astype(bf16)

        ship(lambda: z_copy(s), mine)

        @pl.when(mine)
        def _():
            after_own[:, out_cols(s)] += summed(q)

    near = (me, mate, across, amate)
    fetched_down = (across, amate)
    for s in fetched_down:
        arrive(DOWN, s)
    for s in near:
        multiply(s)
    for s in near:
        add_core(s)
    pass_on(DOWN, far, ACROSS)
    multiply(far)
    pass_on(DOWN, fmate, ACROSS)
    multiply(fmate)
    when(c != q, lambda: after_copy().wait_recv())
    for s in near:
        add_x(s)
    add_core(far)
    add_core(fmate)
    for s in (afar, afmate):
        arrive(DOWN, s)
        multiply(s)
    for s in (afar, afmate):
        add_core(s)
    for s in (far, fmate, afar, afmate):
        add_x(s)
    for k in range(per):
        cols = slice(k * down_cols, (k + 1) * down_cols)
        z_copy(k).wait_recv()
        out[:, cols] = (after_own[:, cols] + from_z[k].astype(f32)).astype(bf16)

    for cond, make in drains:
        when(cond, lambda: make().wait_send())


def fused(sp, tp, *args):
    resid, queries, keys, values = args[:4]
    gate_weight, down_weight = args[8], args[12]
    length, width = queries.shape
    features = resid.shape[1]
    depth, ff = gate_weight.shape
    maps = 2
    heads = tp * (width // VD)
    full = tp * features
    bf16, f32 = jnp.bfloat16, jnp.float32
    dma = pltpu.SemaphoreType.DMA
    vmem = pl.BlockSpec(memory_space=pltpu.VMEM)
    smem = pl.BlockSpec(memory_space=pltpu.SMEM)
    hbm = pl.BlockSpec(memory_space=pl.ANY)
    rows = length + 2 * EDGE
    down_cols = down_weight.shape[1]
    tiles = ff // LANES
    big = (tiles - tiles // 2) * LANES
    per = sp // tp
    args = list(args)
    for i in (5, 7, 11):
        args[i] = args[i].reshape(1, -1)
    return pl.pallas_call(
        functools.partial(layer_kernel, sp, tp),
        out_shape=jax.ShapeDtypeStruct(resid.shape, bf16),
        in_specs=[
            hbm, hbm, hbm, hbm, smem, vmem, hbm, vmem, hbm, hbm, vmem, vmem, hbm,
        ],
        out_specs=vmem,
        scratch_shapes=[
            pltpu.VMEM((2, length, VD), bf16),
            pltpu.VMEM((maps, 2 * length, VD), bf16),
            pltpu.VMEM((sp, 2, length, VD), bf16),
            pltpu.VMEM((sp, depth, big), bf16),
            pltpu.VMEM((sp, depth, big), bf16),
            pltpu.VMEM((sp, big, down_cols), bf16),
            pltpu.VMEM((maps, 2 * length, LANES), f32),
            pltpu.VMEM((maps, 2 * length, LANES), f32),
            pltpu.VMEM((maps, 2 * length, VD), f32),
            pltpu.VMEM((2, length, VD), bf16),
            pltpu.VMEM((heads, length, VD), bf16),
            pltpu.VMEM((tp, heads * VD, features), bf16),
            pltpu.VMEM((tp, length, features), bf16),
            pltpu.VMEM((tp, 1, features), f32),
            pltpu.VMEM((length, full), f32),
            pltpu.VMEM((length, features), f32),
            pltpu.VMEM((2, rows, full), bf16),
            pltpu.VMEM((2, rows, big), f32),
            pltpu.VMEM((2, length, big), f32),
            pltpu.VMEM((2, length, big), bf16),
            pltpu.VMEM((2 * per, 2, length, down_cols), f32),
            pltpu.VMEM((sp, 2, length, down_cols), bf16),
            pltpu.VMEM((2 * per, 2, length, down_cols), bf16),
            pltpu.VMEM((per, 2, length, down_cols), bf16),
            pltpu.VMEM((per, length, down_cols), bf16),
            dma((12,)),
            dma((5, 4, sp)),
            dma((5, sp)),
            dma((2,)),
            dma((8,)),
            dma((heads,)),
            dma((3,)),
            dma((tp,)),
            dma((5,)),
            dma((tp,)),
            dma((3,)),
            dma((tp,)),
            dma((2,)),
            dma((2,)),
            dma((4,)),
            dma((4,)),
            dma((sp,)),
            dma((2 * per,)),
            dma((per,)),
            dma((per,)),
        ],
        compiler_params=pltpu.CompilerParams(
            has_side_effects=True, vmem_limit_bytes=60 * 1024 * 1024
        ),
    )(*args)


def solution(mesh):
    sp, tp = mesh.shape["sp"], mesh.shape["tp"]

    def run(*args):
        width, (depth, ff) = args[1].shape[1], args[8].shape
        small = args[0].shape[0] <= 512
        pairs = tp == 4 and sp == 2 * tp
        if pairs and small and depth % 256 == 0 and width == 2 * VD and ff % 256 == 128:
            return fused(sp, tp, *args)
        return on_device(*args)

    placed = (
        P("sp", "tp"),
        P("sp", "tp"),
        P("sp", "tp"),
        P("sp", "tp"),
        P("tp"),
        P(),
        P(None, "tp"),
        P("tp"),
        P("sp", "tp"),
        P("sp", "tp"),
        P(None, "tp"),
        P("tp"),
        P("tp", "sp"),
    )
    return jax.shard_map(
        run, mesh=mesh, in_specs=placed, out_specs=P("sp", "tp"), check_vma=False
    )
```

```python
import functools
import math

import jax
import jax.numpy as jnp
from jax import lax
from jax.experimental import pallas as pl
from jax.experimental.pallas import tpu as pltpu
from jax.sharding import PartitionSpec as P

D = 2048
HD = 64
VD = 128


def with_halo(cells, sides, width):
    for axis, dim in sides:
        count = lax.axis_size(axis)
        ends = count - 1
        head = lax.slice_in_dim(cells, 0, width, axis=dim)
        tail = lax.slice_in_dim(cells, cells.shape[dim] - width, cells.shape[dim], axis=dim)
        cells = jnp.concatenate(
            [
                lax.ppermute(tail, axis, [(i, (i + 1) % count) for i in range(ends)]),
                cells,
                lax.ppermute(head, axis, [((i + 1) % count, i) for i in range(ends)]),
            ],
            axis=dim,
        )
    return cells


def on_device(
    resid,
    queries,
    keys,
    values,
    mix_lambda,
    head_gain,
    out_weight,
    norm_gain,
    gate_weight,
    up_weight,
    conv_weight,
    conv_bias,
    down_weight,
):
    length = queries.shape[0]
    heads = mix_lambda.shape[0]
    scale = HD ** (-0.5)
    query_heads = queries.reshape(length, heads, 2, HD)
    initial = (
        jnp.full((heads, 2, length), -1e30, jnp.float32),
        jnp.zeros((heads, 2, length), jnp.float32),
        jnp.zeros((heads, 2, length, VD), jnp.float32),
    )
    key_rows = lax.all_gather(keys, "sp", axis=0, tiled=True)
    value_rows = lax.all_gather(values, "sp", axis=0, tiled=True)
    count = key_rows.shape[0]
    block = math.gcd(count, 2048)
    key_blocks = key_rows.reshape(count // block, block, heads, 2, HD)
    value_blocks = value_rows.reshape(count // block, block, heads, VD)

    def advance(state, blocks):
        running, totals, weighted = state
        key_block, value_block = blocks
        scores = (
            jnp.einsum(
                "qhmd,khmd->hmqk", query_heads, key_block, preferred_element_type=jnp.float32
            )
            * scale
        )
        highest = jnp.maximum(running, jnp.max(scores, axis=-1))
        factor = jnp.exp(running - highest)
        shifted = jnp.exp(scores - highest[..., None])
        totals = totals * factor + jnp.sum(shifted, axis=-1)
        weighted = weighted * factor[..., None] + jnp.einsum(
            "hmqk,khe->hmqe",
            shifted.astype(jnp.bfloat16),
            value_block,
            preferred_element_type=jnp.float32,
        )
        return ((highest, totals, weighted), None)

    result, unused = lax.scan(advance, initial, (key_blocks, value_blocks))
    running, totals, weighted = result
    mapped = weighted / totals[..., None]
    mixed = mapped[:, 0] - mix_lambda[:, None, None] * mapped[:, 1]
    spread = jnp.mean(mixed * mixed, axis=-1, keepdims=True)
    normed = mixed * lax.rsqrt(spread + 1e-06) * head_gain * 0.8
    heads_out = jnp.transpose(normed, (1, 0, 2)).reshape(length, heads * VD).astype(jnp.bfloat16)
    projected = jnp.dot(
        lax.all_gather(heads_out, "tp", axis=1, tiled=True),
        out_weight,
        preferred_element_type=jnp.float32,
    )
    after_mixer = resid.astype(jnp.float32) + projected
    squares = lax.psum(jnp.sum(after_mixer * after_mixer, axis=1), "tp")
    normed_rows = (after_mixer * lax.rsqrt(squares / D + 1e-06)[:, None] * norm_gain).astype(
        jnp.bfloat16
    )
    full_rows = lax.all_gather(normed_rows, "tp", axis=1, tiled=True)
    gate_sum = jnp.dot(
        full_rows,
        lax.all_gather(gate_weight, "sp", axis=0, tiled=True),
        preferred_element_type=jnp.float32,
    )
    upward = jnp.dot(
        full_rows,
        lax.all_gather(up_weight, "sp", axis=0, tiled=True),
        preferred_element_type=jnp.float32,
    )
    gated = gate_sum.astype(jnp.bfloat16)
    padded = with_halo(gated, (("sp", 0),), 1).astype(jnp.float32)
    conv = (
        padded[:-2] * conv_weight[0]
        + padded[1:-1] * conv_weight[1]
        + padded[2:] * conv_weight[2]
        + conv_bias
    )
    hidden = (jax.nn.silu(conv) * upward).astype(jnp.bfloat16)
    partial_terms = jnp.dot(
        hidden,
        lax.all_gather(down_weight, "sp", axis=1, tiled=True),
        preferred_element_type=jnp.float32,
    )
    mixer_out = lax.psum_scatter(
        partial_terms.astype(jnp.bfloat16), "tp", scatter_dimension=1, tiled=True
    ).astype(jnp.float32)
    return (after_mixer + mixer_out).astype(jnp.bfloat16)


EDGE = 16
LANES = 128


def layer_kernel(
    sp,
    tp,
    resid,
    queries,
    keys,
    values,
    mix_lambda,
    head_gain,
    out_weight,
    norm_gain,
    gate_weight,
    up_weight,
    conv_weight,
    conv_bias,
    down_weight,
    out,
    q_all,
    qs,
    kv,
    gates,
    ups,
    downs,
    peaks,
    totals,
    weighted,
    heads_own,
    heads_all,
    out_all,
    resid_all,
    gain_all,
    after,
    after_own,
    rows_all,
    gate_acc,
    up_acc,
    hidden,
    held,
    stage,
    from_core,
    from_x,
    from_z,
    local_sem,
    send_sem,
    recv_sem,
    q_sem,
    head_send,
    head_recv,
    out_send,
    out_recv,
    resid_send,
    resid_recv,
    gain_send,
    gain_recv,
    row_sem,
    after_sem,
    edge_send,
    edge_recv,
    part_send,
    core_recv,
    x_recv,
    z_recv,
):
    bf16, f32 = jnp.bfloat16, jnp.float32
    div, rem = lax.div, lax.rem
    me = lax.axis_index("sp")
    t = lax.axis_index("tp")
    z, y = div(me, 2), rem(me, 2)
    h, q = div(z, 2), rem(z, 2)
    x, c = div(t, 2), rem(t, 2)
    mate = me + 2 - 4 * q
    across = me + 1 - 2 * y
    far = me + 4 - 8 * h
    fmate = far + 2 - 4 * q
    adjacent = me + 2 - 4 * h
    amate = across + 2 - 4 * q
    afar = across + 4 - 8 * h
    afmate = afar + 2 - 4 * q
    inner, outer = h != q, h == q
    sibling = t + 1 - 2 * c
    xdev = t + 2 - 4 * x
    xsib = sibling + 2 - 4 * x

    length = queries.shape[0]
    depth, ff = gate_weight.shape
    features = resid.shape[1]
    big = gates.shape[2]
    small = ff - big
    down_cols = down_weight.shape[1]
    half_sp = sp // 2
    K, V, GATE, UP, DOWN = range(5)
    ACROSS, FAR, MATE, ADJACENT = range(4)

    drains = []

    def both(a, b):
        return b if a is None else jnp.logical_and(a, b)

    def when(cond, body):
        if cond is None:
            body()
        else:
            pl.when(cond)(body)

    def remote(src, dst, send, recv, target):
        return pltpu.make_async_remote_copy(
            src_ref=src,
            dst_ref=dst,
            send_sem=send,
            recv_sem=recv,
            device_id=target,
            device_id_type=pl.DeviceIdType.MESH,
        )

    def ship(make, cond=None):
        when(cond, lambda: make().start())
        drains.append((cond, make))

    def variants(array, part):
        if array in (K, V):
            return ((None, 0),)
        return ((c == part, big), (c != part, small))

    def landing(array, src, size):
        if array in (K, V):
            return kv.at[src, array]
        if array == DOWN:
            return downs.at[src, pl.ds(0, size)]
        return (gates, ups)[array - GATE].at[src, :, pl.ds(0, size)]

    def origin(array, part, size):
        if array in (K, V):
            cols = pl.ds(pl.multiple_of(part * VD, VD), VD)
            return (keys, values)[array].at[:, cols]
        cut = pl.ds(pl.multiple_of(part * (ff - size), LANES), size)
        if array == DOWN:
            return down_weight.at[cut]
        return (gate_weight, up_weight)[array - GATE].at[:, cut]

    def send(array, src, way, target, part=None, cond=None):
        for which, size in variants(array, q if part is None else part):

            def make(size=size):
                here = landing(array, src, size)
                return remote(
                    here if part is None else origin(array, part, size),
                    here,
                    send_sem.at[array, way, src],
                    recv_sem.at[array, src],
                    {"sp": target},
                )

            ship(make, both(cond, which) if which is not None else cond)

    def feed(array, *ways, cond=None):
        other = 1 - q
        for way in ways:
            if way == ACROSS:
                send(array, me, ACROSS, across, part=q)
            elif way == FAR:
                send(array, me, FAR, far, part=q, cond=cond)
            elif way == MATE:
                send(array, me, MATE, mate, part=other)
            else:
                send(array, me, ADJACENT, adjacent, part=other, cond=inner)

    def arrive(array, src):
        for which, size in variants(array, q):

            def wait(size=size):
                here = landing(array, src, size)
                remote(
                    here, here, send_sem.at[array, 0, src], recv_sem.at[array, src], {"sp": across}
                ).wait_recv()

            when(which, wait)

    def pass_on(array, src, *ways):
        arrive(array, src)
        for way in ways:
            if way == FAR:
                send(array, src, FAR, far, cond=inner)
            else:
                send(array, src, ACROSS, across)

    for way in (MATE, ADJACENT, FAR, ACROSS):
        for array in (K, V):
            feed(array, way, cond=inner)

    def q_copy():
        cols = pl.ds(pl.multiple_of((1 - q) * VD, VD), VD)
        return remote(queries.at[:, cols], q_all.at[q], q_sem.at[0], q_sem.at[1], {"sp": mate})

    ship(q_copy)

    local = []

    def fetch(src, dst, cond=None):
        sem = local_sem.at[len(local)]
        make = lambda: pltpu.make_async_copy(src, dst, sem)
        local.append((cond, make))
        when(cond, lambda: make().start())

    def fetched(first, last=None):
        for cond, make in local[first:last]:
            when(cond, lambda: make().wait())

    own_cols = pl.ds(pl.multiple_of(q * VD, VD), VD)
    fetch(queries.at[:, own_cols], q_all.at[q])
    for array in (K, V):
        fetch(origin(array, q, 0), landing(array, me, 0))
    early = len(local)
    for array in (GATE, UP, DOWN):
        for which, size in variants(array, q):
            fetch(origin(array, q, size), landing(array, me, size), which)
    fetch(out_weight, out_all.at[t])
    fetch(resid, resid_all.at[t], c == q)
    fetch(norm_gain, gain_all.at[t])

    def out_copy(src, slot, target, send):
        return lambda: remote(
            src, out_all.at[slot], out_send.at[send], out_recv.at[slot], {"tp": target}
        )

    def gain_copy(target, send):
        return lambda: remote(
            norm_gain, gain_all.at[t], gain_send.at[send], gain_recv.at[t], {"tp": target}
        )

    def resid_copy(src, slot, target, send):
        return lambda: remote(
            src, resid_all.at[slot], resid_send.at[send], resid_recv.at[slot], target
        )

    for i, target in enumerate((sibling, xdev, xsib)):
        ship(gain_copy(target, i))
    ship(out_copy(out_weight, t, xdev, 0))
    ship(resid_copy(resid, t, {"tp": 2 * (1 - x) + q}, 0))
    ship(out_copy(out_weight, t, sibling, 1))
    ship(resid_copy(resid, t, {"tp": sibling}, 1), c != q)

    peaks[...] = jnp.full(peaks.shape, -1e30, f32)
    totals[...] = jnp.zeros(totals.shape, f32)
    weighted[...] = jnp.zeros(weighted.shape, f32)

    @pl.when(c != q)
    def _():
        downs[:, small:, :] = jnp.zeros((sp, big - small, down_cols), bf16)

    fetched(0, early)
    lanes = lax.broadcasted_iota(jnp.int32, (1, VD), 1)

    def spread_queries(block):
        value = q_all[block].astype(f32) * HD**-0.5
        at = pl.ds(pl.multiple_of(block * length, length), length)
        for m in range(2):
            keep = lanes < HD if m == 0 else lanes >= HD
            qs[m, at, :] = jnp.where(keep, value, 0.0).astype(bf16)

    rows = math.gcd(length, 256)

    def attend(src, first=0, last=2 * length // rows):
        def row_block(r, carry):
            at = pl.ds(pl.multiple_of(r * rows, rows), rows)
            key_block = kv[src, K]
            value_block = kv[src, V]
            for m in range(2):
                s = lax.dot_general(
                    qs[m, at, :], key_block, (((1,), (1,)), ((), ())), preferred_element_type=f32
                )
                old = peaks[m, at, :]
                new = jnp.maximum(old, jnp.max(s, axis=1, keepdims=True))
                factor = jnp.exp(old - new)
                p = jnp.exp(s - jnp.concatenate([new] * (length // VD), axis=1))
                peaks[m, at, :] = new
                summed = totals[m, at, :] * factor
                for j in range(length // VD):
                    summed = summed + p[:, j * VD : (j + 1) * VD]
                totals[m, at, :] = summed
                weighted[m, at, :] = weighted[m, at, :] * factor + jnp.dot(
                    p.astype(bf16), value_block, preferred_element_type=f32
                )
            return carry

        lax.fori_loop(first, last, row_block, 0)

    def kv_pass(src, *ways):
        for array in (K, V):
            pass_on(array, src, *ways)

    per_block = length // rows
    spread_queries(q)
    attend(me, q * per_block, (q + 1) * per_block)
    for array in (K, V):
        feed(array, FAR, cond=outer)
    ship(resid_copy(resid, t, {"sp": mate, "tp": 2 * x + q}, 2))
    feed(GATE, ACROSS)
    kv_pass(mate, FAR, ACROSS)
    feed(GATE, ADJACENT, FAR, MATE)
    q_copy().wait_recv()
    spread_queries(1 - q)
    attend(me, (1 - q) * per_block, (2 - q) * per_block)
    attend(mate)
    kv_pass(across)
    attend(across)
    kv_pass(far, ACROSS)
    kv_pass(amate)
    attend(amate)
    kv_pass(fmate, ACROSS)
    feed(UP, ACROSS)
    attend(far)

    def resid_wait(slot):
        resid_copy(resid, slot, {"tp": sibling}, 0)().wait_recv()

    for k in range(2):
        slot = 2 * x + k
        when(c != q, lambda: resid_wait(slot))
        ship(resid_copy(resid_all.at[slot], slot, {"tp": xdev}, 3 + k), c != q)
    out_copy(out_weight, xdev, sibling, 0)().wait_recv()
    ship(out_copy(out_all.at[xdev], xdev, sibling, 2))
    attend(fmate)
    kv_pass(afar)
    attend(afar)
    pass_on(GATE, mate, FAR, ACROSS)
    feed(UP, ADJACENT)
    feed(UP, FAR, cond=inner)
    kv_pass(afmate)
    attend(afmate)

    head = 2 * t + q
    for b in range(2):
        at = slice(b * length, (b + 1) * length)
        first = weighted[0, at, :] / jnp.sum(totals[0, at, :], axis=1, keepdims=True)
        second = weighted[1, at, :] / jnp.sum(totals[1, at, :], axis=1, keepdims=True)
        mixed = first - mix_lambda[q] * second
        spread = jnp.mean(mixed * mixed, axis=1, keepdims=True)
        normed = mixed * lax.rsqrt(spread + 1e-06) * head_gain[...] * 0.8
        heads_own[b] = normed.astype(bf16)

        @pl.when(c == b)
        def _():
            heads_all[head] = heads_own[b]

    def head_copy(src, slot, target, send):
        return lambda: remote(
            src, heads_all.at[slot], head_send.at[send], head_recv.at[slot], target
        )

    for b in range(2):
        ship(head_copy(heads_own.at[b], head, {"sp": mate, "tp": 2 * x + b}, b))
    for b in range(2):
        ship(head_copy(heads_own.at[b], head, {"tp": 2 * (1 - x) + b}, 2 + b))
        ship(head_copy(heads_own.at[b], head, {"tp": sibling}, 4 + b), c != b)

    feed(UP, MATE)
    feed(UP, FAR, cond=outer)

    def head_wait(slot):
        head_copy(heads_all.at[slot], slot, {"tp": sibling}, 0)().wait_recv()

    pass_on(GATE, far, ACROSS)
    for k in range(2):
        slot = 2 * (2 * x + k) + 1 - q
        head_wait(slot)
        ship(head_copy(heads_all.at[slot], slot, {"tp": xdev}, 6 + k))

    fetched(early)

    out_copy(out_weight, sibling, sibling, 0)().wait_recv()
    out_copy(out_weight, xsib, sibling, 0)().wait_recv()
    for slot in (sibling, xdev, xsib):
        remote(
            norm_gain, gain_all.at[slot], gain_send.at[0], gain_recv.at[slot], {"tp": sibling}
        ).wait_recv()
    when(c == q, lambda: resid_wait(sibling))
    for k in range(2):
        resid_wait(2 * (1 - x) + k)
    head_wait(2 * sibling + q)
    for k in range(2):
        head_wait(2 * (2 * (1 - x) + k) + q)
    for k in range(2):
        head_wait(2 * (2 * (1 - x) + k) + 1 - q)

    row_sum = jnp.zeros((length, 1), f32)
    for j in range(tp):
        cols = slice(j * features, (j + 1) * features)
        total = resid_all[j].astype(f32) + jnp.dot(
            jnp.concatenate([heads_all[i] for i in range(heads_all.shape[0])], axis=1),
            out_all[j],
            preferred_element_type=f32,
        )
        after[:, cols] = total
        row_sum = row_sum + jnp.sum(total * total, axis=1, keepdims=True)
    inverse = lax.rsqrt(row_sum / D + 1e-06)
    for j in range(tp):
        cols = slice(j * features, (j + 1) * features)
        rows_all[c, EDGE : EDGE + length, cols] = (
            after[:, cols] * inverse * gain_all[j]
        ).astype(bf16)

    def row_copy(block):
        here = rows_all.at[block, pl.ds(EDGE, length)]
        return remote(here, here, row_sem.at[0], row_sem.at[1], {"tp": sibling})

    ship(lambda: row_copy(c))

    def own_features(device):
        return pl.ds(pl.multiple_of(device * features, features), features)

    def after_copy():
        return remote(
            after.at[:, own_features(sibling)],
            after_own,
            after_sem.at[0],
            after_sem.at[1],
            {"tp": sibling},
        )

    ship(after_copy, c == q)

    @pl.when(c == q)
    def _():
        after_own[...] = after[:, own_features(t)]

    pass_on(GATE, fmate, ACROSS)
    pass_on(UP, mate, FAR, ACROSS)
    feed(DOWN, ADJACENT, FAR, MATE)
    row_copy(1 - c).wait_recv()

    begin, end, top, bottom = EDGE, length, 0, EDGE + length

    def edge_copy(i, source_block, source, block, dest, target):
        def rows_at(start):
            return pl.ds(pl.multiple_of(start, EDGE), EDGE)

        return remote(
            rows_all.at[source_block, rows_at(source)],
            rows_all.at[block, rows_at(dest)],
            edge_send.at[i],
            edge_recv.at[i],
            {"sp": target},
        )

    def pick(first, second):
        return first + y * (second - first)

    def edge(i):
        return (
            lambda: edge_copy(0, 0, pick(end, begin), 0, pick(top, bottom), across),
            lambda: edge_copy(
                1, pick(1, 0), pick(begin, end), pick(0, 1), pick(bottom, top), across
            ),
            lambda: edge_copy(2, 1, pick(end, begin), 1, pick(top, bottom), across),
        )[i]

    for i in range(3):
        ship(edge(i))
    before = jnp.logical_and(y == 1, h == 0)
    behind = jnp.logical_and(y == 0, h == 1)
    onward = lambda: edge_copy(3, 1, end, 0, top, jnp.minimum(me + half_sp - 1, sp - 1))
    back = lambda: edge_copy(3, 0, begin, 1, bottom, jnp.maximum(me - half_sp + 1, 0))
    ship(onward, before)
    ship(back, behind)

    @pl.when(jnp.logical_and(y == 0, h == 0))
    def _():
        rows_all[0, 0:EDGE, :] = jnp.zeros((EDGE, rows_all.shape[2]), bf16)

    @pl.when(jnp.logical_and(y == 1, h == 1))
    def _():
        rows_all[1, EDGE + length :, :] = jnp.zeros((EDGE, rows_all.shape[2]), bf16)

    arrive(GATE, across)
    arrive(GATE, amate)

    span = half_sp * depth
    wide = 2 * LANES

    def expand(acc, weight, half, fresh):
        offset = EDGE if acc is gate_acc else 0
        held_rows = pl.ds(offset, length)
        deep = pl.ds(pl.multiple_of(half * span, span), span)
        blocks = pl.ds(half * half_sp, half_sp)

        def tile(i, carry):
            b, cols = rem(i, 2), pl.ds(pl.multiple_of(div(i, 2) * wide, wide), wide)
            part = jnp.dot(
                rows_all[b, EDGE : EDGE + length, deep],
                weight[blocks, :, cols].reshape(span, wide),
                preferred_element_type=f32,
            )
            if fresh:
                acc[b, held_rows, cols] = part
            else:
                acc[b, held_rows, cols] += part
            return carry

        lax.fori_loop(0, 2 * (big // wide), tile, 0)

    expand(gate_acc, gates, h, True)
    arrive(GATE, afar)
    arrive(GATE, afmate)
    expand(gate_acc, gates, 1 - h, False)
    pass_on(UP, far, ACROSS)
    arrive(UP, across)
    arrive(UP, amate)
    expand(up_acc, ups, h, True)
    pass_on(DOWN, mate, FAR)
    pass_on(UP, fmate, ACROSS)
    feed(DOWN, ACROSS)
    send(DOWN, mate, ACROSS, across)
    for i in range(3):
        edge(i)().wait_recv()
    when(before, lambda: onward().wait_recv())
    when(behind, lambda: back().wait_recv())

    def halo(i, carry):
        cols = pl.ds(pl.multiple_of(i * wide, wide), wide)
        sides = (slice(0, EDGE), slice(EDGE + length, length + 2 * EDGE))
        part = jnp.dot(
            jnp.concatenate([rows_all[b, side, :] for b in range(2) for side in sides], axis=0),
            gates[:, :, cols].reshape(sp * depth, wide),
            preferred_element_type=f32,
        )
        for k in range(4):
            gate_acc[k // 2, sides[k % 2], cols] = part[k * EDGE : (k + 1) * EDGE]
        return carry

    lax.fori_loop(0, big // wide, halo, 0)
    arrive(UP, afar)
    arrive(UP, afmate)
    expand(up_acc, ups, 1 - h, False)

    base = jnp.where(c == q, q * (ff - big), q * (ff - small))

    def activate(b, carry):
        for j in range(big // LANES):
            cols = slice(j * LANES, (j + 1) * LANES)
            spot = jnp.minimum(base + j * LANES, ff - LANES)
            taps = pl.ds(pl.multiple_of(spot, LANES), LANES)

            def fill():
                def tap(start):
                    return gate_acc[b, start : start + length, cols].astype(bf16).astype(f32)

                conv = (
                    tap(EDGE - 1) * conv_weight[0:1, taps]
                    + tap(EDGE) * conv_weight[1:2, taps]
                    + tap(EDGE + 1) * conv_weight[2:3, taps]
                    + conv_bias[:, taps]
                )
                hidden[b, :, cols] = (conv / (1.0 + jnp.exp(-conv)) * up_acc[b, :, cols]).astype(
                    bf16
                )

            if (j + 1) * LANES <= small:
                fill()
            else:
                pl.when(c == q)(fill)

                @pl.when(c != q)
                def _():
                    hidden[b, :, cols] = jnp.zeros((length, LANES), bf16)

        return carry

    lax.fori_loop(0, 2, activate, 0)

    per = sp // tp

    def owner(s):
        o = div(s, per)
        return div(o, 2), rem(o, 2)

    def core_slot(s):
        return div(s, half_sp) * per + rem(s, per)

    def core_copy(s):
        return remote(
            stage.at[s], from_core.at[core_slot(s)], part_send.at[0, s],
            core_recv.at[core_slot(s)], {"tp": sibling},
        )

    def z_copy(s):
        return remote(
            stage.at[s, 0], from_z.at[core_slot(s)], part_send.at[0, s],
            z_recv.at[core_slot(s)], {"sp": mate},
        )

    def x_copy(s):
        return remote(
            stage.at[s, 1], from_x.at[rem(s, per)], part_send.at[1, s], x_recv.at[rem(s, per)],
            {"tp": xdev},
        )

    def multiply(s):
        ox, oc = owner(s)
        product = jnp.dot(
            hidden[...].reshape(2 * length, big), downs[s], preferred_element_type=f32
        ).reshape(2, length, down_cols)

        @pl.when(c != oc)
        def _():
            stage[s] = product.astype(bf16)

        @pl.when(c == oc)
        def _():
            held[core_slot(s)] = product

        ship(lambda: core_copy(s), c != oc)

    def add_core(s):
        ox, oc = owner(s)
        mine = c == oc
        slot = core_slot(s)

        @pl.when(mine)
        def _():
            core_copy(s).wait_recv()
            stage[s, 0] = (held[slot, 1 - q] + from_core[slot, 1 - q].astype(f32)).astype(bf16)

        ship(lambda: z_copy(s), mine)

    def out_cols(s):
        return pl.ds(pl.multiple_of(rem(s, per) * down_cols, down_cols), down_cols)

    def add_z(s):
        ox, oc = owner(s)
        mine = c == oc
        slot = core_slot(s)

        def summed():
            return (
                held[slot, q] + from_core[slot, q].astype(f32) + from_z[slot].astype(f32)
            )

        when(mine, lambda: z_copy(s).wait_recv())

        @pl.when(jnp.logical_and(mine, x == ox))
        def _():
            after_own[:, out_cols(s)] += summed()

        @pl.when(jnp.logical_and(mine, x != ox))
        def _():
            stage[s, 1] = summed().astype(bf16)

        ship(lambda: x_copy(s), jnp.logical_and(mine, x != ox))

    multiply(me)
    multiply(mate)
    add_core(me)
    pass_on(DOWN, far, ACROSS)
    arrive(DOWN, across)
    multiply(across)
    add_core(mate)
    arrive(DOWN, amate)
    multiply(amate)
    add_core(across)
    pass_on(DOWN, fmate, ACROSS)
    multiply(far)
    add_core(amate)
    multiply(fmate)
    add_core(far)
    when(c != q, lambda: after_copy().wait_recv())
    add_z(me)
    add_z(mate)
    arrive(DOWN, afar)
    multiply(afar)
    add_core(fmate)
    add_z(across)
    add_z(amate)
    arrive(DOWN, afmate)
    multiply(afmate)
    add_core(afar)
    add_core(afmate)
    for s in (far, fmate, afar, afmate):
        add_z(s)
    for k in range(per):
        cols = slice(k * down_cols, (k + 1) * down_cols)
        x_copy(k).wait_recv()
        out[:, cols] = (after_own[:, cols] + from_x[k].astype(f32)).astype(bf16)

    for cond, make in drains:
        when(cond, lambda: make().wait_send())


def fused(sp, tp, *args):
    resid, queries, keys, values = args[:4]
    gate_weight, down_weight = args[8], args[12]
    length, width = queries.shape
    features = resid.shape[1]
    depth, ff = gate_weight.shape
    maps = 2
    heads = tp * (width // VD)
    full = tp * features
    bf16, f32 = jnp.bfloat16, jnp.float32
    dma = pltpu.SemaphoreType.DMA
    vmem = pl.BlockSpec(memory_space=pltpu.VMEM)
    smem = pl.BlockSpec(memory_space=pltpu.SMEM)
    hbm = pl.BlockSpec(memory_space=pl.ANY)
    rows = length + 2 * EDGE
    down_cols = down_weight.shape[1]
    tiles = ff // LANES
    big = (tiles - tiles // 2) * LANES
    per = sp // tp
    args = list(args)
    for i in (5, 7, 11):
        args[i] = args[i].reshape(1, -1)
    return pl.pallas_call(
        functools.partial(layer_kernel, sp, tp),
        out_shape=jax.ShapeDtypeStruct(resid.shape, bf16),
        in_specs=[
            hbm, hbm, hbm, hbm, smem, vmem, hbm, vmem, hbm, hbm, vmem, vmem, hbm,
        ],
        out_specs=vmem,
        scratch_shapes=[
            pltpu.VMEM((2, length, VD), bf16),
            pltpu.VMEM((maps, 2 * length, VD), bf16),
            pltpu.VMEM((sp, 2, length, VD), bf16),
            pltpu.VMEM((sp, depth, big), bf16),
            pltpu.VMEM((sp, depth, big), bf16),
            pltpu.VMEM((sp, big, down_cols), bf16),
            pltpu.VMEM((maps, 2 * length, LANES), f32),
            pltpu.VMEM((maps, 2 * length, LANES), f32),
            pltpu.VMEM((maps, 2 * length, VD), f32),
            pltpu.VMEM((2, length, VD), bf16),
            pltpu.VMEM((heads, length, VD), bf16),
            pltpu.VMEM((tp, heads * VD, features), bf16),
            pltpu.VMEM((tp, length, features), bf16),
            pltpu.VMEM((tp, 1, features), f32),
            pltpu.VMEM((length, full), f32),
            pltpu.VMEM((length, features), f32),
            pltpu.VMEM((2, rows, full), bf16),
            pltpu.VMEM((2, rows, big), f32),
            pltpu.VMEM((2, length, big), f32),
            pltpu.VMEM((2, length, big), bf16),
            pltpu.VMEM((2 * per, 2, length, down_cols), f32),
            pltpu.VMEM((sp, 2, length, down_cols), bf16),
            pltpu.VMEM((2 * per, 2, length, down_cols), bf16),
            pltpu.VMEM((per, length, down_cols), bf16),
            pltpu.VMEM((2 * per, length, down_cols), bf16),
            dma((12,)),
            dma((5, 4, sp)),
            dma((5, sp)),
            dma((2,)),
            dma((8,)),
            dma((heads,)),
            dma((3,)),
            dma((tp,)),
            dma((5,)),
            dma((tp,)),
            dma((3,)),
            dma((tp,)),
            dma((2,)),
            dma((2,)),
            dma((4,)),
            dma((4,)),
            dma((2, sp)),
            dma((2 * per,)),
            dma((per,)),
            dma((2 * per,)),
        ],
        compiler_params=pltpu.CompilerParams(
            has_side_effects=True, vmem_limit_bytes=60 * 1024 * 1024
        ),
    )(*args)


def solution(mesh):
    sp, tp = mesh.shape["sp"], mesh.shape["tp"]

    def run(*args):
        width, (depth, ff) = args[1].shape[1], args[8].shape
        small = args[0].shape[0] <= 512
        pairs = tp == 4 and sp == 2 * tp
        if pairs and small and depth % 256 == 0 and width == 2 * VD and ff % 256 == 128:
            return fused(sp, tp, *args)
        return on_device(*args)

    placed = (
        P("sp", "tp"),
        P("sp", "tp"),
        P("sp", "tp"),
        P("sp", "tp"),
        P("tp"),
        P(),
        P(None, "tp"),
        P("tp"),
        P("sp", "tp"),
        P("sp", "tp"),
        P(None, "tp"),
        P("tp"),
        P("tp", "sp"),
    )
    return jax.shard_map(
        run, mesh=mesh, in_specs=placed, out_specs=P("sp", "tp"), check_vma=False
    )
```

```python
import functools
import math

import jax
import jax.numpy as jnp
from jax import lax
from jax.experimental import pallas as pl
from jax.experimental.pallas import tpu as pltpu
from jax.sharding import PartitionSpec as P

D = 2048
HD = 64
VD = 128


def with_halo(cells, sides, width):
    for axis, dim in sides:
        count = lax.axis_size(axis)
        ends = count - 1
        head = lax.slice_in_dim(cells, 0, width, axis=dim)
        tail = lax.slice_in_dim(cells, cells.shape[dim] - width, cells.shape[dim], axis=dim)
        cells = jnp.concatenate(
            [
                lax.ppermute(tail, axis, [(i, (i + 1) % count) for i in range(ends)]),
                cells,
                lax.ppermute(head, axis, [((i + 1) % count, i) for i in range(ends)]),
            ],
            axis=dim,
        )
    return cells


def on_device(
    resid,
    queries,
    keys,
    values,
    mix_lambda,
    head_gain,
    out_weight,
    norm_gain,
    gate_weight,
    up_weight,
    conv_weight,
    conv_bias,
    down_weight,
):
    length = queries.shape[0]
    heads = mix_lambda.shape[0]
    scale = HD ** (-0.5)
    query_heads = queries.reshape(length, heads, 2, HD)
    initial = (
        jnp.full((heads, 2, length), -1e30, jnp.float32),
        jnp.zeros((heads, 2, length), jnp.float32),
        jnp.zeros((heads, 2, length, VD), jnp.float32),
    )
    key_rows = lax.all_gather(keys, "sp", axis=0, tiled=True)
    value_rows = lax.all_gather(values, "sp", axis=0, tiled=True)
    count = key_rows.shape[0]
    block = math.gcd(count, 2048)
    key_blocks = key_rows.reshape(count // block, block, heads, 2, HD)
    value_blocks = value_rows.reshape(count // block, block, heads, VD)

    def advance(state, blocks):
        running, totals, weighted = state
        key_block, value_block = blocks
        scores = (
            jnp.einsum(
                "qhmd,khmd->hmqk", query_heads, key_block, preferred_element_type=jnp.float32
            )
            * scale
        )
        highest = jnp.maximum(running, jnp.max(scores, axis=-1))
        factor = jnp.exp(running - highest)
        shifted = jnp.exp(scores - highest[..., None])
        totals = totals * factor + jnp.sum(shifted, axis=-1)
        weighted = weighted * factor[..., None] + jnp.einsum(
            "hmqk,khe->hmqe",
            shifted.astype(jnp.bfloat16),
            value_block,
            preferred_element_type=jnp.float32,
        )
        return ((highest, totals, weighted), None)

    result, unused = lax.scan(advance, initial, (key_blocks, value_blocks))
    running, totals, weighted = result
    mapped = weighted / totals[..., None]
    mixed = mapped[:, 0] - mix_lambda[:, None, None] * mapped[:, 1]
    spread = jnp.mean(mixed * mixed, axis=-1, keepdims=True)
    normed = mixed * lax.rsqrt(spread + 1e-06) * head_gain * 0.8
    heads_out = jnp.transpose(normed, (1, 0, 2)).reshape(length, heads * VD).astype(jnp.bfloat16)
    projected = jnp.dot(
        lax.all_gather(heads_out, "tp", axis=1, tiled=True),
        out_weight,
        preferred_element_type=jnp.float32,
    )
    after_mixer = resid.astype(jnp.float32) + projected
    squares = lax.psum(jnp.sum(after_mixer * after_mixer, axis=1), "tp")
    normed_rows = (after_mixer * lax.rsqrt(squares / D + 1e-06)[:, None] * norm_gain).astype(
        jnp.bfloat16
    )
    full_rows = lax.all_gather(normed_rows, "tp", axis=1, tiled=True)
    gate_sum = jnp.dot(
        full_rows,
        lax.all_gather(gate_weight, "sp", axis=0, tiled=True),
        preferred_element_type=jnp.float32,
    )
    upward = jnp.dot(
        full_rows,
        lax.all_gather(up_weight, "sp", axis=0, tiled=True),
        preferred_element_type=jnp.float32,
    )
    gated = gate_sum.astype(jnp.bfloat16)
    padded = with_halo(gated, (("sp", 0),), 1).astype(jnp.float32)
    conv = (
        padded[:-2] * conv_weight[0]
        + padded[1:-1] * conv_weight[1]
        + padded[2:] * conv_weight[2]
        + conv_bias
    )
    hidden = (jax.nn.silu(conv) * upward).astype(jnp.bfloat16)
    partial_terms = jnp.dot(
        hidden,
        lax.all_gather(down_weight, "sp", axis=1, tiled=True),
        preferred_element_type=jnp.float32,
    )
    mixer_out = lax.psum_scatter(
        partial_terms.astype(jnp.bfloat16), "tp", scatter_dimension=1, tiled=True
    ).astype(jnp.float32)
    return (after_mixer + mixer_out).astype(jnp.bfloat16)


EDGE = 16
LANES = 128


def layer_kernel(
    sp,
    tp,
    resid,
    queries,
    keys,
    values,
    mix_lambda,
    head_gain,
    out_weight,
    norm_gain,
    gate_weight,
    up_weight,
    conv_weight,
    conv_bias,
    down_weight,
    out,
    q_all,
    qs,
    kv,
    gates,
    ups,
    downs,
    peaks,
    totals,
    weighted,
    heads_own,
    heads_all,
    out_all,
    resid_all,
    gain_all,
    after,
    after_own,
    rows_all,
    gate_acc,
    up_acc,
    hidden,
    held,
    stage,
    from_core,
    from_x,
    from_z,
    local_sem,
    send_sem,
    recv_sem,
    q_sem,
    head_send,
    head_recv,
    out_send,
    out_recv,
    resid_send,
    resid_recv,
    gain_send,
    gain_recv,
    row_sem,
    after_sem,
    edge_send,
    edge_recv,
    part_send,
    core_recv,
    x_recv,
    z_recv,
):
    bf16, f32 = jnp.bfloat16, jnp.float32
    div, rem = lax.div, lax.rem
    me = lax.axis_index("sp")
    t = lax.axis_index("tp")
    z, y = div(me, 2), rem(me, 2)
    h, q = div(z, 2), rem(z, 2)
    x, c = div(t, 2), rem(t, 2)
    mate = me + 2 - 4 * q
    across = me + 1 - 2 * y
    far = me + 4 - 8 * h
    fmate = far + 2 - 4 * q
    adjacent = me + 2 - 4 * h
    amate = across + 2 - 4 * q
    afar = across + 4 - 8 * h
    afmate = afar + 2 - 4 * q
    inner, outer = h != q, h == q
    sibling = t + 1 - 2 * c
    xdev = t + 2 - 4 * x
    xsib = sibling + 2 - 4 * x

    length = queries.shape[0]
    depth, ff = gate_weight.shape
    features = resid.shape[1]
    big = gates.shape[2]
    small = ff - big
    down_cols = down_weight.shape[1]
    half_sp = sp // 2
    K, V, GATE, UP, DOWN = range(5)
    ACROSS, FAR, MATE, ADJACENT = range(4)

    drains = []

    def both(a, b):
        return b if a is None else jnp.logical_and(a, b)

    def when(cond, body):
        if cond is None:
            body()
        else:
            pl.when(cond)(body)

    def remote(src, dst, send, recv, target):
        return pltpu.make_async_remote_copy(
            src_ref=src,
            dst_ref=dst,
            send_sem=send,
            recv_sem=recv,
            device_id=target,
            device_id_type=pl.DeviceIdType.MESH,
        )

    def ship(make, cond=None):
        when(cond, lambda: make().start())
        drains.append((cond, make))

    def variants(array, part):
        if array in (K, V):
            return ((None, 0),)
        return ((c == part, big), (c != part, small))

    def landing(array, src, size):
        if array in (K, V):
            return kv.at[src, array]
        if array == DOWN:
            return downs.at[src, pl.ds(0, size)]
        return (gates, ups)[array - GATE].at[src, :, pl.ds(0, size)]

    def origin(array, part, size):
        if array in (K, V):
            cols = pl.ds(pl.multiple_of(part * VD, VD), VD)
            return (keys, values)[array].at[:, cols]
        cut = pl.ds(pl.multiple_of(part * (ff - size), LANES), size)
        if array == DOWN:
            return down_weight.at[cut]
        return (gate_weight, up_weight)[array - GATE].at[:, cut]

    def send(array, src, way, target, part=None, cond=None):
        for which, size in variants(array, q if part is None else part):

            def make(size=size):
                here = landing(array, src, size)
                return remote(
                    here if part is None else origin(array, part, size),
                    here,
                    send_sem.at[array, way, src],
                    recv_sem.at[array, src],
                    {"sp": target},
                )

            ship(make, both(cond, which) if which is not None else cond)

    def feed(array, *ways, cond=None):
        other = 1 - q
        for way in ways:
            if way == ACROSS:
                send(array, me, ACROSS, across, part=q)
            elif way == FAR:
                send(array, me, FAR, far, part=q, cond=cond)
            elif way == MATE:
                send(array, me, MATE, mate, part=other, cond=cond)
            else:
                send(array, me, ADJACENT, adjacent, part=other, cond=inner)

    def arrive(array, src, cond=None):
        for which, size in variants(array, q):

            def wait(size=size):
                here = landing(array, src, size)
                remote(
                    here, here, send_sem.at[array, 0, src], recv_sem.at[array, src], {"sp": across}
                ).wait_recv()

            when(both(cond, which) if which is not None else cond, wait)

    def pass_on(array, src, *ways, cond=None):
        arrive(array, src, cond)
        for way in ways:
            if way == FAR:
                send(array, src, FAR, far, cond=inner)
            else:
                send(array, src, ACROSS, across, cond=cond)

    before = jnp.logical_and(y == 1, h == 0)
    behind = jnp.logical_and(y == 0, h == 1)
    later = jnp.minimum(me + half_sp - 1, sp - 1)
    earlier = jnp.maximum(me - half_sp + 1, 0)
    barrier = pltpu.get_barrier_semaphore()

    def greet(target, cond=None):
        when(
            cond,
            lambda: pl.semaphore_signal(
                barrier, inc=1, device_id=target, device_id_type=pl.DeviceIdType.MESH
            ),
        )

    for target in (
        {"sp": far},
        {"sp": mate},
        {"sp": mate, "tp": sibling},
        {"sp": across},
        {"tp": xdev},
        {"tp": xsib},
        {"tp": sibling},
    ):
        greet(target)
    greet({"sp": adjacent}, inner)
    greet({"sp": later}, before)
    greet({"sp": earlier}, behind)
    pl.semaphore_wait(
        barrier,
        7 + jnp.where(inner, 1, 0) + jnp.where(jnp.logical_or(before, behind), 1, 0),
    )

    for way in (MATE, ADJACENT, ACROSS):
        for array in (K, V):
            feed(array, way)

    def q_copy():
        cols = pl.ds(pl.multiple_of((1 - q) * VD, VD), VD)
        return remote(queries.at[:, cols], q_all.at[q], q_sem.at[0], q_sem.at[1], {"sp": mate})

    local = []

    def fetch(src, dst, cond=None):
        sem = local_sem.at[len(local)]
        make = lambda: pltpu.make_async_copy(src, dst, sem)
        local.append((cond, make))
        when(cond, lambda: make().start())

    def fetched(first, last=None):
        for cond, make in local[first:last]:
            when(cond, lambda: make().wait())

    own_cols = pl.ds(pl.multiple_of(q * VD, VD), VD)
    fetch(queries.at[:, own_cols], q_all.at[q])
    for array in (K, V):
        fetch(origin(array, q, 0), landing(array, me, 0))
    early = len(local)
    for array in (GATE, UP, DOWN):
        for which, size in variants(array, q):
            fetch(origin(array, q, size), landing(array, me, size), which)
    fetch(out_weight, out_all.at[t])
    fetch(resid, resid_all.at[t], c == q)
    fetch(norm_gain, gain_all.at[t])

    def out_copy(src, slot, target, send):
        return lambda: remote(
            src, out_all.at[slot], out_send.at[send], out_recv.at[slot], {"tp": target}
        )

    def gain_copy(target, send):
        return lambda: remote(
            norm_gain, gain_all.at[t], gain_send.at[send], gain_recv.at[t], {"tp": target}
        )

    def resid_copy(src, slot, target, send):
        return lambda: remote(
            src, resid_all.at[slot], resid_send.at[send], resid_recv.at[slot], target
        )

    for i, target in enumerate((sibling, xdev, xsib)):
        ship(gain_copy(target, i))
    ship(out_copy(out_weight, t, xdev, 0))
    ship(resid_copy(resid, t, {"tp": 2 * (1 - x) + q}, 0))
    ship(out_copy(out_weight, t, sibling, 1))
    ship(resid_copy(resid, t, {"tp": sibling}, 1), c != q)

    peaks[...] = jnp.full(peaks.shape, -1e30, f32)
    totals[...] = jnp.zeros(totals.shape, f32)
    weighted[...] = jnp.zeros(weighted.shape, f32)

    @pl.when(c != q)
    def _():
        downs[:, small:, :] = jnp.zeros((sp, big - small, down_cols), bf16)

    fetched(0, early)
    lanes = lax.broadcasted_iota(jnp.int32, (1, VD), 1)

    def spread_queries(block):
        value = q_all[block].astype(f32) * HD**-0.5
        at = pl.ds(pl.multiple_of(block * length, length), length)
        for m in range(2):
            keep = lanes < HD if m == 0 else lanes >= HD
            qs[m, at, :] = jnp.where(keep, value, 0.0).astype(bf16)

    rows = math.gcd(length, 256)

    def attend(src, first=0, last=2 * length // rows):
        def row_block(r, carry):
            at = pl.ds(pl.multiple_of(r * rows, rows), rows)
            key_block = kv[src, K]
            value_block = kv[src, V]
            for m in range(2):
                s = lax.dot_general(
                    qs[m, at, :], key_block, (((1,), (1,)), ((), ())), preferred_element_type=f32
                )
                old = peaks[m, at, :]
                new = jnp.maximum(old, jnp.max(s, axis=1, keepdims=True))
                factor = jnp.exp(old - new)
                p = jnp.exp(s - jnp.concatenate([new] * (length // VD), axis=1))
                peaks[m, at, :] = new
                summed = totals[m, at, :] * factor
                for j in range(length // VD):
                    summed = summed + p[:, j * VD : (j + 1) * VD]
                totals[m, at, :] = summed
                weighted[m, at, :] = weighted[m, at, :] * factor + jnp.dot(
                    p.astype(bf16), value_block, preferred_element_type=f32
                )
            return carry

        lax.fori_loop(first, last, row_block, 0)

    def kv_pass(src, *ways):
        for array in (K, V):
            pass_on(array, src, *ways)

    per_block = length // rows
    spread_queries(q)
    attend(me, q * per_block, (q + 1) * per_block)
    for array in (K, V):
        feed(array, FAR)
    ship(q_copy)
    ship(resid_copy(resid, t, {"sp": mate, "tp": 2 * x + q}, 2))
    feed(GATE, ACROSS)
    kv_pass(mate, FAR, ACROSS)
    feed(GATE, ADJACENT, FAR, MATE)
    attend(mate, q * per_block, (q + 1) * per_block)
    kv_pass(across)
    attend(across, q * per_block, (q + 1) * per_block)
    q_copy().wait_recv()
    spread_queries(1 - q)
    for src in (me, mate, across):
        attend(src, (1 - q) * per_block, (2 - q) * per_block)
    kv_pass(far, ACROSS)
    kv_pass(amate)
    attend(amate)
    kv_pass(fmate, ACROSS)
    feed(UP, ACROSS)
    feed(DOWN, ACROSS)
    attend(far)

    def resid_wait(slot):
        resid_copy(resid, slot, {"tp": sibling}, 0)().wait_recv()

    for k in range(2):
        slot = 2 * x + k
        when(c != q, lambda: resid_wait(slot))
        ship(resid_copy(resid_all.at[slot], slot, {"tp": xdev}, 3 + k), c != q)
    out_copy(out_weight, xdev, sibling, 0)().wait_recv()
    ship(out_copy(out_all.at[xdev], xdev, sibling, 2))
    attend(fmate)
    kv_pass(afar)
    attend(afar)
    pass_on(GATE, mate, FAR, ACROSS, cond=inner)
    feed(UP, ADJACENT)
    feed(UP, FAR, cond=inner)
    kv_pass(afmate)
    attend(afmate)

    head = 2 * t + q
    for b in range(2):
        at = slice(b * length, (b + 1) * length)
        first = weighted[0, at, :] / jnp.sum(totals[0, at, :], axis=1, keepdims=True)
        second = weighted[1, at, :] / jnp.sum(totals[1, at, :], axis=1, keepdims=True)
        mixed = first - mix_lambda[q] * second
        spread = jnp.mean(mixed * mixed, axis=1, keepdims=True)
        normed = mixed * lax.rsqrt(spread + 1e-06) * head_gain[...] * 0.8
        heads_own[b] = normed.astype(bf16)

        @pl.when(c == b)
        def _():
            heads_all[head] = heads_own[b]

    def head_copy(src, slot, target, send):
        return lambda: remote(
            src, heads_all.at[slot], head_send.at[send], head_recv.at[slot], target
        )

    for b in range(2):
        ship(head_copy(heads_own.at[b], head, {"sp": mate, "tp": 2 * x + b}, b))
    for b in range(2):
        ship(head_copy(heads_own.at[b], head, {"tp": 2 * (1 - x) + b}, 2 + b))
        ship(head_copy(heads_own.at[b], head, {"tp": sibling}, 4 + b), c != b)

    feed(UP, MATE)
    feed(UP, FAR, cond=outer)

    def head_wait(slot):
        head_copy(heads_all.at[slot], slot, {"tp": sibling}, 0)().wait_recv()

    pass_on(GATE, far, ACROSS, cond=inner)
    pass_on(GATE, mate, ACROSS, cond=outer)
    pass_on(GATE, far, ACROSS, cond=outer)
    for k in range(2):
        slot = 2 * (2 * x + k) + 1 - q
        head_wait(slot)
        ship(head_copy(heads_all.at[slot], slot, {"tp": xdev}, 6 + k))

    fetched(early)

    out_copy(out_weight, sibling, sibling, 0)().wait_recv()
    out_copy(out_weight, xsib, sibling, 0)().wait_recv()
    for slot in (sibling, xdev, xsib):
        remote(
            norm_gain, gain_all.at[slot], gain_send.at[0], gain_recv.at[slot], {"tp": sibling}
        ).wait_recv()
    when(c == q, lambda: resid_wait(sibling))
    for k in range(2):
        resid_wait(2 * (1 - x) + k)
    head_wait(2 * sibling + q)
    for k in range(2):
        head_wait(2 * (2 * (1 - x) + k) + q)
    for k in range(2):
        head_wait(2 * (2 * (1 - x) + k) + 1 - q)

    pass_on(GATE, fmate, ACROSS)
    row_sum = jnp.zeros((length, 1), f32)
    for j in range(tp):
        cols = slice(j * features, (j + 1) * features)
        total = resid_all[j].astype(f32) + jnp.dot(
            jnp.concatenate([heads_all[i] for i in range(heads_all.shape[0])], axis=1),
            out_all[j],
            preferred_element_type=f32,
        )
        after[:, cols] = total
        row_sum = row_sum + jnp.sum(total * total, axis=1, keepdims=True)
    inverse = lax.rsqrt(row_sum / D + 1e-06)
    for j in range(tp):
        cols = slice(j * features, (j + 1) * features)
        rows_all[c, EDGE : EDGE + length, cols] = (
            after[:, cols] * inverse * gain_all[j]
        ).astype(bf16)

    def row_copy(block):
        here = rows_all.at[block, pl.ds(EDGE, length)]
        return remote(here, here, row_sem.at[0], row_sem.at[1], {"tp": sibling})

    ship(lambda: row_copy(c))

    def own_features(device):
        return pl.ds(pl.multiple_of(device * features, features), features)

    def after_copy():
        return remote(
            after.at[:, own_features(sibling)],
            after_own,
            after_sem.at[0],
            after_sem.at[1],
            {"tp": sibling},
        )

    ship(after_copy, c == q)

    @pl.when(c == q)
    def _():
        after_own[...] = after[:, own_features(t)]

    pass_on(UP, mate, FAR, ACROSS, cond=inner)
    row_copy(1 - c).wait_recv()

    begin, end, top, bottom = EDGE, length, 0, EDGE + length

    def edge_copy(i, source_block, source, block, dest, target):
        def rows_at(start):
            return pl.ds(pl.multiple_of(start, EDGE), EDGE)

        return remote(
            rows_all.at[source_block, rows_at(source)],
            rows_all.at[block, rows_at(dest)],
            edge_send.at[i],
            edge_recv.at[i],
            {"sp": target},
        )

    def pick(first, second):
        return first + y * (second - first)

    def edge(i):
        return (
            lambda: edge_copy(0, 0, pick(end, begin), 0, pick(top, bottom), across),
            lambda: edge_copy(
                1, pick(1, 0), pick(begin, end), pick(0, 1), pick(bottom, top), across
            ),
            lambda: edge_copy(2, 1, pick(end, begin), 1, pick(top, bottom), across),
        )[i]

    for i in range(3):
        ship(edge(i))
    onward = lambda: edge_copy(3, 1, end, 0, top, later)
    back = lambda: edge_copy(3, 0, begin, 1, bottom, earlier)
    ship(onward, before)
    ship(back, behind)
    feed(DOWN, ADJACENT, FAR, MATE)

    @pl.when(jnp.logical_and(y == 0, h == 0))
    def _():
        rows_all[0, 0:EDGE, :] = jnp.zeros((EDGE, rows_all.shape[2]), bf16)

    @pl.when(jnp.logical_and(y == 1, h == 1))
    def _():
        rows_all[1, EDGE + length :, :] = jnp.zeros((EDGE, rows_all.shape[2]), bf16)

    arrive(GATE, across)
    arrive(GATE, amate)

    span = half_sp * depth
    wide = 2 * LANES

    def expand(acc, weight, half, fresh):
        offset = EDGE if acc is gate_acc else 0
        held_rows = pl.ds(offset, length)
        deep = pl.ds(pl.multiple_of(half * span, span), span)
        blocks = pl.ds(half * half_sp, half_sp)

        def tile(i, carry):
            b, cols = rem(i, 2), pl.ds(pl.multiple_of(div(i, 2) * wide, wide), wide)
            part = jnp.dot(
                rows_all[b, EDGE : EDGE + length, deep],
                weight[blocks, :, cols].reshape(span, wide),
                preferred_element_type=f32,
            )
            if fresh:
                acc[b, held_rows, cols] = part
            else:
                acc[b, held_rows, cols] += part
            return carry

        lax.fori_loop(0, 2 * (big // wide), tile, 0)

    expand(gate_acc, gates, h, True)
    pass_on(UP, mate, ACROSS, cond=outer)
    arrive(GATE, afar)
    arrive(GATE, afmate)
    expand(gate_acc, gates, 1 - h, False)
    arrive(UP, across)
    pass_on(UP, far, ACROSS)
    pass_on(UP, fmate, ACROSS)
    arrive(UP, amate)
    expand(up_acc, ups, h, True)
    pass_on(DOWN, mate, FAR)
    send(DOWN, mate, ACROSS, across)
    for i in range(3):
        edge(i)().wait_recv()
    when(before, lambda: onward().wait_recv())
    when(behind, lambda: back().wait_recv())

    def halo(i, carry):
        cols = pl.ds(pl.multiple_of(i * wide, wide), wide)
        sides = (slice(0, EDGE), slice(EDGE + length, length + 2 * EDGE))
        part = jnp.dot(
            jnp.concatenate([rows_all[b, side, :] for b in range(2) for side in sides], axis=0),
            gates[:, :, cols].reshape(sp * depth, wide),
            preferred_element_type=f32,
        )
        for k in range(4):
            gate_acc[k // 2, sides[k % 2], cols] = part[k * EDGE : (k + 1) * EDGE]
        return carry

    lax.fori_loop(0, big // wide, halo, 0)
    arrive(UP, afar)
    arrive(UP, afmate)
    expand(up_acc, ups, 1 - h, False)

    base = jnp.where(c == q, q * (ff - big), q * (ff - small))

    def activate(b, carry):
        for j in range(big // LANES):
            cols = slice(j * LANES, (j + 1) * LANES)
            spot = jnp.minimum(base + j * LANES, ff - LANES)
            taps = pl.ds(pl.multiple_of(spot, LANES), LANES)

            def fill():
                def tap(start):
                    return gate_acc[b, start : start + length, cols].astype(bf16).astype(f32)

                conv = (
                    tap(EDGE - 1) * conv_weight[0:1, taps]
                    + tap(EDGE) * conv_weight[1:2, taps]
                    + tap(EDGE + 1) * conv_weight[2:3, taps]
                    + conv_bias[pl.ds(div(spot, LANES), 1), :]
                )
                hidden[b, :, cols] = (conv / (1.0 + jnp.exp(-conv)) * up_acc[b, :, cols]).astype(
                    bf16
                )

            if (j + 1) * LANES <= small:
                fill()
            else:
                pl.when(c == q)(fill)

                @pl.when(c != q)
                def _():
                    hidden[b, :, cols] = jnp.zeros((length, LANES), bf16)

        return carry

    lax.fori_loop(0, 2, activate, 0)

    per = sp // tp

    def owner(s):
        o = div(s, per)
        return div(o, 2), rem(o, 2)

    def core_slot(s):
        return div(s, half_sp) * per + rem(s, per)

    def core_copy(s):
        return remote(
            stage.at[s], from_core.at[core_slot(s)], part_send.at[0, s],
            core_recv.at[core_slot(s)], {"tp": sibling},
        )

    def z_copy(s):
        return remote(
            stage.at[s, 0], from_z.at[core_slot(s)], part_send.at[0, s],
            z_recv.at[core_slot(s)], {"sp": mate},
        )

    def x_copy(s):
        return remote(
            stage.at[s, 1], from_x.at[rem(s, per)], part_send.at[1, s], x_recv.at[rem(s, per)],
            {"tp": xdev},
        )

    def multiply(s):
        ox, oc = owner(s)
        product = jnp.dot(
            hidden[...].reshape(2 * length, big), downs[s], preferred_element_type=f32
        ).reshape(2, length, down_cols)

        @pl.when(c != oc)
        def _():
            stage[s] = product.astype(bf16)

        @pl.when(c == oc)
        def _():
            held[core_slot(s)] = product

        ship(lambda: core_copy(s), c != oc)

    def add_core(s):
        ox, oc = owner(s)
        mine = c == oc
        slot = core_slot(s)

        @pl.when(mine)
        def _():
            core_copy(s).wait_recv()
            stage[s, 0] = (held[slot, 1 - q] + from_core[slot, 1 - q].astype(f32)).astype(bf16)

        ship(lambda: z_copy(s), mine)

    def out_cols(s):
        return pl.ds(pl.multiple_of(rem(s, per) * down_cols, down_cols), down_cols)

    def add_z(s):
        ox, oc = owner(s)
        mine = c == oc
        slot = core_slot(s)

        def summed():
            return (
                held[slot, q] + from_core[slot, q].astype(f32) + from_z[slot].astype(f32)
            )

        when(mine, lambda: z_copy(s).wait_recv())

        @pl.when(jnp.logical_and(mine, x == ox))
        def _():
            after_own[:, out_cols(s)] += summed()

        @pl.when(jnp.logical_and(mine, x != ox))
        def _():
            stage[s, 1] = summed().astype(bf16)

        ship(lambda: x_copy(s), jnp.logical_and(mine, x != ox))

    multiply(me)
    multiply(mate)
    add_core(me)
    pass_on(DOWN, far, ACROSS)
    arrive(DOWN, across)
    multiply(across)
    add_core(mate)
    arrive(DOWN, amate)
    multiply(amate)
    add_core(across)
    pass_on(DOWN, fmate, ACROSS)
    multiply(far)
    add_core(amate)
    multiply(fmate)
    add_core(far)
    when(c != q, lambda: after_copy().wait_recv())
    add_z(me)
    add_z(mate)
    arrive(DOWN, afar)
    multiply(afar)
    add_core(fmate)
    add_z(across)
    add_z(amate)
    arrive(DOWN, afmate)
    multiply(afmate)
    add_core(afar)
    add_core(afmate)
    for s in (far, fmate, afar, afmate):
        add_z(s)
    for k in range(per):
        cols = slice(k * down_cols, (k + 1) * down_cols)
        x_copy(k).wait_recv()
        out[:, cols] = (after_own[:, cols] + from_x[k].astype(f32)).astype(bf16)

    for cond, make in drains:
        when(cond, lambda: make().wait_send())


def fused(sp, tp, *args):
    resid, queries, keys, values = args[:4]
    gate_weight, down_weight = args[8], args[12]
    length, width = queries.shape
    features = resid.shape[1]
    depth, ff = gate_weight.shape
    maps = 2
    heads = tp * (width // VD)
    full = tp * features
    bf16, f32 = jnp.bfloat16, jnp.float32
    dma = pltpu.SemaphoreType.DMA
    vmem = pl.BlockSpec(memory_space=pltpu.VMEM)
    smem = pl.BlockSpec(memory_space=pltpu.SMEM)
    hbm = pl.BlockSpec(memory_space=pl.ANY)
    rows = length + 2 * EDGE
    down_cols = down_weight.shape[1]
    tiles = ff // LANES
    big = (tiles - tiles // 2) * LANES
    per = sp // tp
    args = list(args)
    for i in (5, 7):
        args[i] = args[i].reshape(1, -1)
    args[11] = args[11].reshape(-1, LANES)
    return pl.pallas_call(
        functools.partial(layer_kernel, sp, tp),
        out_shape=jax.ShapeDtypeStruct(resid.shape, bf16),
        in_specs=[
            hbm, hbm, hbm, hbm, smem, vmem, hbm, vmem, hbm, hbm, vmem, vmem, hbm,
        ],
        out_specs=vmem,
        scratch_shapes=[
            pltpu.VMEM((2, length, VD), bf16),
            pltpu.VMEM((maps, 2 * length, VD), bf16),
            pltpu.VMEM((sp, 2, length, VD), bf16),
            pltpu.VMEM((sp, depth, big), bf16),
            pltpu.VMEM((sp, depth, big), bf16),
            pltpu.VMEM((sp, big, down_cols), bf16),
            pltpu.VMEM((maps, 2 * length, LANES), f32),
            pltpu.VMEM((maps, 2 * length, LANES), f32),
            pltpu.VMEM((maps, 2 * length, VD), f32),
            pltpu.VMEM((2, length, VD), bf16),
            pltpu.VMEM((heads, length, VD), bf16),
            pltpu.VMEM((tp, heads * VD, features), bf16),
            pltpu.VMEM((tp, length, features), bf16),
            pltpu.VMEM((tp, 1, features), f32),
            pltpu.VMEM((length, full), f32),
            pltpu.VMEM((length, features), f32),
            pltpu.VMEM((2, rows, full), bf16),
            pltpu.VMEM((2, rows, big), f32),
            pltpu.VMEM((2, length, big), f32),
            pltpu.VMEM((2, length, big), bf16),
            pltpu.VMEM((2 * per, 2, length, down_cols), f32),
            pltpu.VMEM((sp, 2, length, down_cols), bf16),
            pltpu.VMEM((2 * per, 2, length, down_cols), bf16),
            pltpu.VMEM((per, length, down_cols), bf16),
            pltpu.VMEM((2 * per, length, down_cols), bf16),
            dma((12,)),
            dma((5, 4, sp)),
            dma((5, sp)),
            dma((2,)),
            dma((8,)),
            dma((heads,)),
            dma((3,)),
            dma((tp,)),
            dma((5,)),
            dma((tp,)),
            dma((3,)),
            dma((tp,)),
            dma((2,)),
            dma((2,)),
            dma((4,)),
            dma((4,)),
            dma((2, sp)),
            dma((2 * per,)),
            dma((per,)),
            dma((2 * per,)),
        ],
        compiler_params=pltpu.CompilerParams(
            has_side_effects=True, collective_id=0, vmem_limit_bytes=60 * 1024 * 1024
        ),
    )(*args)


def solution(mesh):
    sp, tp = mesh.shape["sp"], mesh.shape["tp"]

    def run(*args):
        width, (depth, ff) = args[1].shape[1], args[8].shape
        small = args[0].shape[0] <= 512
        pairs = tp == 4 and sp == 2 * tp
        if pairs and small and depth % 256 == 0 and width == 2 * VD and ff % 256 == 128:
            return fused(sp, tp, *args)
        return on_device(*args)

    placed = (
        P("sp", "tp"),
        P("sp", "tp"),
        P("sp", "tp"),
        P("sp", "tp"),
        P("tp"),
        P(),
        P(None, "tp"),
        P("tp"),
        P("sp", "tp"),
        P("sp", "tp"),
        P(None, "tp"),
        P("tp"),
        P("tp", "sp"),
    )
    return jax.shard_map(
        run, mesh=mesh, in_specs=placed, out_specs=P("sp", "tp"), check_vma=False
    )
```

```python
import functools
import math

import jax
import jax.numpy as jnp
from jax import lax
from jax.experimental import pallas as pl
from jax.experimental.pallas import tpu as pltpu
from jax.sharding import PartitionSpec as P

D = 2048
HD = 64
VD = 128


def with_halo(cells, sides, width):
    for axis, dim in sides:
        count = lax.axis_size(axis)
        ends = count - 1
        head = lax.slice_in_dim(cells, 0, width, axis=dim)
        tail = lax.slice_in_dim(cells, cells.shape[dim] - width, cells.shape[dim], axis=dim)
        cells = jnp.concatenate(
            [
                lax.ppermute(tail, axis, [(i, (i + 1) % count) for i in range(ends)]),
                cells,
                lax.ppermute(head, axis, [((i + 1) % count, i) for i in range(ends)]),
            ],
            axis=dim,
        )
    return cells


def on_device(
    resid,
    queries,
    keys,
    values,
    mix_lambda,
    head_gain,
    out_weight,
    norm_gain,
    gate_weight,
    up_weight,
    conv_weight,
    conv_bias,
    down_weight,
):
    length = queries.shape[0]
    heads = mix_lambda.shape[0]
    scale = HD ** (-0.5)
    query_heads = queries.reshape(length, heads, 2, HD)
    initial = (
        jnp.full((heads, 2, length), -1e30, jnp.float32),
        jnp.zeros((heads, 2, length), jnp.float32),
        jnp.zeros((heads, 2, length, VD), jnp.float32),
    )
    key_rows = lax.all_gather(keys, "sp", axis=0, tiled=True)
    value_rows = lax.all_gather(values, "sp", axis=0, tiled=True)
    count = key_rows.shape[0]
    block = math.gcd(count, 2048)
    key_blocks = key_rows.reshape(count // block, block, heads, 2, HD)
    value_blocks = value_rows.reshape(count // block, block, heads, VD)

    def advance(state, blocks):
        running, totals, weighted = state
        key_block, value_block = blocks
        scores = (
            jnp.einsum(
                "qhmd,khmd->hmqk", query_heads, key_block, preferred_element_type=jnp.float32
            )
            * scale
        )
        highest = jnp.maximum(running, jnp.max(scores, axis=-1))
        factor = jnp.exp(running - highest)
        shifted = jnp.exp(scores - highest[..., None])
        totals = totals * factor + jnp.sum(shifted, axis=-1)
        weighted = weighted * factor[..., None] + jnp.einsum(
            "hmqk,khe->hmqe",
            shifted.astype(jnp.bfloat16),
            value_block,
            preferred_element_type=jnp.float32,
        )
        return ((highest, totals, weighted), None)

    result, unused = lax.scan(advance, initial, (key_blocks, value_blocks))
    running, totals, weighted = result
    mapped = weighted / totals[..., None]
    mixed = mapped[:, 0] - mix_lambda[:, None, None] * mapped[:, 1]
    spread = jnp.mean(mixed * mixed, axis=-1, keepdims=True)
    normed = mixed * lax.rsqrt(spread + 1e-06) * head_gain * 0.8
    heads_out = jnp.transpose(normed, (1, 0, 2)).reshape(length, heads * VD).astype(jnp.bfloat16)
    projected = jnp.dot(
        lax.all_gather(heads_out, "tp", axis=1, tiled=True),
        out_weight,
        preferred_element_type=jnp.float32,
    )
    after_mixer = resid.astype(jnp.float32) + projected
    squares = lax.psum(jnp.sum(after_mixer * after_mixer, axis=1), "tp")
    normed_rows = (after_mixer * lax.rsqrt(squares / D + 1e-06)[:, None] * norm_gain).astype(
        jnp.bfloat16
    )
    full_rows = lax.all_gather(normed_rows, "tp", axis=1, tiled=True)
    gate_sum = jnp.dot(
        full_rows,
        lax.all_gather(gate_weight, "sp", axis=0, tiled=True),
        preferred_element_type=jnp.float32,
    )
    upward = jnp.dot(
        full_rows,
        lax.all_gather(up_weight, "sp", axis=0, tiled=True),
        preferred_element_type=jnp.float32,
    )
    gated = gate_sum.astype(jnp.bfloat16)
    padded = with_halo(gated, (("sp", 0),), 1).astype(jnp.float32)
    conv = (
        padded[:-2] * conv_weight[0]
        + padded[1:-1] * conv_weight[1]
        + padded[2:] * conv_weight[2]
        + conv_bias
    )
    hidden = (jax.nn.silu(conv) * upward).astype(jnp.bfloat16)
    partial_terms = jnp.dot(
        hidden,
        lax.all_gather(down_weight, "sp", axis=1, tiled=True),
        preferred_element_type=jnp.float32,
    )
    mixer_out = lax.psum_scatter(
        partial_terms.astype(jnp.bfloat16), "tp", scatter_dimension=1, tiled=True
    ).astype(jnp.float32)
    return (after_mixer + mixer_out).astype(jnp.bfloat16)


EDGE = 16
LANES = 128


def layer_kernel(
    sp,
    tp,
    resid,
    queries,
    keys,
    values,
    mix_lambda,
    head_gain,
    out_weight,
    norm_gain,
    gate_weight,
    up_weight,
    conv_weight,
    conv_bias,
    down_weight,
    out,
    q_all,
    qs,
    kv,
    gates,
    ups,
    downs,
    peaks,
    totals,
    weighted,
    heads_own,
    heads_all,
    out_all,
    resid_all,
    gain_all,
    after,
    after_own,
    rows_all,
    gate_acc,
    up_acc,
    active,
    hidden,
    held,
    stage,
    from_core,
    from_x,
    from_z,
    done,
    local_sem,
    send_sem,
    recv_sem,
    q_sem,
    head_send,
    head_recv,
    out_send,
    out_recv,
    resid_send,
    resid_recv,
    gain_send,
    gain_recv,
    row_sem,
    after_sem,
    edge_send,
    edge_recv,
    part_send,
    core_recv,
    x_recv,
    z_recv,
):
    bf16, f32 = jnp.bfloat16, jnp.float32
    div, rem = lax.div, lax.rem
    me = lax.axis_index("sp")
    t = lax.axis_index("tp")
    z, y = div(me, 2), rem(me, 2)
    h, q = div(z, 2), rem(z, 2)
    x, c = div(t, 2), rem(t, 2)
    mate = me + 2 - 4 * q
    across = me + 1 - 2 * y
    far = me + 4 - 8 * h
    fmate = far + 2 - 4 * q
    adjacent = me + 2 - 4 * h
    amate = across + 2 - 4 * q
    afar = across + 4 - 8 * h
    afmate = afar + 2 - 4 * q
    inner, outer = h != q, h == q
    sibling = t + 1 - 2 * c
    xdev = t + 2 - 4 * x
    xsib = sibling + 2 - 4 * x

    length = queries.shape[0]
    depth, ff = gate_weight.shape
    features = resid.shape[1]
    big = gates.shape[2]
    small = ff - big
    down_cols = down_weight.shape[1]
    half_sp = sp // 2
    K, V = 0, 1
    KEYS, GATE, UP, DOWN = (K, V), (2,), (3, 4), (5, 6)
    ACROSS, FAR, MATE, ADJACENT = range(4)

    drains = []

    def both(a, b):
        return b if a is None else jnp.logical_and(a, b)

    def when(cond, body):
        if cond is None:
            body()
        else:
            pl.when(cond)(body)

    def remote(src, dst, send, recv, target):
        return pltpu.make_async_remote_copy(
            src_ref=src,
            dst_ref=dst,
            send_sem=send,
            recv_sem=recv,
            device_id=target,
            device_id_type=pl.DeviceIdType.MESH,
        )

    def ship(make, cond=None):
        when(cond, lambda: make().start())
        drains.append((cond, make))

    def variants(array, part):
        if array in KEYS:
            return ((None, 0),)
        return ((c == part, big), (c != part, small))

    def landing(array, src, size):
        if array in KEYS:
            return kv.at[src, array]
        if array in DOWN:
            rows = size // len(DOWN)
            return downs.at[src, pl.ds((array - DOWN[0]) * rows, rows)]
        if array in UP:
            rows = depth // len(UP)
            return ups.at[src, pl.ds((array - UP[0]) * rows, rows), pl.ds(0, size)]
        return gates.at[src, :, pl.ds(0, size)]

    def origin(array, part, size):
        if array in KEYS:
            cols = pl.ds(pl.multiple_of(part * VD, VD), VD)
            return (keys, values)[array].at[:, cols]
        start = part * (ff - size)
        if array in DOWN:
            rows = size // len(DOWN)
            first = start + (array - DOWN[0]) * rows
            return down_weight.at[pl.ds(pl.multiple_of(first, LANES // 2), rows)]
        cut = pl.ds(pl.multiple_of(start, LANES), size)
        if array in UP:
            rows = depth // len(UP)
            return up_weight.at[pl.ds((array - UP[0]) * rows, rows), cut]
        return gate_weight.at[:, cut]

    def send_slot(way, src):
        if src is me:
            return way
        return 4 if way == FAR else {id(mate): 5, id(far): 6, id(fmate): 7}[id(src)]

    def send(array, src, way, target, part=None, cond=None):
        for which, size in variants(array, q if part is None else part):

            def make(size=size):
                here = landing(array, src, size)
                return remote(
                    here if part is None else origin(array, part, size),
                    here,
                    send_sem.at[array, send_slot(way, src)],
                    recv_sem.at[array, src],
                    {"sp": target},
                )

            ship(make, both(cond, which) if which is not None else cond)

    def feed(group, *ways, cond=None):
        other = 1 - q
        for way in ways:
            for array in group:
                if way == ACROSS:
                    send(array, me, ACROSS, across, part=q)
                elif way == FAR:
                    send(array, me, FAR, far, part=q, cond=cond)
                elif way == MATE:
                    send(array, me, MATE, mate, part=other, cond=cond)
                else:
                    send(array, me, ADJACENT, adjacent, part=other, cond=inner)

    def arrive(group, src, cond=None):
        for array in group:
            for which, size in variants(array, q):

                def wait(size=size, array=array):
                    here = landing(array, src, size)
                    remote(
                        here, here, send_sem.at[array, 0], recv_sem.at[array, src], {"sp": across}
                    ).wait_recv()

                when(both(cond, which) if which is not None else cond, wait)

    def pass_on(group, src, *ways, cond=None):
        for array in group:
            arrive((array,), src, cond)
            for way in ways:
                if way == FAR:
                    send(array, src, FAR, far, cond=inner)
                else:
                    send(array, src, ACROSS, across, cond=cond)

    before = jnp.logical_and(y == 1, h == 0)
    behind = jnp.logical_and(y == 0, h == 1)
    later = jnp.minimum(me + half_sp - 1, sp - 1)
    earlier = jnp.maximum(me - half_sp + 1, 0)
    barrier = pltpu.get_barrier_semaphore()

    def greet(target, cond=None):
        when(
            cond,
            lambda: pl.semaphore_signal(
                barrier, inc=1, device_id=target, device_id_type=pl.DeviceIdType.MESH
            ),
        )

    for target in (
        {"sp": far},
        {"sp": mate},
        {"sp": mate, "tp": sibling},
        {"sp": across},
        {"tp": xdev},
        {"tp": xsib},
        {"tp": sibling},
    ):
        greet(target)
    greet({"sp": adjacent}, inner)
    greet({"sp": later}, before)
    greet({"sp": earlier}, behind)
    pl.semaphore_wait(
        barrier,
        7 + jnp.where(inner, 1, 0) + jnp.where(jnp.logical_or(before, behind), 1, 0),
    )

    for way in (MATE, ADJACENT, ACROSS):
        feed(KEYS, way)

    def q_copy():
        cols = pl.ds(pl.multiple_of((1 - q) * VD, VD), VD)
        return remote(queries.at[:, cols], q_all.at[q], q_sem.at[0], q_sem.at[1], {"sp": mate})

    local = []

    def fetch(src, dst, cond=None):
        sem = local_sem.at[len(local)]
        make = lambda: pltpu.make_async_copy(src, dst, sem)
        local.append((cond, make))
        when(cond, lambda: make().start())

    def fetched(first, last=None):
        for cond, make in local[first:last]:
            when(cond, lambda: make().wait())

    own_cols = pl.ds(pl.multiple_of(q * VD, VD), VD)
    fetch(queries.at[:, own_cols], q_all.at[q])
    for array in (K, V):
        fetch(origin(array, q, 0), landing(array, me, 0))
    early = len(local)
    for array in GATE + UP + DOWN:
        for which, size in variants(array, q):
            fetch(origin(array, q, size), landing(array, me, size), which)
    fetch(out_weight, out_all.at[t])
    fetch(resid, resid_all.at[t], c == q)
    fetch(norm_gain, gain_all.at[t])

    def out_copy(src, slot, target, send):
        return lambda: remote(
            src, out_all.at[slot], out_send.at[send], out_recv.at[slot], {"tp": target}
        )

    def gain_copy(target, send):
        return lambda: remote(
            norm_gain, gain_all.at[t], gain_send.at[send], gain_recv.at[t], {"tp": target}
        )

    def resid_copy(src, slot, target, send):
        return lambda: remote(
            src, resid_all.at[slot], resid_send.at[send], resid_recv.at[slot], target
        )

    for i, target in enumerate((sibling, xdev, xsib)):
        ship(gain_copy(target, i))
    ship(out_copy(out_weight, t, xdev, 0))
    ship(resid_copy(resid, t, {"tp": 2 * (1 - x) + q}, 0))
    ship(out_copy(out_weight, t, sibling, 1))
    ship(resid_copy(resid, t, {"tp": sibling}, 1), c != q)

    peaks[...] = jnp.full(peaks.shape, -1e30, f32)
    totals[...] = jnp.zeros(totals.shape, f32)
    weighted[...] = jnp.zeros(weighted.shape, f32)

    @pl.when(c != q)
    def _():
        downs[:, small:, :] = jnp.zeros((sp, big - small, down_cols), bf16)

    fetched(0, early)
    lanes = lax.broadcasted_iota(jnp.int32, (1, VD), 1)

    def spread_queries(block):
        value = q_all[block].astype(f32) * HD**-0.5
        at = pl.ds(pl.multiple_of(block * length, length), length)
        for m in range(2):
            keep = lanes < HD if m == 0 else lanes >= HD
            qs[m, at, :] = jnp.where(keep, value, 0.0).astype(bf16)

    rows = math.gcd(length, 256)

    def attend(src, first=0, last=2 * length // rows):
        def row_block(r, carry):
            at = pl.ds(pl.multiple_of(r * rows, rows), rows)
            key_block = kv[src, K]
            value_block = kv[src, V]
            for m in range(2):
                s = lax.dot_general(
                    qs[m, at, :], key_block, (((1,), (1,)), ((), ())), preferred_element_type=f32
                )
                old = peaks[m, at, :]
                new = jnp.maximum(old, jnp.max(s, axis=1, keepdims=True))
                factor = jnp.exp(old - new)
                p = jnp.exp(s - jnp.concatenate([new] * (length // VD), axis=1))
                peaks[m, at, :] = new
                summed = totals[m, at, :] * factor
                for j in range(length // VD):
                    summed = summed + p[:, j * VD : (j + 1) * VD]
                totals[m, at, :] = summed
                weighted[m, at, :] = weighted[m, at, :] * factor + jnp.dot(
                    p.astype(bf16), value_block, preferred_element_type=f32
                )
            return carry

        lax.fori_loop(first, last, row_block, 0)

    def kv_pass(src, *ways):
        pass_on(KEYS, src, *ways)

    per_block = length // rows
    spread_queries(q)
    attend(me, q * per_block, (q + 1) * per_block)
    feed(KEYS, FAR)
    ship(q_copy)
    ship(resid_copy(resid, t, {"sp": mate, "tp": 2 * x + q}, 2))
    feed(GATE, ACROSS)
    kv_pass(mate, FAR, ACROSS)
    feed(GATE, ADJACENT, FAR, MATE)
    attend(mate, q * per_block, (q + 1) * per_block)
    kv_pass(across)
    attend(across, q * per_block, (q + 1) * per_block)
    q_copy().wait_recv()
    spread_queries(1 - q)
    for src in (me, mate, across):
        attend(src, (1 - q) * per_block, (2 - q) * per_block)
    kv_pass(far, ACROSS)
    kv_pass(amate)
    attend(amate)
    kv_pass(fmate, ACROSS)
    feed(UP, ACROSS)
    feed(DOWN, ACROSS)
    attend(far)

    def resid_wait(slot):
        resid_copy(resid, slot, {"tp": sibling}, 0)().wait_recv()

    for k in range(2):
        slot = 2 * x + k
        when(c != q, lambda: resid_wait(slot))
        ship(resid_copy(resid_all.at[slot], slot, {"tp": xdev}, 3 + k), c != q)
    out_copy(out_weight, xdev, sibling, 0)().wait_recv()
    ship(out_copy(out_all.at[xdev], xdev, sibling, 2))
    attend(fmate)
    kv_pass(afar)
    attend(afar)
    pass_on(GATE, mate, FAR, ACROSS, cond=inner)
    feed(UP, ADJACENT)
    feed(UP, FAR, cond=inner)
    kv_pass(afmate)
    attend(afmate)

    head = 2 * t + q
    for b in range(2):
        at = slice(b * length, (b + 1) * length)
        first = weighted[0, at, :] / jnp.sum(totals[0, at, :], axis=1, keepdims=True)
        second = weighted[1, at, :] / jnp.sum(totals[1, at, :], axis=1, keepdims=True)
        mixed = first - mix_lambda[q] * second
        spread = jnp.mean(mixed * mixed, axis=1, keepdims=True)
        normed = mixed * lax.rsqrt(spread + 1e-06) * head_gain[...] * 0.8
        heads_own[b] = normed.astype(bf16)

        @pl.when(c == b)
        def _():
            heads_all[head] = heads_own[b]

    def head_copy(src, slot, target, send):
        return lambda: remote(
            src, heads_all.at[slot], head_send.at[send], head_recv.at[slot], target
        )

    for b in range(2):
        ship(head_copy(heads_own.at[b], head, {"sp": mate, "tp": 2 * x + b}, b))
    for b in range(2):
        ship(head_copy(heads_own.at[b], head, {"tp": 2 * (1 - x) + b}, 2 + b))
        ship(head_copy(heads_own.at[b], head, {"tp": sibling}, 4 + b), c != b)

    feed(UP, MATE)
    feed(UP, FAR, cond=outer)

    def head_wait(slot):
        head_copy(heads_all.at[slot], slot, {"tp": sibling}, 0)().wait_recv()

    pass_on(GATE, far, ACROSS, cond=inner)
    pass_on(GATE, mate, ACROSS, cond=outer)
    pass_on(GATE, far, ACROSS, cond=outer)
    for k in range(2):
        slot = 2 * (2 * x + k) + 1 - q
        head_wait(slot)
        ship(head_copy(heads_all.at[slot], slot, {"tp": xdev}, 6 + k))

    fetched(early)

    out_copy(out_weight, sibling, sibling, 0)().wait_recv()
    out_copy(out_weight, xsib, sibling, 0)().wait_recv()
    for slot in (sibling, xdev, xsib):
        remote(
            norm_gain, gain_all.at[slot], gain_send.at[0], gain_recv.at[slot], {"tp": sibling}
        ).wait_recv()
    when(c == q, lambda: resid_wait(sibling))
    for k in range(2):
        resid_wait(2 * (1 - x) + k)
    head_wait(2 * sibling + q)
    for k in range(2):
        head_wait(2 * (2 * (1 - x) + k) + q)
    for k in range(2):
        head_wait(2 * (2 * (1 - x) + k) + 1 - q)

    pass_on(GATE, fmate, ACROSS)
    row_sum = jnp.zeros((length, 1), f32)
    for j in range(tp):
        cols = slice(j * features, (j + 1) * features)
        total = resid_all[j].astype(f32) + jnp.dot(
            jnp.concatenate([heads_all[i] for i in range(heads_all.shape[0])], axis=1),
            out_all[j],
            preferred_element_type=f32,
        )
        after[:, cols] = total
        row_sum = row_sum + jnp.sum(total * total, axis=1, keepdims=True)
    inverse = lax.rsqrt(row_sum / D + 1e-06)
    for j in range(tp):
        cols = slice(j * features, (j + 1) * features)
        rows_all[c, EDGE : EDGE + length, cols] = (
            after[:, cols] * inverse * gain_all[j]
        ).astype(bf16)

    def row_copy(block):
        here = rows_all.at[block, pl.ds(EDGE, length)]
        return remote(here, here, row_sem.at[0], row_sem.at[1], {"tp": sibling})

    ship(lambda: row_copy(c))

    def own_features(device):
        return pl.ds(pl.multiple_of(device * features, features), features)

    def after_copy():
        return remote(
            after.at[:, own_features(sibling)],
            after_own,
            after_sem.at[0],
            after_sem.at[1],
            {"tp": sibling},
        )

    ship(after_copy, c == q)

    @pl.when(c == q)
    def _():
        after_own[...] = after[:, own_features(t)]

    pass_on(UP, mate, FAR, ACROSS, cond=inner)
    row_copy(1 - c).wait_recv()

    begin, end, top, bottom = EDGE, length, 0, EDGE + length

    def edge_copy(i, source_block, source, block, dest, target):
        def rows_at(start):
            return pl.ds(pl.multiple_of(start, EDGE), EDGE)

        return remote(
            rows_all.at[source_block, rows_at(source)],
            rows_all.at[block, rows_at(dest)],
            edge_send.at[i],
            edge_recv.at[i],
            {"sp": target},
        )

    def pick(first, second):
        return first + y * (second - first)

    def edge(i):
        return (
            lambda: edge_copy(0, 0, pick(end, begin), 0, pick(top, bottom), across),
            lambda: edge_copy(
                1, pick(1, 0), pick(begin, end), pick(0, 1), pick(bottom, top), across
            ),
            lambda: edge_copy(2, 1, pick(end, begin), 1, pick(top, bottom), across),
        )[i]

    for i in range(3):
        ship(edge(i))
    onward = lambda: edge_copy(3, 1, end, 0, top, later)
    back = lambda: edge_copy(3, 0, begin, 1, bottom, earlier)
    ship(onward, before)
    ship(back, behind)
    feed(DOWN, MATE, cond=outer)

    @pl.when(jnp.logical_and(y == 0, h == 0))
    def _():
        rows_all[0, 0:EDGE, :] = jnp.zeros((EDGE, rows_all.shape[2]), bf16)

    @pl.when(jnp.logical_and(y == 1, h == 1))
    def _():
        rows_all[1, EDGE + length :, :] = jnp.zeros((EDGE, rows_all.shape[2]), bf16)

    arrive(GATE, across)
    arrive(GATE, amate)

    wide = 2 * LANES

    def expand(acc, weight, start, count, fresh, store=None):
        span = count * depth
        held_rows = pl.ds(EDGE if acc is gate_acc else 0, length)
        deep = pl.ds(pl.multiple_of(start * depth, depth), span)
        blocks = pl.ds(start, count)

        def tile(i, carry):
            b, cols = rem(i, 2), pl.ds(pl.multiple_of(div(i, 2) * wide, wide), wide)
            part = jnp.dot(
                rows_all[b, EDGE : EDGE + length, deep],
                weight[blocks, :, cols].reshape(span, wide),
                preferred_element_type=f32,
            )
            if store is not None:
                store(b, cols, part)
            elif fresh:
                acc[b, held_rows, cols] = part
            else:
                acc[b, held_rows, cols] += part
            return carry

        lax.fori_loop(0, 2 * (big // wide), tile, 0)

    expand(gate_acc, gates, half_sp * h, half_sp, True)
    pass_on(UP, mate, ACROSS, cond=outer)
    arrive(GATE, afar)
    arrive(GATE, afmate)
    expand(gate_acc, gates, half_sp * (1 - h), half_sp, False)
    arrive(UP, across)
    pass_on(UP, far, ACROSS)
    feed(DOWN, FAR, cond=outer)
    pass_on(UP, fmate, ACROSS, cond=inner)
    arrive(UP, amate)
    feed(DOWN, ADJACENT)
    feed(DOWN, FAR, MATE, cond=inner)
    expand(up_acc, ups, half_sp * h, half_sp, True)
    pass_on(DOWN, mate, FAR, ACROSS, cond=inner)
    pass_on(UP, fmate, ACROSS, cond=outer)
    for i in range(3):
        edge(i)().wait_recv()
    when(before, lambda: onward().wait_recv())
    when(behind, lambda: back().wait_recv())

    def halo(i, carry):
        cols = pl.ds(pl.multiple_of(i * wide, wide), wide)
        sides = (slice(0, EDGE), slice(EDGE + length, length + 2 * EDGE))
        part = jnp.dot(
            jnp.concatenate([rows_all[b, side, :] for b in range(2) for side in sides], axis=0),
            gates[:, :, cols].reshape(sp * depth, wide),
            preferred_element_type=f32,
        )
        for k in range(4):
            gate_acc[k // 2, sides[k % 2], cols] = part[k * EDGE : (k + 1) * EDGE]
        return carry

    lax.fori_loop(0, big // wide, halo, 0)

    base = jnp.where(c == q, q * (ff - big), q * (ff - small))

    def activate(b, carry):
        for j in range(big // LANES):
            cols = slice(j * LANES, (j + 1) * LANES)
            spot = jnp.minimum(base + j * LANES, ff - LANES)
            taps = pl.ds(pl.multiple_of(spot, LANES), LANES)

            def tap(start):
                return gate_acc[b, start : start + length, cols].astype(bf16).astype(f32)

            conv = (
                tap(EDGE - 1) * conv_weight[0:1, taps]
                + tap(EDGE) * conv_weight[1:2, taps]
                + tap(EDGE + 1) * conv_weight[2:3, taps]
                + conv_bias[pl.ds(div(spot, LANES), 1), :]
            )
            active[b, :, cols] = conv / (1.0 + jnp.exp(-conv))

        return carry

    lax.fori_loop(0, 2, activate, 0)
    pass_on(DOWN, mate, ACROSS, cond=outer)
    arrive(UP, afar)
    expand(up_acc, ups, div(far, 2) * 2, 2, False)
    arrive(UP, afmate)

    def finish(b, cols, part):
        hidden[b, :, cols] = (active[b, :, cols] * (up_acc[b, :, cols] + part)).astype(bf16)

    expand(up_acc, ups, div(fmate, 2) * 2, 2, False, finish)

    @pl.when(c != q)
    def _():
        hidden[:, :, small:] = jnp.zeros((2, length, big - small), bf16)

    per = sp // tp

    def owner(s):
        o = div(s, per)
        return div(o, 2), rem(o, 2)

    def core_slot(s):
        return div(s, half_sp) * per + rem(s, per)

    def core_copy(s):
        return remote(
            stage.at[s], from_core.at[core_slot(s)], part_send.at[0, s],
            core_recv.at[core_slot(s)], {"tp": sibling},
        )

    def z_copy(s):
        return remote(
            stage.at[s, 0], from_z.at[core_slot(s)], part_send.at[0, s],
            z_recv.at[core_slot(s)], {"sp": mate},
        )

    def x_copy(s):
        return remote(
            stage.at[s, 1], from_x.at[rem(s, per), 0], part_send.at[1, s],
            x_recv.at[rem(s, per)],
            {"tp": xdev},
        )

    def multiply(s):
        ox, oc = owner(s)
        product = jnp.dot(
            hidden[...].reshape(2 * length, big), downs[s], preferred_element_type=f32
        ).reshape(2, length, down_cols)

        @pl.when(c != oc)
        def _():
            stage[s] = product.astype(bf16)

        @pl.when(c == oc)
        def _():
            held[core_slot(s)] = product

        ship(lambda: core_copy(s), c != oc)

    def wide_copy(s):
        return remote(
            stage.at[s], from_x.at[rem(s, per)], part_send.at[0, s], x_recv.at[rem(s, per)],
            {"tp": xdev},
        )

    def add_core_x(s):
        ox, oc = owner(s)
        mine = c == oc
        slot = core_slot(s)

        @pl.when(mine)
        def _():
            core_copy(s).wait_recv()

        @pl.when(jnp.logical_and(mine, x != ox))
        def _():
            stage[s] = (held[slot] + from_core[slot].astype(f32)).astype(bf16)

        ship(lambda: wide_copy(s), jnp.logical_and(mine, x != ox))

    def add_x(s):
        ox, oc = owner(s)
        mine = jnp.logical_and(c == oc, x == ox)
        slot = core_slot(s)

        def summed(b):
            return (
                held[slot, b]
                + from_core[slot, b].astype(f32)
                + from_x[rem(s, per), b].astype(f32)
            )

        @pl.when(mine)
        def _():
            wide_copy(s).wait_recv()
            stage[s, 0] = summed(1 - q).astype(bf16)

        ship(lambda: z_copy(s), mine)

        @pl.when(mine)
        def _():
            after_own[:, out_cols(s)] += summed(q)

    def add_core(s):
        ox, oc = owner(s)
        mine = c == oc
        slot = core_slot(s)

        @pl.when(mine)
        def _():
            core_copy(s).wait_recv()
            stage[s, 0] = (held[slot, 1 - q] + from_core[slot, 1 - q].astype(f32)).astype(bf16)

        ship(lambda: z_copy(s), mine)

    def out_cols(s):
        return pl.ds(pl.multiple_of(rem(s, per) * down_cols, down_cols), down_cols)

    def add_z(s):
        ox, oc = owner(s)
        mine = c == oc
        slot = core_slot(s)

        def summed():
            return (
                held[slot, q] + from_core[slot, q].astype(f32) + from_z[slot].astype(f32)
            )

        when(mine, lambda: z_copy(s).wait_recv())

        @pl.when(jnp.logical_and(mine, x == ox))
        def _():
            after_own[:, out_cols(s)] += summed()

        @pl.when(jnp.logical_and(mine, x != ox))
        def _():
            stage[s, 1] = summed().astype(bf16)

        ship(lambda: x_copy(s), jnp.logical_and(mine, x != ox))

    settled = len(drains)
    multiply(me)
    multiply(mate)
    pass_on(DOWN, far, ACROSS)
    add_core_x(me)
    arrive(DOWN, across)
    multiply(across)
    add_core_x(mate)
    arrive(DOWN, amate)
    multiply(amate)
    add_core(across)
    pass_on(DOWN, fmate, ACROSS)
    multiply(far)
    add_core(amate)
    multiply(fmate)
    add_core_x(far)
    when(c != q, lambda: after_copy().wait_recv())
    arrive(DOWN, afar)
    multiply(afar)
    add_core_x(fmate)
    add_x(me)
    add_x(mate)
    add_core(afar)
    add_z(across)
    add_z(amate)
    for cond, make in drains[:settled]:
        when(cond, lambda: make().wait_send())
    arrive(DOWN, afmate)
    multiply(afmate)
    add_core(afmate)
    add_x(far)
    add_x(fmate)
    add_z(afar)
    add_z(afmate)

    def out_copy_k(k):
        cols = slice(k * down_cols, (k + 1) * down_cols)
        return pltpu.make_async_copy(done.at[:, cols], out.at[:, cols], local_sem.at[16 + k])

    for k in range(per):
        cols = slice(k * down_cols, (k + 1) * down_cols)
        source = per * t + k

        @pl.when(y == k)
        def _():
            slot = core_slot(source)
            z_copy(source).wait_recv()
            done[:, cols] = (after_own[:, cols] + from_z[slot].astype(f32)).astype(bf16)

        @pl.when(y != k)
        def _():
            x_copy(k).wait_recv()
            done[:, cols] = (after_own[:, cols] + from_x[k, 0].astype(f32)).astype(bf16)

        out_copy_k(k).start()

    for cond, make in drains[settled:]:
        when(cond, lambda: make().wait_send())
    for k in range(per):
        out_copy_k(k).wait()


def fused(sp, tp, *args):
    resid, queries, keys, values = args[:4]
    gate_weight, down_weight = args[8], args[12]
    length, width = queries.shape
    features = resid.shape[1]
    depth, ff = gate_weight.shape
    maps = 2
    heads = tp * (width // VD)
    full = tp * features
    bf16, f32 = jnp.bfloat16, jnp.float32
    dma = pltpu.SemaphoreType.DMA
    vmem = pl.BlockSpec(memory_space=pltpu.VMEM)
    smem = pl.BlockSpec(memory_space=pltpu.SMEM)
    hbm = pl.BlockSpec(memory_space=pl.ANY)
    rows = length + 2 * EDGE
    down_cols = down_weight.shape[1]
    tiles = ff // LANES
    big = (tiles - tiles // 2) * LANES
    per = sp // tp
    args = list(args)
    for i in (5, 7):
        args[i] = args[i].reshape(1, -1)
    args[11] = args[11].reshape(-1, LANES)
    return pl.pallas_call(
        functools.partial(layer_kernel, sp, tp),
        out_shape=jax.ShapeDtypeStruct(resid.shape, bf16),
        in_specs=[
            hbm, hbm, hbm, hbm, smem, vmem, hbm, vmem, hbm, hbm, vmem, vmem, hbm,
        ],
        out_specs=hbm,
        scratch_shapes=[
            pltpu.VMEM((2, length, VD), bf16),
            pltpu.VMEM((maps, 2 * length, VD), bf16),
            pltpu.VMEM((sp, 2, length, VD), bf16),
            pltpu.VMEM((sp, depth, big), bf16),
            pltpu.VMEM((sp, depth, big), bf16),
            pltpu.VMEM((sp, big, down_cols), bf16),
            pltpu.VMEM((maps, 2 * length, LANES), f32),
            pltpu.VMEM((maps, 2 * length, LANES), f32),
            pltpu.VMEM((maps, 2 * length, VD), f32),
            pltpu.VMEM((2, length, VD), bf16),
            pltpu.VMEM((heads, length, VD), bf16),
            pltpu.VMEM((tp, heads * VD, features), bf16),
            pltpu.VMEM((tp, length, features), bf16),
            pltpu.VMEM((tp, 1, features), f32),
            pltpu.VMEM((length, full), f32),
            pltpu.VMEM((length, features), f32),
            pltpu.VMEM((2, rows, full), bf16),
            pltpu.VMEM((2, rows, big), f32),
            pltpu.VMEM((2, length, big), f32),
            pltpu.VMEM((2, length, big), f32),
            pltpu.VMEM((2, length, big), bf16),
            pltpu.VMEM((2 * per, 2, length, down_cols), f32),
            pltpu.VMEM((sp, 2, length, down_cols), bf16),
            pltpu.VMEM((2 * per, 2, length, down_cols), bf16),
            pltpu.VMEM((per, 2, length, down_cols), bf16),
            pltpu.VMEM((2 * per, length, down_cols), bf16),
            pltpu.VMEM(resid.shape, bf16),
            dma((18,)),
            dma((7, 8)),
            dma((7, sp)),
            dma((2,)),
            dma((8,)),
            dma((heads,)),
            dma((3,)),
            dma((tp,)),
            dma((5,)),
            dma((tp,)),
            dma((3,)),
            dma((tp,)),
            dma((2,)),
            dma((2,)),
            dma((4,)),
            dma((4,)),
            dma((2, sp)),
            dma((2 * per,)),
            dma((per,)),
            dma((2 * per,)),
        ],
        compiler_params=pltpu.CompilerParams(
            has_side_effects=True, collective_id=0, vmem_limit_bytes=60 * 1024 * 1024
        ),
    )(*args)


def solution(mesh):
    sp, tp = mesh.shape["sp"], mesh.shape["tp"]

    def run(*args):
        width, (depth, ff) = args[1].shape[1], args[8].shape
        small = args[0].shape[0] <= 512
        pairs = tp == 4 and sp == 2 * tp
        if pairs and small and depth % 256 == 0 and width == 2 * VD and ff % 256 == 128:
            return fused(sp, tp, *args)
        return on_device(*args)

    placed = (
        P("sp", "tp"),
        P("sp", "tp"),
        P("sp", "tp"),
        P("sp", "tp"),
        P("tp"),
        P(),
        P(None, "tp"),
        P("tp"),
        P("sp", "tp"),
        P("sp", "tp"),
        P(None, "tp"),
        P("tp"),
        P("tp", "sp"),
    )
    return jax.shard_map(
        run, mesh=mesh, in_specs=placed, out_specs=P("sp", "tp"), check_vma=False
    )
```

```python
import functools
import math

import jax
import jax.numpy as jnp
from jax import lax
from jax.experimental import pallas as pl
from jax.experimental.pallas import tpu as pltpu
from jax.sharding import PartitionSpec as P

D = 2048
HD = 64
VD = 128


def with_halo(cells, sides, width):
    for axis, dim in sides:
        count = lax.axis_size(axis)
        ends = count - 1
        head = lax.slice_in_dim(cells, 0, width, axis=dim)
        tail = lax.slice_in_dim(cells, cells.shape[dim] - width, cells.shape[dim], axis=dim)
        cells = jnp.concatenate(
            [
                lax.ppermute(tail, axis, [(i, (i + 1) % count) for i in range(ends)]),
                cells,
                lax.ppermute(head, axis, [((i + 1) % count, i) for i in range(ends)]),
            ],
            axis=dim,
        )
    return cells


def on_device(
    resid,
    queries,
    keys,
    values,
    mix_lambda,
    head_gain,
    out_weight,
    norm_gain,
    gate_weight,
    up_weight,
    conv_weight,
    conv_bias,
    down_weight,
):
    length = queries.shape[0]
    heads = mix_lambda.shape[0]
    scale = HD ** (-0.5)
    query_heads = queries.reshape(length, heads, 2, HD)
    initial = (
        jnp.full((heads, 2, length), -1e30, jnp.float32),
        jnp.zeros((heads, 2, length), jnp.float32),
        jnp.zeros((heads, 2, length, VD), jnp.float32),
    )
    key_rows = lax.all_gather(keys, "sp", axis=0, tiled=True)
    value_rows = lax.all_gather(values, "sp", axis=0, tiled=True)
    count = key_rows.shape[0]
    block = math.gcd(count, 2048)
    key_blocks = key_rows.reshape(count // block, block, heads, 2, HD)
    value_blocks = value_rows.reshape(count // block, block, heads, VD)

    def advance(state, blocks):
        running, totals, weighted = state
        key_block, value_block = blocks
        scores = (
            jnp.einsum(
                "qhmd,khmd->hmqk", query_heads, key_block, preferred_element_type=jnp.float32
            )
            * scale
        )
        highest = jnp.maximum(running, jnp.max(scores, axis=-1))
        factor = jnp.exp(running - highest)
        shifted = jnp.exp(scores - highest[..., None])
        totals = totals * factor + jnp.sum(shifted, axis=-1)
        weighted = weighted * factor[..., None] + jnp.einsum(
            "hmqk,khe->hmqe",
            shifted.astype(jnp.bfloat16),
            value_block,
            preferred_element_type=jnp.float32,
        )
        return ((highest, totals, weighted), None)

    result, unused = lax.scan(advance, initial, (key_blocks, value_blocks))
    running, totals, weighted = result
    mapped = weighted / totals[..., None]
    mixed = mapped[:, 0] - mix_lambda[:, None, None] * mapped[:, 1]
    spread = jnp.mean(mixed * mixed, axis=-1, keepdims=True)
    normed = mixed * lax.rsqrt(spread + 1e-06) * head_gain * 0.8
    heads_out = jnp.transpose(normed, (1, 0, 2)).reshape(length, heads * VD).astype(jnp.bfloat16)
    projected = jnp.dot(
        lax.all_gather(heads_out, "tp", axis=1, tiled=True),
        out_weight,
        preferred_element_type=jnp.float32,
    )
    after_mixer = resid.astype(jnp.float32) + projected
    squares = lax.psum(jnp.sum(after_mixer * after_mixer, axis=1), "tp")
    normed_rows = (after_mixer * lax.rsqrt(squares / D + 1e-06)[:, None] * norm_gain).astype(
        jnp.bfloat16
    )
    full_rows = lax.all_gather(normed_rows, "tp", axis=1, tiled=True)
    gate_sum = jnp.dot(
        full_rows,
        lax.all_gather(gate_weight, "sp", axis=0, tiled=True),
        preferred_element_type=jnp.float32,
    )
    upward = jnp.dot(
        full_rows,
        lax.all_gather(up_weight, "sp", axis=0, tiled=True),
        preferred_element_type=jnp.float32,
    )
    gated = gate_sum.astype(jnp.bfloat16)
    padded = with_halo(gated, (("sp", 0),), 1).astype(jnp.float32)
    conv = (
        padded[:-2] * conv_weight[0]
        + padded[1:-1] * conv_weight[1]
        + padded[2:] * conv_weight[2]
        + conv_bias
    )
    hidden = (jax.nn.silu(conv) * upward).astype(jnp.bfloat16)
    partial_terms = jnp.dot(
        hidden,
        lax.all_gather(down_weight, "sp", axis=1, tiled=True),
        preferred_element_type=jnp.float32,
    )
    mixer_out = lax.psum_scatter(
        partial_terms.astype(jnp.bfloat16), "tp", scatter_dimension=1, tiled=True
    ).astype(jnp.float32)
    return (after_mixer + mixer_out).astype(jnp.bfloat16)


EDGE = 16
LANES = 128


def layer_kernel(
    sp,
    tp,
    resid,
    queries,
    keys,
    values,
    mix_lambda,
    head_gain,
    out_weight,
    norm_gain,
    gate_weight,
    up_weight,
    conv_weight,
    conv_bias,
    down_weight,
    out,
    q_all,
    qs,
    kv,
    gates,
    ups,
    downs,
    peaks,
    totals,
    weighted,
    heads_own,
    heads_all,
    out_all,
    resid_all,
    gain_all,
    after,
    after_own,
    rows_all,
    gate_acc,
    up_acc,
    active,
    hidden,
    held,
    stage,
    from_core,
    from_x,
    from_z,
    local_sem,
    send_sem,
    recv_sem,
    q_sem,
    head_send,
    head_recv,
    out_send,
    out_recv,
    resid_send,
    resid_recv,
    gain_send,
    gain_recv,
    row_sem,
    after_sem,
    edge_send,
    edge_recv,
    part_send,
    core_recv,
    x_recv,
    z_recv,
):
    bf16, f32 = jnp.bfloat16, jnp.float32
    div, rem = lax.div, lax.rem
    me = lax.axis_index("sp")
    t = lax.axis_index("tp")
    z, y = div(me, 2), rem(me, 2)
    h, q = div(z, 2), rem(z, 2)
    x, c = div(t, 2), rem(t, 2)
    mate = me + 2 - 4 * q
    across = me + 1 - 2 * y
    far = me + 4 - 8 * h
    fmate = far + 2 - 4 * q
    adjacent = me + 2 - 4 * h
    amate = across + 2 - 4 * q
    afar = across + 4 - 8 * h
    afmate = afar + 2 - 4 * q
    inner, outer = h != q, h == q
    sibling = t + 1 - 2 * c
    xdev = t + 2 - 4 * x
    xsib = sibling + 2 - 4 * x

    length = queries.shape[0]
    depth, ff = gate_weight.shape
    features = resid.shape[1]
    big = gates.shape[2]
    small = ff - big
    down_cols = down_weight.shape[1]
    half_sp = sp // 2
    K, V = 0, 1
    KEYS, GATE, UP, DOWN = (K, V), (2,), (3, 4), (5, 6)
    ACROSS, FAR, MATE, ADJACENT = range(4)

    drains = []

    def both(a, b):
        return b if a is None else jnp.logical_and(a, b)

    def when(cond, body):
        if cond is None:
            body()
        else:
            pl.when(cond)(body)

    def remote(src, dst, send, recv, target):
        return pltpu.make_async_remote_copy(
            src_ref=src,
            dst_ref=dst,
            send_sem=send,
            recv_sem=recv,
            device_id=target,
            device_id_type=pl.DeviceIdType.MESH,
        )

    def ship(make, cond=None):
        when(cond, lambda: make().start())
        drains.append((cond, make))

    def variants(array, part):
        if array in KEYS:
            return ((None, 0),)
        return ((c == part, big), (c != part, small))

    def landing(array, src, size):
        if array in KEYS:
            return kv.at[src, array]
        if array in DOWN:
            rows = size // len(DOWN)
            return downs.at[src, pl.ds((array - DOWN[0]) * rows, rows)]
        if array in UP:
            rows = depth // len(UP)
            return ups.at[src, pl.ds((array - UP[0]) * rows, rows), pl.ds(0, size)]
        return gates.at[src, :, pl.ds(0, size)]

    def origin(array, part, size):
        if array in KEYS:
            cols = pl.ds(pl.multiple_of(part * VD, VD), VD)
            return (keys, values)[array].at[:, cols]
        start = part * (ff - size)
        if array in DOWN:
            rows = size // len(DOWN)
            first = start + (array - DOWN[0]) * rows
            return down_weight.at[pl.ds(pl.multiple_of(first, LANES // 2), rows)]
        cut = pl.ds(pl.multiple_of(start, LANES), size)
        if array in UP:
            rows = depth // len(UP)
            return up_weight.at[pl.ds((array - UP[0]) * rows, rows), cut]
        return gate_weight.at[:, cut]

    def send_slot(way, src):
        if src is me:
            return way
        return 4 if way == FAR else {id(mate): 5, id(far): 6, id(fmate): 7}[id(src)]

    def send(array, src, way, target, part=None, cond=None):
        for which, size in variants(array, q if part is None else part):

            def make(size=size):
                here = landing(array, src, size)
                return remote(
                    here if part is None else origin(array, part, size),
                    here,
                    send_sem.at[array, send_slot(way, src)],
                    recv_sem.at[array, src],
                    {"sp": target},
                )

            ship(make, both(cond, which) if which is not None else cond)

    def feed(group, *ways, cond=None):
        other = 1 - q
        for way in ways:
            for array in group:
                if way == ACROSS:
                    send(array, me, ACROSS, across, part=q)
                elif way == FAR:
                    send(array, me, FAR, far, part=q, cond=cond)
                elif way == MATE:
                    send(array, me, MATE, mate, part=other, cond=cond)
                else:
                    send(array, me, ADJACENT, adjacent, part=other, cond=inner)

    def arrive(group, src, cond=None):
        for array in group:
            for which, size in variants(array, q):

                def wait(size=size, array=array):
                    here = landing(array, src, size)
                    remote(
                        here, here, send_sem.at[array, 0], recv_sem.at[array, src], {"sp": across}
                    ).wait_recv()

                when(both(cond, which) if which is not None else cond, wait)

    def pass_on(group, src, *ways, cond=None):
        for array in group:
            arrive((array,), src, cond)
            for way in ways:
                if way == FAR:
                    send(array, src, FAR, far, cond=inner)
                else:
                    send(array, src, ACROSS, across, cond=cond)

    before = jnp.logical_and(y == 1, h == 0)
    behind = jnp.logical_and(y == 0, h == 1)
    later = jnp.minimum(me + half_sp - 1, sp - 1)
    earlier = jnp.maximum(me - half_sp + 1, 0)
    barrier = pltpu.get_barrier_semaphore()

    def greet(target, cond=None):
        when(
            cond,
            lambda: pl.semaphore_signal(
                barrier, inc=1, device_id=target, device_id_type=pl.DeviceIdType.MESH
            ),
        )

    for target in (
        {"sp": far},
        {"sp": mate},
        {"sp": mate, "tp": sibling},
        {"sp": across},
        {"tp": xdev},
        {"tp": xsib},
        {"tp": sibling},
    ):
        greet(target)
    greet({"sp": adjacent}, inner)
    greet({"sp": later}, before)
    greet({"sp": earlier}, behind)
    pl.semaphore_wait(
        barrier,
        7 + jnp.where(inner, 1, 0) + jnp.where(jnp.logical_or(before, behind), 1, 0),
    )

    for way in (MATE, ADJACENT, ACROSS):
        feed(KEYS, way)

    def q_copy():
        cols = pl.ds(pl.multiple_of((1 - q) * VD, VD), VD)
        return remote(queries.at[:, cols], q_all.at[q], q_sem.at[0], q_sem.at[1], {"sp": mate})

    local = []

    def fetch(src, dst, cond=None):
        sem = local_sem.at[len(local)]
        make = lambda: pltpu.make_async_copy(src, dst, sem)
        local.append((cond, make))
        when(cond, lambda: make().start())

    def fetched(first, last=None):
        for cond, make in local[first:last]:
            when(cond, lambda: make().wait())

    own_cols = pl.ds(pl.multiple_of(q * VD, VD), VD)
    fetch(queries.at[:, own_cols], q_all.at[q])
    for array in (K, V):
        fetch(origin(array, q, 0), landing(array, me, 0))
    early = len(local)
    for array in GATE + UP + DOWN:
        for which, size in variants(array, q):
            fetch(origin(array, q, size), landing(array, me, size), which)
    fetch(out_weight, out_all.at[t])
    fetch(resid, resid_all.at[t], c == q)
    fetch(norm_gain, gain_all.at[t])

    def out_copy(src, slot, target, send):
        return lambda: remote(
            src, out_all.at[slot], out_send.at[send], out_recv.at[slot], {"tp": target}
        )

    def gain_copy(target, send):
        return lambda: remote(
            norm_gain, gain_all.at[t], gain_send.at[send], gain_recv.at[t], {"tp": target}
        )

    def resid_copy(src, slot, target, send):
        return lambda: remote(
            src, resid_all.at[slot], resid_send.at[send], resid_recv.at[slot], target
        )

    for i, target in enumerate((sibling, xdev, xsib)):
        ship(gain_copy(target, i))
    ship(out_copy(out_weight, t, xdev, 0))
    ship(resid_copy(resid, t, {"tp": 2 * (1 - x) + q}, 0))
    ship(out_copy(out_weight, t, sibling, 1))
    ship(resid_copy(resid, t, {"tp": sibling}, 1), c != q)

    peaks[...] = jnp.full(peaks.shape, -1e30, f32)
    totals[...] = jnp.zeros(totals.shape, f32)
    weighted[...] = jnp.zeros(weighted.shape, f32)

    @pl.when(c != q)
    def _():
        downs[:, small:, :] = jnp.zeros((sp, big - small, down_cols), bf16)

    fetched(0, early)
    lanes = lax.broadcasted_iota(jnp.int32, (1, VD), 1)

    def spread_queries(block):
        value = q_all[block].astype(f32) * HD**-0.5
        at = pl.ds(pl.multiple_of(block * length, length), length)
        for m in range(2):
            keep = lanes < HD if m == 0 else lanes >= HD
            qs[m, at, :] = jnp.where(keep, value, 0.0).astype(bf16)

    rows = math.gcd(length, 256)

    def attend(src, first=0, last=2 * length // rows):
        def row_block(r, carry):
            at = pl.ds(pl.multiple_of(r * rows, rows), rows)
            key_block = kv[src, K]
            value_block = kv[src, V]
            for m in range(2):
                s = lax.dot_general(
                    qs[m, at, :], key_block, (((1,), (1,)), ((), ())), preferred_element_type=f32
                )
                old = peaks[m, at, :]
                new = jnp.maximum(old, jnp.max(s, axis=1, keepdims=True))
                factor = jnp.exp(old - new)
                p = jnp.exp(s - jnp.concatenate([new] * (length // VD), axis=1))
                peaks[m, at, :] = new
                summed = totals[m, at, :] * factor
                for j in range(length // VD):
                    summed = summed + p[:, j * VD : (j + 1) * VD]
                totals[m, at, :] = summed
                weighted[m, at, :] = weighted[m, at, :] * factor + jnp.dot(
                    p.astype(bf16), value_block, preferred_element_type=f32
                )
            return carry

        lax.fori_loop(first, last, row_block, 0)

    def kv_pass(src, *ways):
        pass_on(KEYS, src, *ways)

    per_block = length // rows
    spread_queries(q)
    attend(me, q * per_block, (q + 1) * per_block)
    feed(KEYS, FAR)
    ship(q_copy)
    ship(resid_copy(resid, t, {"sp": mate, "tp": 2 * x + q}, 2))
    feed(GATE, ACROSS)
    kv_pass(mate, FAR, ACROSS)
    feed(GATE, ADJACENT, FAR, MATE)
    attend(mate, q * per_block, (q + 1) * per_block)
    kv_pass(across)
    attend(across, q * per_block, (q + 1) * per_block)
    q_copy().wait_recv()
    spread_queries(1 - q)
    for src in (me, mate, across):
        attend(src, (1 - q) * per_block, (2 - q) * per_block)
    kv_pass(far, ACROSS)
    kv_pass(amate)
    attend(amate)
    kv_pass(fmate, ACROSS)
    feed(UP, ACROSS)
    feed(DOWN, ACROSS)
    attend(far)

    def resid_wait(slot):
        resid_copy(resid, slot, {"tp": sibling}, 0)().wait_recv()

    for k in range(2):
        slot = 2 * x + k
        when(c != q, lambda: resid_wait(slot))
        ship(resid_copy(resid_all.at[slot], slot, {"tp": xdev}, 3 + k), c != q)
    out_copy(out_weight, xdev, sibling, 0)().wait_recv()
    ship(out_copy(out_all.at[xdev], xdev, sibling, 2))
    attend(fmate)
    kv_pass(afar)
    attend(afar)
    pass_on(GATE, mate, FAR, ACROSS, cond=inner)
    feed(UP, ADJACENT)
    feed(UP, FAR, cond=inner)
    kv_pass(afmate)
    attend(afmate)

    head = 2 * t + q
    for b in range(2):
        at = slice(b * length, (b + 1) * length)
        first = weighted[0, at, :] / jnp.sum(totals[0, at, :], axis=1, keepdims=True)
        second = weighted[1, at, :] / jnp.sum(totals[1, at, :], axis=1, keepdims=True)
        mixed = first - mix_lambda[q] * second
        spread = jnp.mean(mixed * mixed, axis=1, keepdims=True)
        normed = mixed * lax.rsqrt(spread + 1e-06) * head_gain[...] * 0.8
        heads_own[b] = normed.astype(bf16)

        @pl.when(c == b)
        def _():
            heads_all[head] = heads_own[b]

    def head_copy(src, slot, target, send):
        return lambda: remote(
            src, heads_all.at[slot], head_send.at[send], head_recv.at[slot], target
        )

    for b in range(2):
        ship(head_copy(heads_own.at[b], head, {"sp": mate, "tp": 2 * x + b}, b))
    for b in range(2):
        ship(head_copy(heads_own.at[b], head, {"tp": 2 * (1 - x) + b}, 2 + b))
        ship(head_copy(heads_own.at[b], head, {"tp": sibling}, 4 + b), c != b)

    feed(UP, MATE)
    feed(UP, FAR, cond=outer)

    def head_wait(slot):
        head_copy(heads_all.at[slot], slot, {"tp": sibling}, 0)().wait_recv()

    pass_on(GATE, far, ACROSS, cond=inner)
    pass_on(GATE, mate, ACROSS, cond=outer)
    pass_on(GATE, far, ACROSS, cond=outer)
    for k in range(2):
        slot = 2 * (2 * x + k) + 1 - q
        head_wait(slot)
        ship(head_copy(heads_all.at[slot], slot, {"tp": xdev}, 6 + k))

    fetched(early)

    out_copy(out_weight, sibling, sibling, 0)().wait_recv()
    out_copy(out_weight, xsib, sibling, 0)().wait_recv()
    for slot in (sibling, xdev, xsib):
        remote(
            norm_gain, gain_all.at[slot], gain_send.at[0], gain_recv.at[slot], {"tp": sibling}
        ).wait_recv()
    when(c == q, lambda: resid_wait(sibling))
    for k in range(2):
        resid_wait(2 * (1 - x) + k)
    head_wait(2 * sibling + q)
    for k in range(2):
        head_wait(2 * (2 * (1 - x) + k) + q)
    for k in range(2):
        head_wait(2 * (2 * (1 - x) + k) + 1 - q)

    pass_on(GATE, fmate, ACROSS)
    row_sum = jnp.zeros((length, 1), f32)
    for j in range(tp):
        cols = slice(j * features, (j + 1) * features)
        total = resid_all[j].astype(f32) + jnp.dot(
            jnp.concatenate([heads_all[i] for i in range(heads_all.shape[0])], axis=1),
            out_all[j],
            preferred_element_type=f32,
        )
        after[:, cols] = total
        row_sum = row_sum + jnp.sum(total * total, axis=1, keepdims=True)
    inverse = lax.rsqrt(row_sum / D + 1e-06)
    for j in range(tp):
        cols = slice(j * features, (j + 1) * features)
        rows_all[c, EDGE : EDGE + length, cols] = (
            after[:, cols] * inverse * gain_all[j]
        ).astype(bf16)

    def row_copy(block):
        here = rows_all.at[block, pl.ds(EDGE, length)]
        return remote(here, here, row_sem.at[0], row_sem.at[1], {"tp": sibling})

    ship(lambda: row_copy(c))

    def own_features(device):
        return pl.ds(pl.multiple_of(device * features, features), features)

    def after_copy():
        return remote(
            after.at[:, own_features(sibling)],
            after_own,
            after_sem.at[0],
            after_sem.at[1],
            {"tp": sibling},
        )

    ship(after_copy, c == q)

    @pl.when(c == q)
    def _():
        after_own[...] = after[:, own_features(t)]

    pass_on(UP, mate, FAR, ACROSS, cond=inner)
    row_copy(1 - c).wait_recv()

    begin, end, top, bottom = EDGE, length, 0, EDGE + length

    def edge_copy(i, source_block, source, block, dest, target):
        def rows_at(start):
            return pl.ds(pl.multiple_of(start, EDGE), EDGE)

        return remote(
            rows_all.at[source_block, rows_at(source)],
            rows_all.at[block, rows_at(dest)],
            edge_send.at[i],
            edge_recv.at[i],
            {"sp": target},
        )

    def pick(first, second):
        return first + y * (second - first)

    def edge(i):
        return (
            lambda: edge_copy(0, 0, pick(end, begin), 0, pick(top, bottom), across),
            lambda: edge_copy(
                1, pick(1, 0), pick(begin, end), pick(0, 1), pick(bottom, top), across
            ),
            lambda: edge_copy(2, 1, pick(end, begin), 1, pick(top, bottom), across),
        )[i]

    for i in range(3):
        ship(edge(i))
    onward = lambda: edge_copy(3, 1, end, 0, top, later)
    back = lambda: edge_copy(3, 0, begin, 1, bottom, earlier)
    ship(onward, before)
    ship(back, behind)
    feed(DOWN, MATE, cond=outer)

    @pl.when(jnp.logical_and(y == 0, h == 0))
    def _():
        rows_all[0, 0:EDGE, :] = jnp.zeros((EDGE, rows_all.shape[2]), bf16)

    @pl.when(jnp.logical_and(y == 1, h == 1))
    def _():
        rows_all[1, EDGE + length :, :] = jnp.zeros((EDGE, rows_all.shape[2]), bf16)

    arrive(GATE, across)
    arrive(GATE, amate)

    wide = 2 * LANES

    def expand(acc, weight, start, count, fresh, store=None):
        span = count * depth
        held_rows = pl.ds(EDGE if acc is gate_acc else 0, length)
        deep = pl.ds(pl.multiple_of(start * depth, depth), span)
        blocks = pl.ds(start, count)

        def tile(i, carry):
            b, cols = rem(i, 2), pl.ds(pl.multiple_of(div(i, 2) * wide, wide), wide)
            part = jnp.dot(
                rows_all[b, EDGE : EDGE + length, deep],
                weight[blocks, :, cols].reshape(span, wide),
                preferred_element_type=f32,
            )
            if store is not None:
                store(b, cols, part)
            elif fresh:
                acc[b, held_rows, cols] = part
            else:
                acc[b, held_rows, cols] += part
            return carry

        lax.fori_loop(0, 2 * (big // wide), tile, 0)

    expand(gate_acc, gates, half_sp * h, half_sp, True)
    pass_on(UP, mate, ACROSS, cond=outer)
    arrive(GATE, afar)
    arrive(GATE, afmate)
    expand(gate_acc, gates, half_sp * (1 - h), half_sp, False)
    arrive(UP, across)
    pass_on(UP, far, ACROSS)
    feed(DOWN, FAR, cond=outer)
    pass_on(UP, fmate, ACROSS, cond=inner)
    arrive(UP, amate)
    feed(DOWN, ADJACENT)
    feed(DOWN, FAR, MATE, cond=inner)
    expand(up_acc, ups, half_sp * h, half_sp, True)
    pass_on(DOWN, mate, FAR, ACROSS, cond=inner)
    pass_on(UP, fmate, ACROSS, cond=outer)
    for i in range(3):
        edge(i)().wait_recv()
    when(before, lambda: onward().wait_recv())
    when(behind, lambda: back().wait_recv())

    def halo(i, carry):
        cols = pl.ds(pl.multiple_of(i * wide, wide), wide)
        sides = (slice(0, EDGE), slice(EDGE + length, length + 2 * EDGE))
        part = jnp.dot(
            jnp.concatenate([rows_all[b, side, :] for b in range(2) for side in sides], axis=0),
            gates[:, :, cols].reshape(sp * depth, wide),
            preferred_element_type=f32,
        )
        for k in range(4):
            gate_acc[k // 2, sides[k % 2], cols] = part[k * EDGE : (k + 1) * EDGE]
        return carry

    lax.fori_loop(0, big // wide, halo, 0)

    base = jnp.where(c == q, q * (ff - big), q * (ff - small))

    def activate(b, carry):
        for j in range(big // LANES):
            cols = slice(j * LANES, (j + 1) * LANES)
            spot = jnp.minimum(base + j * LANES, ff - LANES)
            taps = pl.ds(pl.multiple_of(spot, LANES), LANES)

            def tap(start):
                return gate_acc[b, start : start + length, cols].astype(bf16).astype(f32)

            conv = (
                tap(EDGE - 1) * conv_weight[0:1, taps]
                + tap(EDGE) * conv_weight[1:2, taps]
                + tap(EDGE + 1) * conv_weight[2:3, taps]
                + conv_bias[pl.ds(div(spot, LANES), 1), :]
            )
            active[b, :, cols] = conv / (1.0 + jnp.exp(-conv))

        return carry

    lax.fori_loop(0, 2, activate, 0)
    pass_on(DOWN, mate, ACROSS, cond=outer)
    arrive(UP, afar)
    expand(up_acc, ups, div(far, 2) * 2, 2, False)
    arrive(UP, afmate)

    def finish(b, cols, part):
        hidden[b, :, cols] = (active[b, :, cols] * (up_acc[b, :, cols] + part)).astype(bf16)

    expand(up_acc, ups, div(fmate, 2) * 2, 2, False, finish)

    @pl.when(c != q)
    def _():
        hidden[:, :, small:] = jnp.zeros((2, length, big - small), bf16)

    per = sp // tp

    def owner(s):
        o = div(s, per)
        return div(o, 2), rem(o, 2)

    def core_slot(s):
        return div(s, half_sp) * per + rem(s, per)

    def core_copy(s):
        return remote(
            stage.at[s], from_core.at[core_slot(s)], part_send.at[0, s],
            core_recv.at[core_slot(s)], {"tp": sibling},
        )

    def z_copy(s):
        return remote(
            stage.at[s, 0], from_z.at[core_slot(s)], part_send.at[0, s],
            z_recv.at[core_slot(s)], {"sp": mate},
        )

    def x_copy(s):
        return remote(
            stage.at[s, 1], from_x.at[rem(s, per), 0], part_send.at[1, s],
            x_recv.at[rem(s, per)],
            {"tp": xdev},
        )

    def multiply(s):
        ox, oc = owner(s)
        product = jnp.dot(
            hidden[...].reshape(2 * length, big), downs[s], preferred_element_type=f32
        ).reshape(2, length, down_cols)

        @pl.when(c != oc)
        def _():
            stage[s] = product.astype(bf16)

        @pl.when(c == oc)
        def _():
            held[core_slot(s)] = product

        ship(lambda: core_copy(s), c != oc)

    def wide_copy(s):
        return remote(
            stage.at[s], from_x.at[rem(s, per)], part_send.at[0, s], x_recv.at[rem(s, per)],
            {"tp": xdev},
        )

    def add_core_x(s):
        ox, oc = owner(s)
        mine = c == oc
        slot = core_slot(s)

        @pl.when(mine)
        def _():
            core_copy(s).wait_recv()

        @pl.when(jnp.logical_and(mine, x != ox))
        def _():
            stage[s] = (held[slot] + from_core[slot].astype(f32)).astype(bf16)

        ship(lambda: wide_copy(s), jnp.logical_and(mine, x != ox))

    def add_x(s):
        ox, oc = owner(s)
        mine = jnp.logical_and(c == oc, x == ox)
        slot = core_slot(s)

        def summed(b):
            return (
                held[slot, b]
                + from_core[slot, b].astype(f32)
                + from_x[rem(s, per), b].astype(f32)
            )

        @pl.when(mine)
        def _():
            wide_copy(s).wait_recv()
            stage[s, 0] = summed(1 - q).astype(bf16)

        ship(lambda: z_copy(s), mine)

        @pl.when(mine)
        def _():
            after_own[:, out_cols(s)] += summed(q)

    def add_core(s):
        ox, oc = owner(s)
        mine = c == oc
        slot = core_slot(s)

        @pl.when(mine)
        def _():
            core_copy(s).wait_recv()
            stage[s, 0] = (held[slot, 1 - q] + from_core[slot, 1 - q].astype(f32)).astype(bf16)

        ship(lambda: z_copy(s), mine)

    def out_cols(s):
        return pl.ds(pl.multiple_of(rem(s, per) * down_cols, down_cols), down_cols)

    def add_z(s):
        ox, oc = owner(s)
        mine = c == oc
        slot = core_slot(s)

        def summed():
            return (
                held[slot, q] + from_core[slot, q].astype(f32) + from_z[slot].astype(f32)
            )

        when(mine, lambda: z_copy(s).wait_recv())

        @pl.when(jnp.logical_and(mine, x == ox))
        def _():
            after_own[:, out_cols(s)] += summed()

        @pl.when(jnp.logical_and(mine, x != ox))
        def _():
            stage[s, 1] = summed().astype(bf16)

        ship(lambda: x_copy(s), jnp.logical_and(mine, x != ox))

    settled = len(drains)
    multiply(me)
    multiply(mate)
    pass_on(DOWN, far, ACROSS, cond=inner)
    pass_on(DOWN[:1], far, ACROSS, cond=outer)
    add_core_x(me)
    arrive(DOWN, across)
    multiply(across)
    pass_on(DOWN[1:], far, ACROSS, cond=outer)
    add_core_x(mate)
    arrive(DOWN, amate)
    multiply(amate)
    add_core(across)
    multiply(far)
    add_core(amate)
    add_core_x(far)
    pass_on(DOWN, fmate, ACROSS)
    multiply(fmate)
    when(c != q, lambda: after_copy().wait_recv())
    arrive(DOWN, afar)
    multiply(afar)
    add_core_x(fmate)
    add_x(me)
    add_x(mate)
    add_core(afar)
    add_z(across)
    add_z(amate)
    for cond, make in drains[:settled]:
        when(cond, lambda: make().wait_send())
    arrive(DOWN, afmate)
    multiply(afmate)
    add_core(afmate)
    add_x(far)
    add_x(fmate)
    add_z(afar)
    add_z(afmate)
    for cond, make in drains[settled:]:
        when(cond, lambda: make().wait_send())
    for k in range(per):
        cols = slice(k * down_cols, (k + 1) * down_cols)
        source = per * t + k

        @pl.when(y == k)
        def _():
            slot = core_slot(source)
            z_copy(source).wait_recv()
            out[:, cols] = (after_own[:, cols] + from_z[slot].astype(f32)).astype(bf16)

        @pl.when(y != k)
        def _():
            x_copy(k).wait_recv()
            out[:, cols] = (after_own[:, cols] + from_x[k, 0].astype(f32)).astype(bf16)


def fused(sp, tp, *args):
    resid, queries, keys, values = args[:4]
    gate_weight, down_weight = args[8], args[12]
    length, width = queries.shape
    features = resid.shape[1]
    depth, ff = gate_weight.shape
    maps = 2
    heads = tp * (width // VD)
    full = tp * features
    bf16, f32 = jnp.bfloat16, jnp.float32
    dma = pltpu.SemaphoreType.DMA
    vmem = pl.BlockSpec(memory_space=pltpu.VMEM)
    smem = pl.BlockSpec(memory_space=pltpu.SMEM)
    hbm = pl.BlockSpec(memory_space=pl.ANY)
    rows = length + 2 * EDGE
    down_cols = down_weight.shape[1]
    tiles = ff // LANES
    big = (tiles - tiles // 2) * LANES
    per = sp // tp
    args = list(args)
    for i in (5, 7):
        args[i] = args[i].reshape(1, -1)
    args[11] = args[11].reshape(-1, LANES)
    return pl.pallas_call(
        functools.partial(layer_kernel, sp, tp),
        out_shape=pltpu.VMEM(resid.shape, bf16),
        in_specs=[
            hbm, hbm, hbm, hbm, smem, vmem, hbm, vmem, hbm, hbm, vmem, vmem, hbm,
        ],
        out_specs=vmem,
        scratch_shapes=[
            pltpu.VMEM((2, length, VD), bf16),
            pltpu.VMEM((maps, 2 * length, VD), bf16),
            pltpu.VMEM((sp, 2, length, VD), bf16),
            pltpu.VMEM((sp, depth, big), bf16),
            pltpu.VMEM((sp, depth, big), bf16),
            pltpu.VMEM((sp, big, down_cols), bf16),
            pltpu.VMEM((maps, 2 * length, LANES), f32),
            pltpu.VMEM((maps, 2 * length, LANES), f32),
            pltpu.VMEM((maps, 2 * length, VD), f32),
            pltpu.VMEM((2, length, VD), bf16),
            pltpu.VMEM((heads, length, VD), bf16),
            pltpu.VMEM((tp, heads * VD, features), bf16),
            pltpu.VMEM((tp, length, features), bf16),
            pltpu.VMEM((tp, 1, features), f32),
            pltpu.VMEM((length, full), f32),
            pltpu.VMEM((length, features), f32),
            pltpu.VMEM((2, rows, full), bf16),
            pltpu.VMEM((2, rows, big), f32),
            pltpu.VMEM((2, length, big), f32),
            pltpu.VMEM((2, length, big), f32),
            pltpu.VMEM((2, length, big), bf16),
            pltpu.VMEM((2 * per, 2, length, down_cols), f32),
            pltpu.VMEM((sp, 2, length, down_cols), bf16),
            pltpu.VMEM((2 * per, 2, length, down_cols), bf16),
            pltpu.VMEM((per, 2, length, down_cols), bf16),
            pltpu.VMEM((2 * per, length, down_cols), bf16),
            dma((16,)),
            dma((7, 8)),
            dma((7, sp)),
            dma((2,)),
            dma((8,)),
            dma((heads,)),
            dma((3,)),
            dma((tp,)),
            dma((5,)),
            dma((tp,)),
            dma((3,)),
            dma((tp,)),
            dma((2,)),
            dma((2,)),
            dma((4,)),
            dma((4,)),
            dma((2, sp)),
            dma((2 * per,)),
            dma((per,)),
            dma((2 * per,)),
        ],
        compiler_params=pltpu.CompilerParams(
            has_side_effects=True, collective_id=0, vmem_limit_bytes=60 * 1024 * 1024
        ),
    )(*args)


def solution(mesh):
    sp, tp = mesh.shape["sp"], mesh.shape["tp"]

    def run(*args):
        width, (depth, ff) = args[1].shape[1], args[8].shape
        small = args[0].shape[0] <= 512
        pairs = tp == 4 and sp == 2 * tp
        if pairs and small and depth % 256 == 0 and width == 2 * VD and ff % 256 == 128:
            return fused(sp, tp, *args)
        return on_device(*args)

    placed = (
        P("sp", "tp"),
        P("sp", "tp"),
        P("sp", "tp"),
        P("sp", "tp"),
        P("tp"),
        P(),
        P(None, "tp"),
        P("tp"),
        P("sp", "tp"),
        P("sp", "tp"),
        P(None, "tp"),
        P("tp"),
        P("tp", "sp"),
    )
    return jax.shard_map(
        run, mesh=mesh, in_specs=placed, out_specs=P("sp", "tp"), check_vma=False
    )
```

```python
import functools
import math

import jax
import jax.numpy as jnp
from jax import lax
from jax.experimental import pallas as pl
from jax.experimental.pallas import tpu as pltpu
from jax.sharding import PartitionSpec as P

D = 2048
HD = 64
VD = 128


def with_halo(cells, sides, width):
    for axis, dim in sides:
        count = lax.axis_size(axis)
        ends = count - 1
        head = lax.slice_in_dim(cells, 0, width, axis=dim)
        tail = lax.slice_in_dim(cells, cells.shape[dim] - width, cells.shape[dim], axis=dim)
        cells = jnp.concatenate(
            [
                lax.ppermute(tail, axis, [(i, (i + 1) % count) for i in range(ends)]),
                cells,
                lax.ppermute(head, axis, [((i + 1) % count, i) for i in range(ends)]),
            ],
            axis=dim,
        )
    return cells


def on_device(
    resid,
    queries,
    keys,
    values,
    mix_lambda,
    head_gain,
    out_weight,
    norm_gain,
    gate_weight,
    up_weight,
    conv_weight,
    conv_bias,
    down_weight,
):
    length = queries.shape[0]
    heads = mix_lambda.shape[0]
    scale = HD ** (-0.5)
    query_heads = queries.reshape(length, heads, 2, HD)
    initial = (
        jnp.full((heads, 2, length), -1e30, jnp.float32),
        jnp.zeros((heads, 2, length), jnp.float32),
        jnp.zeros((heads, 2, length, VD), jnp.float32),
    )
    key_rows = lax.all_gather(keys, "sp", axis=0, tiled=True)
    value_rows = lax.all_gather(values, "sp", axis=0, tiled=True)
    count = key_rows.shape[0]
    block = math.gcd(count, 2048)
    key_blocks = key_rows.reshape(count // block, block, heads, 2, HD)
    value_blocks = value_rows.reshape(count // block, block, heads, VD)

    def advance(state, blocks):
        running, totals, weighted = state
        key_block, value_block = blocks
        scores = (
            jnp.einsum(
                "qhmd,khmd->hmqk", query_heads, key_block, preferred_element_type=jnp.float32
            )
            * scale
        )
        highest = jnp.maximum(running, jnp.max(scores, axis=-1))
        factor = jnp.exp(running - highest)
        shifted = jnp.exp(scores - highest[..., None])
        totals = totals * factor + jnp.sum(shifted, axis=-1)
        weighted = weighted * factor[..., None] + jnp.einsum(
            "hmqk,khe->hmqe",
            shifted.astype(jnp.bfloat16),
            value_block,
            preferred_element_type=jnp.float32,
        )
        return ((highest, totals, weighted), None)

    result, unused = lax.scan(advance, initial, (key_blocks, value_blocks))
    running, totals, weighted = result
    mapped = weighted / totals[..., None]
    mixed = mapped[:, 0] - mix_lambda[:, None, None] * mapped[:, 1]
    spread = jnp.mean(mixed * mixed, axis=-1, keepdims=True)
    normed = mixed * lax.rsqrt(spread + 1e-06) * head_gain * 0.8
    heads_out = jnp.transpose(normed, (1, 0, 2)).reshape(length, heads * VD).astype(jnp.bfloat16)
    projected = jnp.dot(
        lax.all_gather(heads_out, "tp", axis=1, tiled=True),
        out_weight,
        preferred_element_type=jnp.float32,
    )
    after_mixer = resid.astype(jnp.float32) + projected
    squares = lax.psum(jnp.sum(after_mixer * after_mixer, axis=1), "tp")
    normed_rows = (after_mixer * lax.rsqrt(squares / D + 1e-06)[:, None] * norm_gain).astype(
        jnp.bfloat16
    )
    full_rows = lax.all_gather(normed_rows, "tp", axis=1, tiled=True)
    gate_sum = jnp.dot(
        full_rows,
        lax.all_gather(gate_weight, "sp", axis=0, tiled=True),
        preferred_element_type=jnp.float32,
    )
    upward = jnp.dot(
        full_rows,
        lax.all_gather(up_weight, "sp", axis=0, tiled=True),
        preferred_element_type=jnp.float32,
    )
    gated = gate_sum.astype(jnp.bfloat16)
    padded = with_halo(gated, (("sp", 0),), 1).astype(jnp.float32)
    conv = (
        padded[:-2] * conv_weight[0]
        + padded[1:-1] * conv_weight[1]
        + padded[2:] * conv_weight[2]
        + conv_bias
    )
    hidden = (jax.nn.silu(conv) * upward).astype(jnp.bfloat16)
    partial_terms = jnp.dot(
        hidden,
        lax.all_gather(down_weight, "sp", axis=1, tiled=True),
        preferred_element_type=jnp.float32,
    )
    mixer_out = lax.psum_scatter(
        partial_terms.astype(jnp.bfloat16), "tp", scatter_dimension=1, tiled=True
    ).astype(jnp.float32)
    return (after_mixer + mixer_out).astype(jnp.bfloat16)


EDGE = 16
LANES = 128


def layer_kernel(
    sp,
    tp,
    resid,
    queries,
    keys,
    values,
    mix_lambda,
    head_gain,
    out_weight,
    norm_gain,
    gate_weight,
    up_weight,
    conv_weight,
    conv_bias,
    down_weight,
    out,
    q_all,
    qs,
    kv,
    gates,
    ups,
    downs,
    peaks,
    totals,
    weighted,
    heads_own,
    heads_all,
    out_all,
    resid_all,
    gain_all,
    after,
    after_own,
    rows_all,
    gate_acc,
    up_acc,
    active,
    hidden,
    held,
    stage,
    from_core,
    from_x,
    from_z,
    local_sem,
    send_sem,
    recv_sem,
    q_sem,
    head_send,
    head_recv,
    out_send,
    out_recv,
    resid_send,
    resid_recv,
    gain_send,
    gain_recv,
    row_sem,
    after_sem,
    edge_send,
    edge_recv,
    part_send,
    core_recv,
    x_recv,
    z_recv,
):
    bf16, f32 = jnp.bfloat16, jnp.float32
    div, rem = lax.div, lax.rem
    me = lax.axis_index("sp")
    t = lax.axis_index("tp")
    z, y = div(me, 2), rem(me, 2)
    h, q = div(z, 2), rem(z, 2)
    x, c = div(t, 2), rem(t, 2)
    mate = me + 2 - 4 * q
    across = me + 1 - 2 * y
    far = me + 4 - 8 * h
    fmate = far + 2 - 4 * q
    adjacent = me + 2 - 4 * h
    amate = across + 2 - 4 * q
    afar = across + 4 - 8 * h
    afmate = afar + 2 - 4 * q
    inner, outer = h != q, h == q
    sibling = t + 1 - 2 * c
    xdev = t + 2 - 4 * x
    xsib = sibling + 2 - 4 * x

    length = queries.shape[0]
    depth, ff = gate_weight.shape
    features = resid.shape[1]
    big = gates.shape[2]
    small = ff - big
    down_cols = down_weight.shape[1]
    half_sp = sp // 2
    K, V = 0, 1
    KEYS, GATE, UP, DOWN = (K, V), (2,), (3, 4), (5, 6)
    ACROSS, FAR, MATE, ADJACENT = range(4)

    drains = []

    def both(a, b):
        return b if a is None else jnp.logical_and(a, b)

    def when(cond, body):
        if cond is None:
            body()
        else:
            pl.when(cond)(body)

    def remote(src, dst, send, recv, target):
        return pltpu.make_async_remote_copy(
            src_ref=src,
            dst_ref=dst,
            send_sem=send,
            recv_sem=recv,
            device_id=target,
            device_id_type=pl.DeviceIdType.MESH,
        )

    def ship(make, cond=None):
        when(cond, lambda: make().start())
        drains.append((cond, make))

    def variants(array, part):
        if array in KEYS:
            return ((None, 0),)
        return ((c == part, big), (c != part, small))

    def landing(array, src, size):
        if array in KEYS:
            return kv.at[src, array]
        if array in DOWN:
            rows = size // len(DOWN)
            return downs.at[src, pl.ds((array - DOWN[0]) * rows, rows)]
        if array in UP:
            rows = depth // len(UP)
            return ups.at[src, pl.ds((array - UP[0]) * rows, rows), pl.ds(0, size)]
        return gates.at[src, :, pl.ds(0, size)]

    def origin(array, part, size):
        if array in KEYS:
            cols = pl.ds(pl.multiple_of(part * VD, VD), VD)
            return (keys, values)[array].at[:, cols]
        start = part * (ff - size)
        if array in DOWN:
            rows = size // len(DOWN)
            first = start + (array - DOWN[0]) * rows
            return down_weight.at[pl.ds(pl.multiple_of(first, LANES // 2), rows)]
        cut = pl.ds(pl.multiple_of(start, LANES), size)
        if array in UP:
            rows = depth // len(UP)
            return up_weight.at[pl.ds((array - UP[0]) * rows, rows), cut]
        return gate_weight.at[:, cut]

    def send_slot(way, src):
        if src is me:
            return way
        return 4 if way == FAR else {id(mate): 5, id(far): 6, id(fmate): 7}[id(src)]

    def send(array, src, way, target, part=None, cond=None):
        for which, size in variants(array, q if part is None else part):

            def make(size=size):
                here = landing(array, src, size)
                return remote(
                    here if part is None else origin(array, part, size),
                    here,
                    send_sem.at[array, send_slot(way, src)],
                    recv_sem.at[array, src],
                    {"sp": target},
                )

            ship(make, both(cond, which) if which is not None else cond)

    def feed(group, *ways, cond=None):
        other = 1 - q
        for way in ways:
            for array in group:
                if way == ACROSS:
                    send(array, me, ACROSS, across, part=q)
                elif way == FAR:
                    send(array, me, FAR, far, part=q, cond=cond)
                elif way == MATE:
                    send(array, me, MATE, mate, part=other, cond=cond)
                else:
                    send(array, me, ADJACENT, adjacent, part=other, cond=inner)

    def arrive(group, src, cond=None):
        for array in group:
            for which, size in variants(array, q):

                def wait(size=size, array=array):
                    here = landing(array, src, size)
                    remote(
                        here, here, send_sem.at[array, 0], recv_sem.at[array, src], {"sp": across}
                    ).wait_recv()

                when(both(cond, which) if which is not None else cond, wait)

    def pass_on(group, src, *ways, cond=None):
        for array in group:
            arrive((array,), src, cond)
            for way in ways:
                if way == FAR:
                    send(array, src, FAR, far, cond=inner)
                else:
                    send(array, src, ACROSS, across, cond=cond)

    before = jnp.logical_and(y == 1, h == 0)
    behind = jnp.logical_and(y == 0, h == 1)
    later = jnp.minimum(me + half_sp - 1, sp - 1)
    earlier = jnp.maximum(me - half_sp + 1, 0)
    barrier = pltpu.get_barrier_semaphore()

    def greet(target, cond=None):
        when(
            cond,
            lambda: pl.semaphore_signal(
                barrier, inc=1, device_id=target, device_id_type=pl.DeviceIdType.MESH
            ),
        )

    for target in (
        {"sp": far},
        {"sp": mate},
        {"sp": mate, "tp": sibling},
        {"sp": across},
        {"tp": xdev},
        {"tp": xsib},
        {"tp": sibling},
    ):
        greet(target)
    greet({"sp": adjacent}, inner)
    greet({"sp": later}, before)
    greet({"sp": earlier}, behind)
    pl.semaphore_wait(
        barrier,
        7 + jnp.where(inner, 1, 0) + jnp.where(jnp.logical_or(before, behind), 1, 0),
    )

    for way in (MATE, ADJACENT, ACROSS):
        feed(KEYS, way)

    def q_copy():
        cols = pl.ds(pl.multiple_of((1 - q) * VD, VD), VD)
        return remote(queries.at[:, cols], q_all.at[q], q_sem.at[0], q_sem.at[1], {"sp": mate})

    local = []

    def fetch(src, dst, cond=None):
        sem = local_sem.at[len(local)]
        make = lambda: pltpu.make_async_copy(src, dst, sem)
        local.append((cond, make))
        when(cond, lambda: make().start())

    def fetched(first, last=None):
        for cond, make in local[first:last]:
            when(cond, lambda: make().wait())

    own_cols = pl.ds(pl.multiple_of(q * VD, VD), VD)
    fetch(queries.at[:, own_cols], q_all.at[q])
    for array in (K, V):
        fetch(origin(array, q, 0), landing(array, me, 0))
    early = len(local)
    for array in GATE + UP + DOWN:
        for which, size in variants(array, q):
            fetch(origin(array, q, size), landing(array, me, size), which)
    fetch(out_weight, out_all.at[t])
    fetch(resid, resid_all.at[t], c == q)
    fetch(norm_gain, gain_all.at[t])

    def out_copy(src, slot, target, send):
        return lambda: remote(
            src, out_all.at[slot], out_send.at[send], out_recv.at[slot], {"tp": target}
        )

    def gain_copy(target, send):
        return lambda: remote(
            norm_gain, gain_all.at[t], gain_send.at[send], gain_recv.at[t], {"tp": target}
        )

    def resid_copy(src, slot, target, send):
        return lambda: remote(
            src, resid_all.at[slot], resid_send.at[send], resid_recv.at[slot], target
        )

    for i, target in enumerate((sibling, xdev, xsib)):
        ship(gain_copy(target, i))
    ship(out_copy(out_weight, t, xdev, 0))
    ship(resid_copy(resid, t, {"tp": 2 * (1 - x) + q}, 0))
    ship(out_copy(out_weight, t, sibling, 1))
    ship(resid_copy(resid, t, {"tp": sibling}, 1), c != q)

    peaks[...] = jnp.full(peaks.shape, -1e30, f32)
    totals[...] = jnp.zeros(totals.shape, f32)
    weighted[...] = jnp.zeros(weighted.shape, f32)

    @pl.when(c != q)
    def _():
        downs[:, small:, :] = jnp.zeros((sp, big - small, down_cols), bf16)

    fetched(0, early)
    lanes = lax.broadcasted_iota(jnp.int32, (1, VD), 1)

    def spread_queries(block):
        value = q_all[block].astype(f32) * HD**-0.5
        at = pl.ds(pl.multiple_of(block * length, length), length)
        for m in range(2):
            keep = lanes < HD if m == 0 else lanes >= HD
            qs[m, at, :] = jnp.where(keep, value, 0.0).astype(bf16)

    rows = math.gcd(length, 256)

    def attend(src, first=0, last=2 * length // rows):
        def row_block(r, carry):
            at = pl.ds(pl.multiple_of(r * rows, rows), rows)
            key_block = kv[src, K]
            value_block = kv[src, V]
            for m in range(2):
                s = lax.dot_general(
                    qs[m, at, :], key_block, (((1,), (1,)), ((), ())), preferred_element_type=f32
                )
                old = peaks[m, at, :]
                new = jnp.maximum(old, jnp.max(s, axis=1, keepdims=True))
                factor = jnp.exp(old - new)
                p = jnp.exp(s - jnp.concatenate([new] * (length // VD), axis=1))
                peaks[m, at, :] = new
                summed = totals[m, at, :] * factor
                for j in range(length // VD):
                    summed = summed + p[:, j * VD : (j + 1) * VD]
                totals[m, at, :] = summed
                weighted[m, at, :] = weighted[m, at, :] * factor + jnp.dot(
                    p.astype(bf16), value_block, preferred_element_type=f32
                )
            return carry

        lax.fori_loop(first, last, row_block, 0)

    def kv_pass(src, *ways):
        pass_on(KEYS, src, *ways)

    per_block = length // rows
    spread_queries(q)
    attend(me, q * per_block, (q + 1) * per_block)
    feed(KEYS, FAR)
    ship(q_copy)
    ship(resid_copy(resid, t, {"sp": mate, "tp": 2 * x + q}, 2))
    feed(GATE, ACROSS)
    kv_pass(mate, FAR, ACROSS)
    feed(GATE, ADJACENT, FAR, MATE)
    attend(mate, q * per_block, (q + 1) * per_block)
    kv_pass(across)
    attend(across, q * per_block, (q + 1) * per_block)
    q_copy().wait_recv()
    spread_queries(1 - q)
    for src in (me, mate, across):
        attend(src, (1 - q) * per_block, (2 - q) * per_block)
    kv_pass(far, ACROSS)
    kv_pass(amate)
    attend(amate)
    kv_pass(fmate, ACROSS)
    feed(UP, ACROSS)
    feed(DOWN, ACROSS)
    attend(far)

    def resid_wait(slot):
        resid_copy(resid, slot, {"tp": sibling}, 0)().wait_recv()

    for k in range(2):
        slot = 2 * x + k
        when(c != q, lambda: resid_wait(slot))
        ship(resid_copy(resid_all.at[slot], slot, {"tp": xdev}, 3 + k), c != q)
    out_copy(out_weight, xdev, sibling, 0)().wait_recv()
    ship(out_copy(out_all.at[xdev], xdev, sibling, 2))
    attend(fmate)
    kv_pass(afar)
    attend(afar)
    pass_on(GATE, mate, FAR, ACROSS, cond=inner)
    feed(UP, ADJACENT)
    feed(UP, FAR, cond=inner)
    kv_pass(afmate)
    attend(afmate)

    head = 2 * t + q
    for b in range(2):
        at = slice(b * length, (b + 1) * length)
        first = weighted[0, at, :] / jnp.sum(totals[0, at, :], axis=1, keepdims=True)
        second = weighted[1, at, :] / jnp.sum(totals[1, at, :], axis=1, keepdims=True)
        mixed = first - mix_lambda[q] * second
        spread = jnp.mean(mixed * mixed, axis=1, keepdims=True)
        normed = mixed * lax.rsqrt(spread + 1e-06) * head_gain[...] * 0.8
        heads_own[b] = normed.astype(bf16)

        @pl.when(c == b)
        def _():
            heads_all[head] = heads_own[b]

    def head_copy(src, slot, target, send):
        return lambda: remote(
            src, heads_all.at[slot], head_send.at[send], head_recv.at[slot], target
        )

    for b in range(2):
        ship(head_copy(heads_own.at[b], head, {"sp": mate, "tp": 2 * x + b}, b))
    for b in range(2):
        ship(head_copy(heads_own.at[b], head, {"tp": 2 * (1 - x) + b}, 2 + b))
        ship(head_copy(heads_own.at[b], head, {"tp": sibling}, 4 + b), c != b)

    feed(UP, MATE)
    feed(UP, FAR, cond=outer)

    def head_wait(slot):
        head_copy(heads_all.at[slot], slot, {"tp": sibling}, 0)().wait_recv()

    pass_on(GATE, far, ACROSS, cond=inner)
    pass_on(GATE, mate, ACROSS, cond=outer)
    pass_on(GATE, far, ACROSS, cond=outer)
    for k in range(2):
        slot = 2 * (2 * x + k) + 1 - q
        head_wait(slot)
        ship(head_copy(heads_all.at[slot], slot, {"tp": xdev}, 6 + k))

    fetched(early)

    out_copy(out_weight, sibling, sibling, 0)().wait_recv()
    out_copy(out_weight, xsib, sibling, 0)().wait_recv()
    for slot in (sibling, xdev, xsib):
        remote(
            norm_gain, gain_all.at[slot], gain_send.at[0], gain_recv.at[slot], {"tp": sibling}
        ).wait_recv()
    when(c == q, lambda: resid_wait(sibling))
    for k in range(2):
        resid_wait(2 * (1 - x) + k)
    head_wait(2 * sibling + q)
    for k in range(2):
        head_wait(2 * (2 * (1 - x) + k) + q)
    for k in range(2):
        head_wait(2 * (2 * (1 - x) + k) + 1 - q)

    pass_on(GATE, fmate, ACROSS)
    row_sum = jnp.zeros((length, 1), f32)
    for j in range(tp):
        cols = slice(j * features, (j + 1) * features)
        total = resid_all[j].astype(f32) + jnp.dot(
            jnp.concatenate([heads_all[i] for i in range(heads_all.shape[0])], axis=1),
            out_all[j],
            preferred_element_type=f32,
        )
        after[:, cols] = total
        row_sum = row_sum + jnp.sum(total * total, axis=1, keepdims=True)
    inverse = lax.rsqrt(row_sum / D + 1e-06)
    for j in range(tp):
        cols = slice(j * features, (j + 1) * features)
        rows_all[c, EDGE : EDGE + length, cols] = (
            after[:, cols] * inverse * gain_all[j]
        ).astype(bf16)

    def row_copy(block):
        here = rows_all.at[block, pl.ds(EDGE, length)]
        return remote(here, here, row_sem.at[0], row_sem.at[1], {"tp": sibling})

    ship(lambda: row_copy(c))

    def own_features(device):
        return pl.ds(pl.multiple_of(device * features, features), features)

    def after_copy():
        return remote(
            after.at[:, own_features(sibling)],
            after_own,
            after_sem.at[0],
            after_sem.at[1],
            {"tp": sibling},
        )

    ship(after_copy, c == q)

    @pl.when(c == q)
    def _():
        after_own[...] = after[:, own_features(t)]

    pass_on(UP, mate, FAR, ACROSS, cond=inner)
    row_copy(1 - c).wait_recv()

    begin, end, top, bottom = EDGE, length, 0, EDGE + length

    def edge_copy(i, source_block, source, block, dest, target):
        def rows_at(start):
            return pl.ds(pl.multiple_of(start, EDGE), EDGE)

        return remote(
            rows_all.at[source_block, rows_at(source)],
            rows_all.at[block, rows_at(dest)],
            edge_send.at[i],
            edge_recv.at[i],
            {"sp": target},
        )

    def pick(first, second):
        return first + y * (second - first)

    def edge(i):
        return (
            lambda: edge_copy(0, 0, pick(end, begin), 0, pick(top, bottom), across),
            lambda: edge_copy(
                1, pick(1, 0), pick(begin, end), pick(0, 1), pick(bottom, top), across
            ),
            lambda: edge_copy(2, 1, pick(end, begin), 1, pick(top, bottom), across),
        )[i]

    for i in range(3):
        ship(edge(i))
    onward = lambda: edge_copy(3, 1, end, 0, top, later)
    back = lambda: edge_copy(3, 0, begin, 1, bottom, earlier)
    ship(onward, before)
    ship(back, behind)
    feed(DOWN, MATE, cond=outer)

    @pl.when(jnp.logical_and(y == 0, h == 0))
    def _():
        rows_all[0, 0:EDGE, :] = jnp.zeros((EDGE, rows_all.shape[2]), bf16)

    @pl.when(jnp.logical_and(y == 1, h == 1))
    def _():
        rows_all[1, EDGE + length :, :] = jnp.zeros((EDGE, rows_all.shape[2]), bf16)

    arrive(GATE, across)
    arrive(GATE, amate)

    wide = 2 * LANES

    def expand(acc, weight, start, count, fresh, store=None):
        span = count * depth
        held_rows = pl.ds(EDGE if acc is gate_acc else 0, length)
        deep = pl.ds(pl.multiple_of(start * depth, depth), span)
        blocks = pl.ds(start, count)

        def tile(i, carry):
            b, cols = rem(i, 2), pl.ds(pl.multiple_of(div(i, 2) * wide, wide), wide)
            part = jnp.dot(
                rows_all[b, EDGE : EDGE + length, deep],
                weight[blocks, :, cols].reshape(span, wide),
                preferred_element_type=f32,
            )
            if store is not None:
                store(b, cols, part)
            elif fresh:
                acc[b, held_rows, cols] = part
            else:
                acc[b, held_rows, cols] += part
            return carry

        lax.fori_loop(0, 2 * (big // wide), tile, 0)

    expand(gate_acc, gates, half_sp * h, half_sp, True)
    pass_on(UP, mate, ACROSS, cond=outer)
    arrive(GATE, afar)
    arrive(GATE, afmate)
    expand(gate_acc, gates, half_sp * (1 - h), half_sp, False)
    arrive(UP, across)
    pass_on(UP, far, ACROSS)
    feed(DOWN, FAR, cond=outer)
    pass_on(UP, fmate, ACROSS, cond=inner)
    arrive(UP, amate)
    feed(DOWN, MATE, cond=inner)
    expand(up_acc, ups, half_sp * h, half_sp, True)
    for piece in DOWN:
        feed((piece,), FAR, cond=inner)
        feed((piece,), ADJACENT)
    pass_on(DOWN, mate, FAR, ACROSS, cond=inner)
    pass_on(UP, fmate, ACROSS, cond=outer)
    for i in range(3):
        edge(i)().wait_recv()
    when(before, lambda: onward().wait_recv())
    when(behind, lambda: back().wait_recv())

    def halo(i, carry):
        cols = pl.ds(pl.multiple_of(i * wide, wide), wide)
        sides = (slice(0, EDGE), slice(EDGE + length, length + 2 * EDGE))
        part = jnp.dot(
            jnp.concatenate([rows_all[b, side, :] for b in range(2) for side in sides], axis=0),
            gates[:, :, cols].reshape(sp * depth, wide),
            preferred_element_type=f32,
        )
        for k in range(4):
            gate_acc[k // 2, sides[k % 2], cols] = part[k * EDGE : (k + 1) * EDGE]
        return carry

    lax.fori_loop(0, big // wide, halo, 0)

    base = jnp.where(c == q, q * (ff - big), q * (ff - small))

    def activate(b, carry):
        for j in range(big // LANES):
            cols = slice(j * LANES, (j + 1) * LANES)
            spot = jnp.minimum(base + j * LANES, ff - LANES)
            taps = pl.ds(pl.multiple_of(spot, LANES), LANES)

            def tap(start):
                return gate_acc[b, start : start + length, cols].astype(bf16).astype(f32)

            conv = (
                tap(EDGE - 1) * conv_weight[0:1, taps]
                + tap(EDGE) * conv_weight[1:2, taps]
                + tap(EDGE + 1) * conv_weight[2:3, taps]
                + conv_bias[pl.ds(div(spot, LANES), 1), :]
            )
            active[b, :, cols] = conv / (1.0 + jnp.exp(-conv))

        return carry

    lax.fori_loop(0, 2, activate, 0)
    arrive(UP, afar)
    expand(up_acc, ups, div(far, 2) * 2, 2, False)
    arrive(UP, afmate)

    def finish(b, cols, part):
        hidden[b, :, cols] = (active[b, :, cols] * (up_acc[b, :, cols] + part)).astype(bf16)

    expand(up_acc, ups, div(fmate, 2) * 2, 2, False, finish)

    @pl.when(c != q)
    def _():
        hidden[:, :, small:] = jnp.zeros((2, length, big - small), bf16)

    per = sp // tp

    def owner(s):
        o = div(s, per)
        return div(o, 2), rem(o, 2)

    def core_slot(s):
        return div(s, half_sp) * per + rem(s, per)

    def core_copy(s):
        return remote(
            stage.at[s], from_core.at[core_slot(s)], part_send.at[0, s],
            core_recv.at[core_slot(s)], {"tp": sibling},
        )

    def z_copy(s):
        return remote(
            stage.at[s, 0], from_z.at[core_slot(s)], part_send.at[0, s],
            z_recv.at[core_slot(s)], {"sp": mate},
        )

    def x_copy(s):
        return remote(
            stage.at[s, 1], from_x.at[rem(s, per), 0], part_send.at[1, s],
            x_recv.at[rem(s, per)],
            {"tp": xdev},
        )

    def multiply(s):
        ox, oc = owner(s)
        product = jnp.dot(
            hidden[...].reshape(2 * length, big), downs[s], preferred_element_type=f32
        ).reshape(2, length, down_cols)

        @pl.when(c != oc)
        def _():
            stage[s] = product.astype(bf16)

        @pl.when(c == oc)
        def _():
            held[core_slot(s)] = product

        ship(lambda: core_copy(s), c != oc)

    def wide_copy(s):
        return remote(
            stage.at[s], from_x.at[rem(s, per)], part_send.at[0, s], x_recv.at[rem(s, per)],
            {"tp": xdev},
        )

    def add_core_x(s):
        ox, oc = owner(s)
        mine = c == oc
        slot = core_slot(s)

        @pl.when(mine)
        def _():
            core_copy(s).wait_recv()

        @pl.when(jnp.logical_and(mine, x != ox))
        def _():
            stage[s] = (held[slot] + from_core[slot].astype(f32)).astype(bf16)

        ship(lambda: wide_copy(s), jnp.logical_and(mine, x != ox))

    def add_x(s):
        ox, oc = owner(s)
        mine = jnp.logical_and(c == oc, x == ox)
        slot = core_slot(s)

        def summed(b):
            return (
                held[slot, b]
                + from_core[slot, b].astype(f32)
                + from_x[rem(s, per), b].astype(f32)
            )

        @pl.when(mine)
        def _():
            wide_copy(s).wait_recv()
            stage[s, 0] = summed(1 - q).astype(bf16)

        ship(lambda: z_copy(s), mine)

        @pl.when(mine)
        def _():
            after_own[:, out_cols(s)] += summed(q)

    def add_core(s):
        ox, oc = owner(s)
        mine = c == oc
        slot = core_slot(s)

        @pl.when(mine)
        def _():
            core_copy(s).wait_recv()
            stage[s, 0] = (held[slot, 1 - q] + from_core[slot, 1 - q].astype(f32)).astype(bf16)

        ship(lambda: z_copy(s), mine)

    def out_cols(s):
        return pl.ds(pl.multiple_of(rem(s, per) * down_cols, down_cols), down_cols)

    def add_z(s):
        ox, oc = owner(s)
        mine = c == oc
        slot = core_slot(s)

        def summed():
            return (
                held[slot, q] + from_core[slot, q].astype(f32) + from_z[slot].astype(f32)
            )

        when(mine, lambda: z_copy(s).wait_recv())

        @pl.when(jnp.logical_and(mine, x == ox))
        def _():
            after_own[:, out_cols(s)] += summed()

        @pl.when(jnp.logical_and(mine, x != ox))
        def _():
            stage[s, 1] = summed().astype(bf16)

        ship(lambda: x_copy(s), jnp.logical_and(mine, x != ox))

    settled = len(drains)
    multiply(me)
    pass_on(DOWN, mate, ACROSS, cond=outer)
    multiply(mate)
    pass_on(DOWN, far, ACROSS, cond=inner)
    pass_on(DOWN[:1], far, ACROSS, cond=outer)
    add_core_x(me)
    arrive(DOWN, across)
    multiply(across)
    pass_on(DOWN[1:], far, ACROSS, cond=outer)
    add_core_x(mate)
    arrive(DOWN, amate)
    multiply(amate)
    add_core(across)
    multiply(far)
    add_core(amate)
    add_core_x(far)
    pass_on(DOWN, fmate, ACROSS)
    multiply(fmate)
    when(c != q, lambda: after_copy().wait_recv())
    arrive(DOWN, afar)
    multiply(afar)
    add_core_x(fmate)
    add_x(me)
    add_x(mate)
    add_core(afar)
    add_z(across)
    add_z(amate)
    for cond, make in drains[:settled]:
        when(cond, lambda: make().wait_send())
    arrive(DOWN, afmate)
    multiply(afmate)
    add_core(afmate)
    add_x(far)
    add_x(fmate)
    add_z(afar)
    add_z(afmate)
    for cond, make in drains[settled:]:
        when(cond, lambda: make().wait_send())
    for k in range(per):
        cols = slice(k * down_cols, (k + 1) * down_cols)
        source = per * t + k

        @pl.when(y == k)
        def _():
            slot = core_slot(source)
            z_copy(source).wait_recv()
            out[:, cols] = (after_own[:, cols] + from_z[slot].astype(f32)).astype(bf16)

        @pl.when(y != k)
        def _():
            x_copy(k).wait_recv()
            out[:, cols] = (after_own[:, cols] + from_x[k, 0].astype(f32)).astype(bf16)


def fused(sp, tp, *args):
    resid, queries, keys, values = args[:4]
    gate_weight, down_weight = args[8], args[12]
    length, width = queries.shape
    features = resid.shape[1]
    depth, ff = gate_weight.shape
    maps = 2
    heads = tp * (width // VD)
    full = tp * features
    bf16, f32 = jnp.bfloat16, jnp.float32
    dma = pltpu.SemaphoreType.DMA
    vmem = pl.BlockSpec(memory_space=pltpu.VMEM)
    smem = pl.BlockSpec(memory_space=pltpu.SMEM)
    hbm = pl.BlockSpec(memory_space=pl.ANY)
    rows = length + 2 * EDGE
    down_cols = down_weight.shape[1]
    tiles = ff // LANES
    big = (tiles - tiles // 2) * LANES
    per = sp // tp
    args = list(args)
    for i in (5, 7):
        args[i] = args[i].reshape(1, -1)
    args[11] = args[11].reshape(-1, LANES)
    return pl.pallas_call(
        functools.partial(layer_kernel, sp, tp),
        out_shape=pltpu.VMEM(resid.shape, bf16),
        in_specs=[
            hbm, hbm, hbm, hbm, smem, vmem, hbm, vmem, hbm, hbm, vmem, vmem, hbm,
        ],
        out_specs=vmem,
        scratch_shapes=[
            pltpu.VMEM((2, length, VD), bf16),
            pltpu.VMEM((maps, 2 * length, VD), bf16),
            pltpu.VMEM((sp, 2, length, VD), bf16),
            pltpu.VMEM((sp, depth, big), bf16),
            pltpu.VMEM((sp, depth, big), bf16),
            pltpu.VMEM((sp, big, down_cols), bf16),
            pltpu.VMEM((maps, 2 * length, LANES), f32),
            pltpu.VMEM((maps, 2 * length, LANES), f32),
            pltpu.VMEM((maps, 2 * length, VD), f32),
            pltpu.VMEM((2, length, VD), bf16),
            pltpu.VMEM((heads, length, VD), bf16),
            pltpu.VMEM((tp, heads * VD, features), bf16),
            pltpu.VMEM((tp, length, features), bf16),
            pltpu.VMEM((tp, 1, features), f32),
            pltpu.VMEM((length, full), f32),
            pltpu.VMEM((length, features), f32),
            pltpu.VMEM((2, rows, full), bf16),
            pltpu.VMEM((2, rows, big), f32),
            pltpu.VMEM((2, length, big), f32),
            pltpu.VMEM((2, length, big), f32),
            pltpu.VMEM((2, length, big), bf16),
            pltpu.VMEM((2 * per, 2, length, down_cols), f32),
            pltpu.VMEM((sp, 2, length, down_cols), bf16),
            pltpu.VMEM((2 * per, 2, length, down_cols), bf16),
            pltpu.VMEM((per, 2, length, down_cols), bf16),
            pltpu.VMEM((2 * per, length, down_cols), bf16),
            dma((16,)),
            dma((7, 8)),
            dma((7, sp)),
            dma((2,)),
            dma((8,)),
            dma((heads,)),
            dma((3,)),
            dma((tp,)),
            dma((5,)),
            dma((tp,)),
            dma((3,)),
            dma((tp,)),
            dma((2,)),
            dma((2,)),
            dma((4,)),
            dma((4,)),
            dma((2, sp)),
            dma((2 * per,)),
            dma((per,)),
            dma((2 * per,)),
        ],
        compiler_params=pltpu.CompilerParams(
            has_side_effects=True, collective_id=0, vmem_limit_bytes=60 * 1024 * 1024
        ),
    )(*args)


def solution(mesh):
    sp, tp = mesh.shape["sp"], mesh.shape["tp"]

    def run(*args):
        width, (depth, ff) = args[1].shape[1], args[8].shape
        small = args[0].shape[0] <= 512
        pairs = tp == 4 and sp == 2 * tp
        if pairs and small and depth % 256 == 0 and width == 2 * VD and ff % 256 == 128:
            return fused(sp, tp, *args)
        return on_device(*args)

    placed = (
        P("sp", "tp"),
        P("sp", "tp"),
        P("sp", "tp"),
        P("sp", "tp"),
        P("tp"),
        P(),
        P(None, "tp"),
        P("tp"),
        P("sp", "tp"),
        P("sp", "tp"),
        P(None, "tp"),
        P("tp"),
        P("tp", "sp"),
    )
    return jax.shard_map(
        run, mesh=mesh, in_specs=placed, out_specs=P("sp", "tp"), check_vma=False
    )
```
